512 devices in a mesh: sp: 128 (over z, x, core), tp: 4 (over y).
Axes of the slice: x: 4, y: 4, z: 16, core: 2. Of those that a mesh axis runs over, the one named last changes fastest.
Arguments:
- tokens: bfloat16 [65536, 2048], P('sp', 'tp'), may hold values from -72 to 72
- w_query: bfloat16 [2048, 1024], P('sp', 'tp'), may hold values from -0.125 to 0.125
- w_key: bfloat16 [2048, 256], P('sp', 'tp'), may hold values from -0.125 to 0.125
- w_value: bfloat16 [2048, 256], P('sp', 'tp'), may hold values from -0.125 to 0.125
- w_pool_in: bfloat16 [2048, 1024], P('sp', 'tp'), may hold values from -0.125 to 0.125
- sink: float32 [16], P('tp'), may hold values from 3 to 7
- w_pool: bfloat16 [4, 256, 256], P('tp'), may hold values from -0.375 to 0.375
- pool_scale: float32 [1024], P('tp'), may hold values from 0.1 to 1.9
- w_out_attn: bfloat16 [1024, 2048], P('tp', 'sp'), may hold values from -0.5 to 0.5
- w_out_pool: bfloat16 [1024, 2048], P('tp', 'sp'), may hold values from -0.125 to 0.125
- out_gain: float32 [2048], P('tp'), may hold values from 0.1 to 1.9
Outputs:
- mixed: bfloat16 [65536, 2048], P('sp', 'tp')
The draws below stay inside these ranges and needn't reach their ends.
All inputs are finite; a program needn't handle non-finite values.
Results may differ from the reference program's by a relative error of at most 0.012.
The reference program's roundings to bfloat16 on the way count: a program that leaves them out, or rounds other values in their place, can miss the bound.
Values may be sent and summed in bfloat16 or wider, within the bound.
No kernel may reach another device: no remote copies, remote signals or barrier semaphores. Data moves between devices by JAX's collectives and lax.ppermute only.
A program may use at most 64 MiB of HBM per device.

```python
import jax
import jax.numpy as jnp
from jax import lax

D = 2048
HEADS = 16
KV_HEADS = 4
HEAD_DIM = 64
POOL_GROUPS = 4
GROUP_DIM = 256
WINDOW = 128
SEQ = 65536
ATTN_WIDTH = 1024
KV_WIDTH = 256
POOL_WIDTH = 1024
N_TP = 4


def draw_tokens(key, part):
    base = jnp.clip(jax.random.normal(key, (SEQ, D), jnp.float32), -6.0, 6.0)
    return base.astype(jnp.bfloat16)


def levels(stream_key, dims, pieces, smallest, top_value):
    level = 1.0
    for position, shards_of in pieces:
        heights = jax.random.uniform(jax.random.fold_in(jax.random.fold_in(stream_key, 6), position), (shards_of,), jnp.float32, smallest / len(pieces), top_value / len(pieces))
        level = level * jnp.repeat(jnp.exp(heights), dims[position] // shards_of).reshape((-1,) + (1,) * (len(dims) - 1 - position))
    return level


def centred(rng, shape, deviation, bound, shards=(), kind=jnp.bfloat16):
    entries = jax.random.normal(rng, shape, jnp.float32) * deviation
    if len(shards) > 0:
        entries = levels(rng, shape, shards, -0.22, 0.18) * entries
    return jnp.clip(entries, min=-bound, max=bound).astype(kind)


def setup_inputs(seed: int = 0) -> dict:
    splits = jax.random.split(jax.random.key(seed), 12)
    return {
        "tokens": draw_tokens(jax.random.fold_in(splits[11], 71), 0),
        "w_query": centred(splits[1], (D, ATTN_WIDTH), D ** -0.5, 0.125, ((0, 128), (1, 4))),
        "w_key": centred(splits[2], (D, KV_WIDTH), D ** -0.5, 0.125, ((0, 128), (1, 4))),
        "w_value": centred(splits[3], (D, KV_WIDTH), D ** -0.5, 0.125, ((0, 128), (1, 4))),
        "w_pool_in": centred(splits[4], (D, POOL_WIDTH), D ** -0.5, 0.125, ((0, 128), (1, 4))),
        "sink": jnp.clip(3.0 + 4.0 * jax.random.uniform(splits[5], (HEADS,), jnp.float32) ** levels(splits[5], (HEADS,), ((0, 4),), -0.2, 0.2), 3.0, 7.0),
        "w_pool": centred(splits[6], (POOL_GROUPS, GROUP_DIM, GROUP_DIM), GROUP_DIM ** -0.5, 0.375, ((0, 4),)),
        "pool_scale": jnp.clip(1.0 + 0.18 * jax.random.normal(splits[7], (POOL_WIDTH,), jnp.float32), 0.1, 1.9),
        "w_out_attn": centred(splits[8], (ATTN_WIDTH, D), (ATTN_WIDTH // 8) ** -0.5, 0.5, ((0, 4), (1, 128))),
        "w_out_pool": centred(splits[9], (POOL_WIDTH, D), (ATTN_WIDTH + POOL_WIDTH) ** -0.5, 0.125, ((0, 4), (1, 128))),
        "out_gain": jnp.clip(1.0 + 0.18 * jax.random.normal(splits[10], (D,), jnp.float32), 0.1, 1.9),
    }


epsilon = 1e-05
masked_score = -1e+30

def attend_head(query_one, key_one, value_one, sink_one):
    seq_len = query_one.shape[0]
    group = query_one.shape[1]
    block_count = seq_len // WINDOW
    query_blocks = query_one.reshape(block_count, WINDOW, group, HEAD_DIM).astype(jnp.float32)

    def banded(source):
        padded = jnp.pad(source, ((WINDOW, WINDOW), (0, 0))).reshape(block_count + 2, WINDOW, HEAD_DIM)
        return jnp.concatenate([padded[:-2], padded[1:-1], padded[2:]], axis=1).astype(jnp.float32)
    key_band = banded(key_one)
    value_band = banded(value_one)
    scores = jnp.einsum('nqgd,nsd->ngqs', query_blocks, key_band) * HEAD_DIM ** (-0.5)
    starts = jnp.arange(block_count, dtype=jnp.int32) * WINDOW
    query_pos = starts[:, None] + jnp.arange(WINDOW, dtype=jnp.int32)[None, :]
    key_pos = starts[:, None] + jnp.arange(3 * WINDOW, dtype=jnp.int32)[None, :] - WINDOW
    distance = key_pos[:, None, :] - query_pos[:, :, None]
    inside = (key_pos >= 0) & (key_pos < seq_len)
    keep = (jnp.abs(distance) <= WINDOW) & inside[:, None, :]
    scores = jnp.where(keep[:, None], scores, masked_score)
    sink_logit = sink_one.astype(jnp.float32)[None, :, None, None]
    top = jnp.maximum(lax.optimization_barrier(jnp.max(scores, axis=-1, keepdims=True)), sink_logit)
    raised = jnp.exp(scores - top)
    total = lax.optimization_barrier(jnp.sum(raised, axis=-1, keepdims=True)) + jnp.exp(sink_logit - top)
    probs = (raised / total).astype(jnp.bfloat16)
    attended = jnp.einsum('ngqs,nsd->nqgd', probs.astype(jnp.float32), value_band)
    return attended.astype(jnp.bfloat16).reshape(seq_len, group * HEAD_DIM)

def reference(tokens, w_query, w_key, w_value, w_pool_in, sink, w_pool, pool_scale, w_out_attn, w_out_pool, out_gain):
    seq_len = tokens.shape[0]
    group = HEADS // KV_HEADS
    query = jnp.dot(tokens, w_query, preferred_element_type=jnp.float32).astype(jnp.bfloat16)
    keys = jnp.dot(tokens, w_key, preferred_element_type=jnp.float32).astype(jnp.bfloat16)
    values = jnp.dot(tokens, w_value, preferred_element_type=jnp.float32).astype(jnp.bfloat16)
    chan = jnp.dot(tokens, w_pool_in, preferred_element_type=jnp.float32).astype(jnp.bfloat16)
    query_heads = query.reshape(seq_len, KV_HEADS, group, HEAD_DIM).transpose(1, 0, 2, 3)
    key_heads = keys.reshape(seq_len, KV_HEADS, HEAD_DIM).transpose(1, 0, 2)
    value_heads = values.reshape(seq_len, KV_HEADS, HEAD_DIM).transpose(1, 0, 2)
    sink_heads = sink.reshape(KV_HEADS, group)
    attended = lax.map(lambda parts: attend_head(*parts), (query_heads, key_heads, value_heads, sink_heads))
    attended = attended.transpose(1, 0, 2).reshape(seq_len, HEADS * HEAD_DIM)
    chan_float = chan.astype(jnp.float32)
    running = jnp.concatenate([jnp.zeros((1, POOL_WIDTH), jnp.float32), jnp.cumsum(chan_float, axis=0)], axis=0)
    positions = jnp.arange(seq_len, dtype=jnp.int32)
    outputs = []
    for level in range(POOL_GROUPS):
        half = 2 ** level
        lower = jnp.clip(positions - half, 0, seq_len)
        upper = jnp.clip(positions + half, 0, seq_len)
        columns = slice(level * GROUP_DIM, (level + 1) * GROUP_DIM)
        band = running[:, columns]
        count = (upper - lower).astype(jnp.float32)
        spread = ((band[upper] - band[lower]) / count[:, None] - chan_float[:, columns]).astype(jnp.bfloat16)
        outputs.append(jnp.dot(spread, w_pool[level], preferred_element_type=jnp.float32))
    pooled = (jnp.concatenate(outputs, axis=1) * pool_scale).astype(jnp.bfloat16)
    attn_share = ATTN_WIDTH // N_TP
    pool_share = POOL_WIDTH // N_TP
    mix = jnp.zeros((seq_len, D), jnp.float32)
    for device in range(N_TP):
        attn_cols = slice(device * attn_share, (device + 1) * attn_share)
        pool_cols = slice(device * pool_share, (device + 1) * pool_share)
        partial_sum = jnp.dot(attended[:, attn_cols], w_out_attn[attn_cols], preferred_element_type=jnp.float32)
        partial_sum = partial_sum + jnp.dot(pooled[:, pool_cols], w_out_pool[pool_cols], preferred_element_type=jnp.float32)
        mix = mix + partial_sum.astype(jnp.bfloat16).astype(jnp.float32)
    row_mean = lax.optimization_barrier(jnp.sum(mix, axis=1)) / D
    variance = lax.optimization_barrier(jnp.sum(mix * mix, axis=1)) / D - row_mean * row_mean
    normed = (mix - row_mean[:, None]) * lax.rsqrt(variance + epsilon)[:, None] * out_gain
    return normed.astype(jnp.bfloat16)
```

```python
import jax
import jax.numpy as jnp
from jax import lax
from jax.sharding import Mesh
from jax.sharding import PartitionSpec as P


HEAD_DIM = 64
POOL_GROUPS = 4
WINDOW = 128
SP = ("sp_0", "sp_1", "sp_2")
Z, X, CORE = SP


epsilon = 1e-05
masked_score = -1e30


def from_everyone(shard, axis):
    count = lax.axis_size(axis)
    return lax.all_to_all(
        jnp.broadcast_to(shard[None], (count, *shard.shape)), axis, 0, 0, tiled=True
    )


def in_order(pieces, dim):
    dims = list(pieces.shape[1:])
    dims[dim] *= pieces.shape[0]
    return jnp.moveaxis(pieces, 0, dim).reshape(dims)


def gather_directly(shard, axis, dim):
    pieces = from_everyone(shard, axis)
    return in_order(pieces, dim)


def gather_weights(pieces):
    packed = jnp.concatenate(pieces, axis=1)
    over_z = lax.all_gather(packed, Z, axis=0)
    return over_z


def over_x_and_cores(over_z):
    own = from_everyone(over_z, X).reshape(lax.axis_size(X), *over_z.shape)
    other = lax.ppermute(own, CORE, [(0, 1), (1, 0)])
    first = lax.axis_index(CORE) == 0
    both = jnp.stack([jnp.where(first, own, other), jnp.where(first, other, own)])
    core, x, z, rows, cols = both.shape
    return both.transpose(2, 1, 0, 3, 4).reshape(z * x * core * rows, cols)


def neighbours(head, tail, axis):
    count = lax.axis_size(axis)
    before = lax.ppermute(tail, axis, [(i, i + 1) for i in range(count - 1)])
    after = lax.ppermute(head, axis, [(i + 1, i) for i in range(count - 1)])
    return before, after


def cut_along(shard, dim, count):
    dims = shard.shape
    pieces = shard.reshape(*dims[:dim], count, dims[dim] // count, *dims[dim + 1 :])
    return jnp.moveaxis(pieces, dim, 0)


def sent_and_summed(shard, axis, dim):
    count = lax.axis_size(axis)
    pieces = lax.all_to_all(cut_along(shard, dim, count), axis, 0, 0, tiled=True)
    return jnp.sum(pieces.astype(jnp.float32), axis=0)


def of_everyone(shard, axis):
    everything = from_everyone(shard, axis)
    return jnp.sum(everything, axis=0)


def in_one(arrays, axis):
    ends = [0]
    for a in arrays:
        ends.append(ends[-1] + a.size)
    so_far = of_everyone(jnp.concatenate([a.ravel() for a in arrays]), axis)
    return tuple((so_far[b:e].reshape(a.shape) for a, b, e in zip(arrays, ends, ends[1:])))


def attend_local(query, keys_ext, sinks, offset, seq_len, key_cols):
    tok_rows, query_cols = query.shape
    kv_local = key_cols // HEAD_DIM
    group = query_cols // key_cols
    block_count = tok_rows // WINDOW
    stacked = keys_ext.reshape(block_count + 2, WINDOW, 2 * key_cols)
    banded = jnp.concatenate([stacked[:-2], stacked[1:-1], stacked[2:]], axis=1)
    key_band = banded[:, :, :key_cols].reshape(block_count, 3 * WINDOW, kv_local, HEAD_DIM)
    value_band = banded[:, :, key_cols:].reshape(block_count, 3 * WINDOW, kv_local, HEAD_DIM)
    query_blocks = query.reshape(block_count, WINDOW, kv_local, group, HEAD_DIM)
    scores = jnp.einsum(
        "nqkgd,nskd->nkgqs", query_blocks, key_band, preferred_element_type=jnp.float32
    ) * HEAD_DIM ** (-0.5)
    starts = offset + jnp.arange(block_count, dtype=jnp.int32) * WINDOW
    query_pos = starts[:, None] + jnp.arange(WINDOW, dtype=jnp.int32)[None, :]
    key_pos = starts[:, None] + jnp.arange(3 * WINDOW, dtype=jnp.int32)[None, :] - WINDOW
    distance = key_pos[:, None, :] - query_pos[:, :, None]
    inside = (key_pos >= 0) & (key_pos < seq_len)
    keep = (jnp.abs(distance) <= WINDOW) & inside[:, None, :]
    scores = jnp.where(keep[:, None, None], scores, masked_score)
    sink_logit = sinks.reshape(kv_local, group)[None, :, :, None, None]
    top = jnp.maximum(jnp.max(scores, axis=-1, keepdims=True), sink_logit)
    raised = jnp.exp(scores - top)
    total = jnp.sum(raised, axis=-1, keepdims=True) + jnp.exp(sink_logit - top)
    probs = (raised / total).astype(jnp.bfloat16)
    attended = jnp.einsum(
        "nkgqs,nskd->nqkgd", probs, value_band, preferred_element_type=jnp.float32
    )
    return attended.astype(jnp.bfloat16).reshape(tok_rows, query_cols)


def layer(
    tokens,
    w_query,
    w_key,
    w_value,
    w_pool_in,
    sink,
    w_pool,
    pool_scale,
    w_out_attn,
    w_out_pool,
    out_gain,
):
    tok_rows = tokens.shape[0]
    seq_len = tok_rows * lax.axis_size(SP)
    offset = lax.axis_index(SP) * tok_rows
    key_cols = w_key.shape[1]
    chan_cols = w_pool_in.shape[1]
    gathered = gather_directly(tokens, "tp", 1)
    pieces = (w_query, w_key, w_value, w_pool_in, w_out_attn.T, w_out_pool.T)
    in_cols = w_query.shape[1] + 2 * key_cols + chan_cols
    over_z = gather_weights(pieces)
    in_whole = over_x_and_cores(over_z[:, :, :in_cols])
    out_whole = over_x_and_cores(over_z[:, :, in_cols:])
    projected = jnp.dot(gathered, in_whole, preferred_element_type=jnp.float32)
    projected = projected.astype(jnp.bfloat16)
    query = projected[:, : w_query.shape[1]]
    key_value = projected[:, w_query.shape[1] : in_cols - chan_cols]
    chan = projected[:, in_cols - chan_cols :]
    rim_rows = 2 ** (POOL_GROUPS - 1)

    def rim(start_kv, start_chan):
        return jnp.concatenate(
            [
                key_value[start_kv : start_kv + WINDOW],
                chan[start_chan : start_chan + rim_rows].reshape(-1, 2 * key_cols),
            ]
        )

    before, after = neighbours(rim(0, 0), rim(tok_rows - WINDOW, tok_rows - rim_rows), SP)
    keys_ext = jnp.concatenate([before[:WINDOW], key_value, after[:WINDOW]])
    chan_ext = jnp.concatenate(
        [
            before[WINDOW:].reshape(rim_rows, chan_cols),
            chan,
            after[WINDOW:].reshape(rim_rows, chan_cols),
        ]
    )
    attended = attend_local(query, keys_ext, sink, offset, seq_len, key_cols)
    running = jnp.concatenate(
        [jnp.zeros((1, chan_cols), jnp.float32), jnp.cumsum(chan_ext.astype(jnp.float32), axis=0)],
        axis=0,
    )
    chan_float = chan.astype(jnp.float32)
    positions = offset + jnp.arange(tok_rows, dtype=jnp.int32)
    group_count = w_pool.shape[0]
    level = lax.axis_index("tp") * group_count + 0
    half = jnp.left_shift(jnp.int32(1), level)
    upper = lax.dynamic_slice_in_dim(running, rim_rows + half, tok_rows, 0)
    lower = lax.dynamic_slice_in_dim(running, rim_rows - half, tok_rows, 0)
    count = (
        jnp.clip(positions + half, 0, seq_len) - jnp.clip(positions - half, 0, seq_len)
    ).astype(jnp.float32)
    spread = ((upper - lower) / count[:, None] - chan_float).astype(jnp.bfloat16)
    outputs = jnp.dot(spread, w_pool[0], preferred_element_type=jnp.float32)
    pooled = (outputs * pool_scale).astype(jnp.bfloat16)
    hidden = jnp.concatenate([attended, pooled], axis=1)
    terms = lax.dot_general(
        hidden, out_whole, (((1,), (1,)), ((), ())), preferred_element_type=jnp.float32
    )
    share_width = out_gain.shape[0]
    model_width = share_width * lax.axis_size("tp")
    share = sent_and_summed(terms.astype(jnp.bfloat16), "tp", 1)
    row_total, row_square = in_one((jnp.sum(share, axis=1), jnp.sum(share * share, axis=1)), "tp")
    row_mean = row_total / model_width
    variance = row_square / model_width - row_mean * row_mean
    normed = (share - row_mean[:, None]) * lax.rsqrt(variance + epsilon)[:, None] * out_gain
    return normed.astype(jnp.bfloat16)


def solution(mesh):
    finer = Mesh(mesh.devices.reshape(16, 4, 2, mesh.shape["tp"]), ("sp_0", "sp_1", "sp_2", "tp"))
    return jax.shard_map(
        layer,
        mesh=finer,
        in_specs=(
            P(SP, "tp"),
            P(SP, "tp"),
            P(SP, "tp"),
            P(SP, "tp"),
            P(SP, "tp"),
            P("tp"),
            P("tp", None, None),
            P("tp"),
            P("tp", SP),
            P("tp", SP),
            P("tp"),
        ),
        out_specs=P(SP, "tp"),
        check_vma=False,
    )
```

```python
import functools

import jax
import jax.numpy as jnp
from jax import lax
from jax.experimental import pallas as pl
from jax.experimental.pallas import tpu as pltpu
from jax.sharding import Mesh
from jax.sharding import PartitionSpec as P


HEAD_DIM = 64
PAIR = 2 * HEAD_DIM
POOL_GROUPS = 4
RIM = 2 ** (POOL_GROUPS - 1)
WINDOW = 128
SP = ("sp_0", "sp_1", "sp_2")
Z, X, CORE = SP
TP = "tp"
BF16, F32 = jnp.bfloat16, jnp.float32

epsilon = 1e-05
masked_score = -1e30
nt = (((1,), (1,)), ((), ()))


def from_everyone(shard, axis):
    count = lax.axis_size(axis)
    return lax.all_to_all(
        jnp.broadcast_to(shard[None], (count, *shard.shape)), axis, 0, 0, tiled=True
    )


def of_everyone(shard, axis):
    return jnp.sum(from_everyone(shard, axis), axis=0)


def swapped(shard, axis, mask):
    return lax.ppermute(shard, axis, [(i, i ^ mask) for i in range(lax.axis_size(axis))])


def neighbours(head, tail, axis):
    count = lax.axis_size(axis)
    before = lax.ppermute(tail, axis, [(i, i + 1) for i in range(count - 1)])
    after = lax.ppermute(head, axis, [(i + 1, i) for i in range(count - 1)])
    return before, after


def in_stored_order(place, own_ref, other_ref, first, count):
    core = lax.axis_index(CORE)
    xs, rows = own_ref.shape[0], own_ref.shape[2]
    for z in range(count):
        for x in range(xs):
            base = ((first + z) * xs + x) * 2 * rows
            place(pl.multiple_of(base + core * rows, rows), own_ref[x, first + z])
            place(pl.multiple_of(base + (1 - core) * rows, rows), other_ref[x, first + z])


def project_kernel(
    widths, tokens_ref, own_ref, other_ref, query_ref, kv_ref, chan_ref, head_ref, tail_ref, w_ref
):
    pieces, rows, depth = tokens_ref.shape

    def place(at, block):
        w_ref[pl.ds(at, block.shape[0]), :] = block

    in_stored_order(place, own_ref, other_ref, 0, own_ref.shape[1])
    at = 0
    for ref, width in zip((query_ref, kv_ref, chan_ref), widths):
        total = jnp.dot(tokens_ref[0], w_ref[:depth, at : at + width], preferred_element_type=F32)
        for p in range(1, pieces):
            total += jnp.dot(
                tokens_ref[p],
                w_ref[p * depth : (p + 1) * depth, at : at + width],
                preferred_element_type=F32,
            )
        ref[...] = total.astype(BF16)
        at += width
    for ref, kv_at, chan_at in ((head_ref, 0, 0), (tail_ref, rows - WINDOW, rows - RIM)):
        ref[:WINDOW] = kv_ref[kv_at : kv_at + WINDOW]
        edge = chan_ref[chan_at : chan_at + RIM].astype(F32)
        ref[WINDOW:] = jnp.concatenate([edge[:, :PAIR], edge[:, PAIR:]]).astype(BF16)


def mix_kernel(
    half,
    seq_len,
    query_ref,
    kv_ref,
    chan_ref,
    rim_ref,
    sink_ref,
    w_pool_ref,
    scale_ref,
    own_ref,
    other_ref,
    sent_ref,
    kept_ref,
    band_ref,
    hidden_ref,
    w_ref,
):
    rows = query_ref.shape[0] // 2
    row0 = half * rows
    y = lax.axis_index(TP)
    offset = lax.axis_index(SP) * query_ref.shape[0] + row0
    blocks = rows // WINDOW
    query_cols = query_ref.shape[1]

    rim_kv = rim_ref[:WINDOW]
    rim_chan = rim_ref[WINDOW:].astype(F32)
    rim_chan = jnp.concatenate([rim_chan[:RIM], rim_chan[RIM:]], axis=1)
    if half == 0:
        kv = jnp.concatenate([rim_kv, kv_ref[: rows + WINDOW]])
        chan = jnp.concatenate([rim_chan, chan_ref[: rows + 2 * RIM].astype(F32)[: rows + RIM]])
    else:
        kv = jnp.concatenate([kv_ref[row0 - WINDOW :], rim_kv])
        chan = jnp.concatenate([chan_ref[row0 - 2 * RIM :].astype(F32)[RIM:], rim_chan])

    kv = kv.astype(F32)
    turned = pltpu.roll(kv, HEAD_DIM, 1)
    low = lax.broadcasted_iota(jnp.int32, kv.shape, 1) < HEAD_DIM
    band_ref[0] = jnp.where(low, kv, 0.0).astype(BF16)
    band_ref[1] = jnp.where(low, 0.0, turned).astype(BF16)
    band_ref[2] = jnp.where(low, turned, 0.0).astype(BF16)
    band_ref[3] = jnp.where(low, 0.0, kv).astype(BF16)

    row = lax.broadcasted_iota(jnp.int32, (WINDOW, 3 * WINDOW), 0)
    col = lax.broadcasted_iota(jnp.int32, (WINDOW, 3 * WINDOW), 1)
    near = (col >= row) & (col <= row + 2 * WINDOW)
    for b in range(blocks):
        key_pos = col + (offset + (b - 1) * WINDOW)
        keep = near & (key_pos >= 0) & (key_pos < seq_len)
        band = pl.ds(b * WINDOW, 3 * WINDOW)
        for pair in range(query_cols // PAIR):
            queries = query_ref[
                row0 + b * WINDOW : row0 + (b + 1) * WINDOW, pair * PAIR : (pair + 1) * PAIR
            ]
            attended = jnp.zeros((WINDOW, PAIR), F32)
            for side in range(2):
                scores = lax.dot_general(
                    queries, band_ref[side, band], nt, preferred_element_type=F32
                ) * HEAD_DIM ** (-0.5)
                scores = jnp.where(keep, scores, masked_score)
                sink = sink_ref[2 * pair + side]
                top = jnp.maximum(jnp.max(scores, axis=1, keepdims=True), sink)
                raised = jnp.exp(scores - top)
                total = jnp.sum(raised, axis=1, keepdims=True) + jnp.exp(sink - top)
                probs = (raised * (1.0 / total)).astype(BF16)
                attended += jnp.dot(probs, band_ref[2 + side, band], preferred_element_type=F32)
            hidden_ref[b * WINDOW : (b + 1) * WINDOW, pair * PAIR : (pair + 1) * PAIR] = (
                attended.astype(BF16)
            )

    length = chan.shape[0]
    sums = chan + pltpu.roll(chan, 1, 0)
    window_sum = sums
    for level in range(1, POOL_GROUPS):
        step = 2 ** (level - 1)
        sums = pltpu.roll(sums, step, 0) + pltpu.roll(sums, length - step, 0)
        window_sum = jnp.where(y >= level, sums, window_sum)
    half_width = jnp.left_shift(jnp.int32(1), y)
    pos = offset + lax.broadcasted_iota(jnp.int32, (rows, 1), 0)
    count = jnp.minimum(pos + half_width, seq_len) - jnp.maximum(pos - half_width, 0)
    spread = window_sum[RIM : RIM + rows] / count.astype(F32) - chan[RIM : RIM + rows]
    pooled = jnp.dot(spread.astype(BF16), w_pool_ref[0], preferred_element_type=F32)
    hidden_ref[:, query_cols:] = (pooled * scale_ref[...]).astype(BF16)

    def place(at, block):
        w_ref[pl.ds(at, block.shape[0]), :] = block

    in_stored_order(place, own_ref, other_ref, 0, own_ref.shape[1])
    share = sent_ref.shape[2]
    near_mask, far_mask = (1, 3) if half == 0 else (3, 1)
    hidden = hidden_ref[...]
    for ref, slot, mask in (
        (sent_ref, 0, near_mask),
        (sent_ref, 1, 2),
        (kept_ref, 0, 0),
        (kept_ref, 1, far_mask),
    ):
        columns = w_ref[pl.ds(pl.multiple_of((y ^ mask) * share, share), share)]
        ref[slot] = lax.dot_general(hidden, columns, nt, preferred_element_type=F32).astype(BF16)


VMEM = pl.BlockSpec(memory_space=pltpu.VMEM)
SMEM = pl.BlockSpec(memory_space=pltpu.SMEM)
LIMIT = pltpu.CompilerParams(vmem_limit_bytes=48 * 1024 * 1024)


def layer(
    tokens,
    w_query,
    w_key,
    w_value,
    w_pool_in,
    sink,
    w_pool,
    pool_scale,
    w_out_attn,
    w_out_pool,
    out_gain,
):
    rows = tokens.shape[0]
    seq_len = rows * lax.axis_size(SP)
    query_cols, key_cols, chan_cols = w_query.shape[1], w_key.shape[1], w_pool_in.shape[1]
    widths = (query_cols, 2 * key_cols, chan_cols)
    in_cols = sum(widths)
    hidden_cols = query_cols + chan_cols
    share = out_gain.shape[0]
    model_width = share * lax.axis_size(TP)

    gathered = from_everyone(tokens, TP)
    packed = jnp.concatenate(
        (w_query, w_key, w_value, w_pool_in, w_out_attn.T, w_out_pool.T), axis=1
    )
    over_z = lax.all_gather(packed, Z, axis=0)

    def over_x_and_cores(part):
        own = from_everyone(part, X)
        return own, swapped(own, CORE, 1)

    in_own, in_other = over_x_and_cores(over_z[:, :, :in_cols])
    out_own, out_other = over_x_and_cores(over_z[:, :, in_cols:])

    rim_shape = jax.ShapeDtypeStruct((WINDOW + 2 * RIM, PAIR), BF16)
    query, kv, chan, head, tail = pl.pallas_call(
        functools.partial(project_kernel, widths),
        out_shape=[jax.ShapeDtypeStruct((rows, w), BF16) for w in widths] + [rim_shape] * 2,
        in_specs=[VMEM] * 3,
        out_specs=[VMEM] * 5,
        scratch_shapes=[pltpu.VMEM((model_width, in_cols), BF16)],
        compiler_params=LIMIT,
        cost_estimate=pl.CostEstimate(
            flops=2 * rows * model_width * in_cols, bytes_accessed=6 << 20, transcendentals=0
        ),
        name="project",
    )(gathered, in_own, in_other)
    rims = neighbours(head, tail, SP)

    def mixed_half(half):
        block = jax.ShapeDtypeStruct((2, rows // 2, share), BF16)
        return pl.pallas_call(
            functools.partial(mix_kernel, half, seq_len),
            out_shape=[block, block],
            in_specs=[VMEM] * 4 + [SMEM] + [VMEM] * 4,
            out_specs=[VMEM] * 2,
            scratch_shapes=[
                pltpu.VMEM((4, rows // 2 + 2 * WINDOW, PAIR), BF16),
                pltpu.VMEM((rows // 2, hidden_cols), BF16),
                pltpu.VMEM((model_width, hidden_cols), BF16),
            ],
            compiler_params=LIMIT,
            cost_estimate=pl.CostEstimate(
                flops=rows * model_width * hidden_cols,
                bytes_accessed=6 << 20,
                transcendentals=0,
            ),
        )(query, kv, chan, rims[half], sink, w_pool, pool_scale.reshape(1, -1), out_own, out_other)

    def summed(half):
        near_mask, far_mask = (1, 3) if half == 0 else (3, 1)
        sent, kept = mixed_half(half)
        came = swapped(sent, TP, near_mask)
        both = kept.astype(F32) + came.astype(F32)
        rest = swapped(both[1].astype(BF16), TP, far_mask)
        return both[0] + rest.astype(F32)

    mix = jnp.concatenate([summed(0), summed(1)])
    stats = jnp.stack([jnp.sum(mix, axis=1), jnp.sum(mix * mix, axis=1)])
    stats = of_everyone(stats, TP)
    row_mean = stats[0] / model_width
    variance = stats[1] / model_width - row_mean * row_mean
    normed = (mix - row_mean[:, None]) * lax.rsqrt(variance + epsilon)[:, None] * out_gain
    return normed.astype(BF16)


def solution(mesh):
    finer = Mesh(mesh.devices.reshape(16, 4, 2, mesh.shape["tp"]), ("sp_0", "sp_1", "sp_2", "tp"))
    return jax.shard_map(
        layer,
        mesh=finer,
        in_specs=(
            P(SP, "tp"),
            P(SP, "tp"),
            P(SP, "tp"),
            P(SP, "tp"),
            P(SP, "tp"),
            P("tp"),
            P("tp", None, None),
            P("tp"),
            P("tp", SP),
            P("tp", SP),
            P("tp"),
        ),
        out_specs=P(SP, "tp"),
        check_vma=False,
    )
```

```python
import functools

import jax
import jax.numpy as jnp
from jax import lax
from jax.experimental import pallas as pl
from jax.experimental.pallas import tpu as pltpu
from jax.sharding import Mesh
from jax.sharding import PartitionSpec as P


HEAD_DIM = 64
PAIR = 2 * HEAD_DIM
POOL_GROUPS = 4
RIM = 2 ** (POOL_GROUPS - 1)
WINDOW = 128
SP = ("sp_0", "sp_1", "sp_2")
Z, X, CORE = SP
TP = "tp"
BF16, F32 = jnp.bfloat16, jnp.float32

epsilon = 1e-05
masked_score = -1e30
nt = (((1,), (1,)), ((), ()))


def from_everyone(shard, axis):
    count = lax.axis_size(axis)
    return lax.all_to_all(
        jnp.broadcast_to(shard[None], (count, *shard.shape)), axis, 0, 0, tiled=True
    )


def of_everyone(shard, axis):
    return jnp.sum(from_everyone(shard, axis), axis=0)


def swapped(shard, axis, mask):
    return lax.ppermute(shard, axis, [(i, i ^ mask) for i in range(lax.axis_size(axis))])


def neighbours(head, tail, axis):
    count = lax.axis_size(axis)
    before = lax.ppermute(tail, axis, [(i, i + 1) for i in range(count - 1)])
    after = lax.ppermute(head, axis, [(i + 1, i) for i in range(count - 1)])
    return before, after


def in_stored_order(place, own_ref, other_ref, count):
    core = lax.axis_index(CORE)
    xs, rows = own_ref.shape[0], own_ref.shape[2]
    for z in range(count):
        for x in range(xs):
            base = (z * xs + x) * 2 * rows
            place(pl.multiple_of(base + core * rows, rows), own_ref[x, z])
            place(pl.multiple_of(base + (1 - core) * rows, rows), other_ref[x, z])


def whole_weights(own_ref, other_ref, w_ref, at):
    def place(row, block):
        w_ref[pl.ds(row, block.shape[0]), :] = block[:, at : at + w_ref.shape[1]]

    in_stored_order(place, own_ref, other_ref, own_ref.shape[1])


def side_by_side(tokens_ref, rows_ref):
    depth = tokens_ref.shape[2]
    for p in range(tokens_ref.shape[0]):
        rows_ref[:, p * depth : (p + 1) * depth] = tokens_ref[p]


def project_kernel(
    tokens_ref, own_ref, other_ref, kv_ref, chan_ref, head_ref, tail_ref, rows_ref, w_ref
):
    rows = tokens_ref.shape[1]
    whole_weights(own_ref, other_ref, w_ref, 0)
    side_by_side(tokens_ref, rows_ref)
    at = 0
    for ref in (kv_ref, chan_ref):
        width = ref.shape[1]
        ref[...] = jnp.dot(
            rows_ref[...], w_ref[:, at : at + width], preferred_element_type=F32
        ).astype(BF16)
        at += width
    for ref, kv_at, chan_at in ((head_ref, 0, 0), (tail_ref, rows - WINDOW, rows - RIM)):
        ref[:WINDOW] = kv_ref[kv_at : kv_at + WINDOW]
        edge = chan_ref[chan_at : chan_at + RIM].astype(F32)
        ref[WINDOW:] = jnp.concatenate([edge[:, :PAIR], edge[:, PAIR:]]).astype(BF16)


def pool_kernel(seq_len, chan_ref, before_ref, after_ref, w_pool_ref, scale_ref, pooled_ref):
    rows = chan_ref.shape[0]
    y = lax.axis_index(TP)
    offset = lax.axis_index(SP) * rows

    def rim(ref):
        packed = ref[WINDOW:].astype(F32)
        return jnp.concatenate([packed[:RIM], packed[RIM:]], axis=1)

    own = chan_ref[...].astype(F32)
    chan = jnp.concatenate([rim(before_ref), own, rim(after_ref)])
    length = chan.shape[0]
    sums = chan + pltpu.roll(chan, 1, 0)
    window_sum = sums
    for level in range(1, POOL_GROUPS):
        step = 2 ** (level - 1)
        sums = pltpu.roll(sums, step, 0) + pltpu.roll(sums, length - step, 0)
        window_sum = jnp.where(y >= level, sums, window_sum)
    half_width = jnp.left_shift(jnp.int32(1), y)
    pos = offset + lax.broadcasted_iota(jnp.int32, (rows, 1), 0)
    count = jnp.minimum(pos + half_width, seq_len) - jnp.maximum(pos - half_width, 0)
    spread = window_sum[RIM : RIM + rows] / count.astype(F32) - own
    pooled = jnp.dot(spread.astype(BF16), w_pool_ref[0], preferred_element_type=F32)
    pooled_ref[...] = (pooled * scale_ref[...]).astype(BF16)


def mix_kernel(
    seq_len,
    tokens_ref,
    kv_ref,
    before_ref,
    after_ref,
    pooled_ref,
    sink_ref,
    own_ref,
    other_ref,
    sent0_ref,
    sent1_ref,
    kept0_ref,
    kept1_ref,
    rows_ref,
    query_ref,
    band_ref,
    hidden_ref,
    w_query_ref,
    w_out_ref,
):
    rows, query_cols = query_ref.shape
    y = lax.axis_index(TP)
    offset = lax.axis_index(SP) * rows

    whole_weights(own_ref, other_ref, w_query_ref, 0)
    side_by_side(tokens_ref, rows_ref)
    query_ref[...] = jnp.dot(
        rows_ref[...], w_query_ref[...], preferred_element_type=F32
    ).astype(BF16)
    whole_weights(own_ref, other_ref, w_out_ref, query_cols)

    kv = jnp.concatenate([before_ref[:WINDOW], kv_ref[...], after_ref[:WINDOW]]).astype(F32)
    turned = pltpu.roll(kv, HEAD_DIM, 1)
    low = lax.broadcasted_iota(jnp.int32, kv.shape, 1) < HEAD_DIM
    band_ref[0] = jnp.where(low, kv, 0.0).astype(BF16)
    band_ref[1] = jnp.where(low, 0.0, turned).astype(BF16)
    band_ref[2] = jnp.where(low, turned, 0.0).astype(BF16)
    band_ref[3] = jnp.where(low, 0.0, kv).astype(BF16)

    row = lax.broadcasted_iota(jnp.int32, (WINDOW, 3 * WINDOW), 0)
    col = lax.broadcasted_iota(jnp.int32, (WINDOW, 3 * WINDOW), 1)
    near = (col >= row) & (col <= row + 2 * WINDOW)
    for b in range(rows // WINDOW):
        key_pos = col + (offset + (b - 1) * WINDOW)
        keep = near & (key_pos >= 0) & (key_pos < seq_len)
        here = pl.ds(b * WINDOW, WINDOW)
        band = pl.ds(b * WINDOW, 3 * WINDOW)
        for pair in range(query_cols // PAIR):
            lanes = slice(pair * PAIR, (pair + 1) * PAIR)
            queries = query_ref[here, lanes]
            attended = jnp.zeros((WINDOW, PAIR), F32)
            for side in range(2):
                scores = lax.dot_general(
                    queries, band_ref[side, band], nt, preferred_element_type=F32
                ) * HEAD_DIM ** (-0.5)
                scores = jnp.where(keep, scores, masked_score)
                sink = sink_ref[2 * pair + side]
                top = jnp.maximum(jnp.max(scores, axis=1, keepdims=True), sink)
                raised = jnp.exp(scores - top)
                total = jnp.sum(raised, axis=1, keepdims=True) + jnp.exp(sink - top)
                probs = (raised * (1.0 / total)).astype(BF16)
                attended += jnp.dot(probs, band_ref[2 + side, band], preferred_element_type=F32)
            hidden_ref[here, lanes] = attended.astype(BF16)
    hidden_ref[:, query_cols:] = pooled_ref[...]

    half, share = sent0_ref.shape[1:]
    for at, sent_ref, kept_ref, near_mask, far_mask in (
        (0, sent0_ref, kept0_ref, 1, 3),
        (half, sent1_ref, kept1_ref, 3, 1),
    ):
        hidden = hidden_ref[at : at + half]
        for ref, slot, mask in (
            (sent_ref, 0, near_mask),
            (sent_ref, 1, 2),
            (kept_ref, 0, 0),
            (kept_ref, 1, far_mask),
        ):
            columns = w_out_ref[pl.ds(pl.multiple_of((y ^ mask) * share, share), share)]
            ref[slot] = lax.dot_general(
                hidden, columns, nt, preferred_element_type=F32
            ).astype(BF16)


VMEM = pl.BlockSpec(memory_space=pltpu.VMEM)
SMEM = pl.BlockSpec(memory_space=pltpu.SMEM)
LIMIT = pltpu.CompilerParams(vmem_limit_bytes=20 * 1024 * 1024)


def layer(
    tokens,
    w_query,
    w_key,
    w_value,
    w_pool_in,
    sink,
    w_pool,
    pool_scale,
    w_out_attn,
    w_out_pool,
    out_gain,
):
    rows = tokens.shape[0]
    seq_len = rows * lax.axis_size(SP)
    query_cols, key_cols, chan_cols = w_query.shape[1], w_key.shape[1], w_pool_in.shape[1]
    first_cols = 2 * key_cols + chan_cols
    hidden_cols = query_cols + chan_cols
    share = out_gain.shape[0]
    model_width = share * lax.axis_size(TP)

    gathered = from_everyone(tokens, TP)
    packed = jnp.concatenate(
        (w_key, w_value, w_pool_in, w_query, w_out_attn.T, w_out_pool.T), axis=1
    )
    over_z = lax.all_gather(packed, Z, axis=0)

    def over_x_and_cores(part):
        own = from_everyone(part, X)
        return own, swapped(own, CORE, 1)

    own1, other1 = over_x_and_cores(over_z[:, :, :first_cols])
    own2, other2 = over_x_and_cores(over_z[:, :, first_cols:])

    def rows_of(width):
        return jax.ShapeDtypeStruct((rows, width), BF16)

    def cost(flops, size):
        return pl.CostEstimate(flops=flops, bytes_accessed=size, transcendentals=0)

    rim_shape = jax.ShapeDtypeStruct((WINDOW + 2 * RIM, PAIR), BF16)
    kv, chan, head, tail = pl.pallas_call(
        project_kernel,
        out_shape=[rows_of(2 * key_cols), rows_of(chan_cols), rim_shape, rim_shape],
        in_specs=[VMEM] * 3,
        out_specs=[VMEM] * 4,
        scratch_shapes=[
            pltpu.VMEM((rows, model_width), BF16),
            pltpu.VMEM((model_width, first_cols), BF16),
        ],
        compiler_params=LIMIT,
        cost_estimate=cost(2 * rows * model_width * first_cols, 4 << 20),
        name="project",
    )(gathered, own1, other1)
    before, after = neighbours(head, tail, SP)
    pooled = pl.pallas_call(
        functools.partial(pool_kernel, seq_len),
        out_shape=rows_of(chan_cols),
        in_specs=[VMEM] * 5,
        out_specs=VMEM,
        compiler_params=LIMIT,
        cost_estimate=cost(2 * rows * chan_cols * chan_cols, 1 << 20),
        name="pool",
    )(chan, before, after, w_pool, pool_scale.reshape(1, -1))
    block = jax.ShapeDtypeStruct((2, rows // 2, share), BF16)
    sent0, sent1, kept0, kept1 = pl.pallas_call(
        functools.partial(mix_kernel, seq_len),
        out_shape=[block] * 4,
        in_specs=[VMEM] * 5 + [SMEM] + [VMEM] * 2,
        out_specs=[VMEM] * 4,
        scratch_shapes=[
            pltpu.VMEM((rows, model_width), BF16),
            pltpu.VMEM((rows, query_cols), BF16),
            pltpu.VMEM((4, rows + 2 * WINDOW, PAIR), BF16),
            pltpu.VMEM((rows, hidden_cols), BF16),
            pltpu.VMEM((model_width, query_cols), BF16),
            pltpu.VMEM((model_width, hidden_cols), BF16),
        ],
        compiler_params=LIMIT,
        cost_estimate=cost(2 * rows * model_width * (hidden_cols + query_cols), 8 << 20),
        name="mix",
    )(gathered, kv, before, after, pooled, sink, own2, other2)

    def exchanged(sent, kept, near_mask, far_mask):
        came = swapped(sent, TP, near_mask)
        both = kept.astype(F32) + came.astype(F32)
        passed = both[1].astype(BF16)
        rest = swapped(passed, TP, far_mask)
        return both[0] + rest.astype(F32)

    mix = (exchanged(sent0, kept0, 1, 3), exchanged(sent1, kept1, 3, 1))
    mix = jnp.concatenate(mix)
    stats = jnp.stack([jnp.sum(mix, axis=1), jnp.sum(mix * mix, axis=1)])
    stats = of_everyone(stats, TP)
    row_mean = stats[0] / model_width
    variance = stats[1] / model_width - row_mean * row_mean
    normed = (mix - row_mean[:, None]) * lax.rsqrt(variance + epsilon)[:, None] * out_gain
    return normed.astype(BF16)


def solution(mesh):
    finer = Mesh(mesh.devices.reshape(16, 4, 2, mesh.shape["tp"]), ("sp_0", "sp_1", "sp_2", "tp"))
    return jax.shard_map(
        layer,
        mesh=finer,
        in_specs=(
            P(SP, "tp"),
            P(SP, "tp"),
            P(SP, "tp"),
            P(SP, "tp"),
            P(SP, "tp"),
            P("tp"),
            P("tp", None, None),
            P("tp"),
            P("tp", SP),
            P("tp", SP),
            P("tp"),
        ),
        out_specs=P(SP, "tp"),
        check_vma=False,
    )
```

```python
import functools

import jax
import jax.numpy as jnp
from jax import lax
from jax.experimental import pallas as pl
from jax.experimental.pallas import tpu as pltpu
from jax.sharding import Mesh
from jax.sharding import PartitionSpec as P


HEAD_DIM = 64
PAIR = 2 * HEAD_DIM
POOL_GROUPS = 4
RIM = 2 ** (POOL_GROUPS - 1)
WINDOW = 128
SP = ("sp_0", "sp_1", "sp_2")
Z, X, CORE = SP
TP = "tp"
BF16, F32 = jnp.bfloat16, jnp.float32

epsilon = 1e-05
masked_score = -1e30
nt = (((1,), (1,)), ((), ()))


def from_everyone(shard, axis):
    count = lax.axis_size(axis)
    return lax.all_to_all(
        jnp.broadcast_to(shard[None], (count, *shard.shape)), axis, 0, 0, tiled=True
    )


def of_everyone(shard, axis):
    return jnp.sum(from_everyone(shard, axis), axis=0)


def swapped(shard, axis, mask):
    return lax.ppermute(shard, axis, [(i, i ^ mask) for i in range(lax.axis_size(axis))])


def neighbours(head, tail, axis):
    count = lax.axis_size(axis)
    before = lax.ppermute(tail, axis, [(i, i + 1) for i in range(count - 1)])
    after = lax.ppermute(head, axis, [(i + 1, i) for i in range(count - 1)])
    return before, after


def whole_weights(own_ref, other_ref, w_ref, at):
    core = lax.axis_index(CORE)
    xs, zs, rows = own_ref.shape[:3]
    lanes = slice(at, at + w_ref.shape[1])
    for z in range(zs):
        for x in range(xs):
            base = (z * xs + x) * 2 * rows
            w_ref[pl.ds(pl.multiple_of(base + core * rows, rows), rows), :] = own_ref[
                x, z, :, lanes
            ]
            w_ref[pl.ds(pl.multiple_of(base + (1 - core) * rows, rows), rows), :] = other_ref[
                x, z, :, lanes
            ]


def projected(tokens_ref, w_ref, at, width):
    depth = tokens_ref.shape[2]
    total = None
    for p in range(tokens_ref.shape[0]):
        part = jnp.dot(
            tokens_ref[p],
            w_ref[p * depth : (p + 1) * depth, at : at + width],
            preferred_element_type=F32,
        )
        total = part if total is None else total + part
    return total.astype(BF16)


def project_kernel(tokens_ref, own_ref, other_ref, kv_ref, chan_ref, head_ref, tail_ref, w_ref):
    rows = tokens_ref.shape[1]
    whole_weights(own_ref, other_ref, w_ref, 0)
    kv_cols = kv_ref.shape[1]
    kv_ref[...] = projected(tokens_ref, w_ref, 0, kv_cols)
    chan_ref[...] = projected(tokens_ref, w_ref, kv_cols, chan_ref.shape[1])
    for ref, kv_at, chan_at in ((head_ref, 0, 0), (tail_ref, rows - WINDOW, rows - RIM)):
        ref[:WINDOW] = kv_ref[kv_at : kv_at + WINDOW]
        edge = chan_ref[chan_at : chan_at + RIM].astype(F32)
        ref[WINDOW:] = jnp.concatenate([edge[:, :PAIR], edge[:, PAIR:]]).astype(BF16)


def split_band(kv, band_ref):
    kv = kv.astype(F32)
    turned = pltpu.roll(kv, HEAD_DIM, 1)
    low = lax.broadcasted_iota(jnp.int32, kv.shape, 1) < HEAD_DIM
    band_ref[0] = jnp.where(low, kv, 0.0).astype(BF16)
    band_ref[1] = jnp.where(low, 0.0, turned).astype(BF16)
    band_ref[2] = jnp.where(low, turned, 0.0).astype(BF16)
    band_ref[3] = jnp.where(low, 0.0, kv).astype(BF16)


def attend_block(queries, first_key, edge, seq_len, band_ref, at, sink_ref, attended_ref, to):
    row = lax.broadcasted_iota(jnp.int32, (WINDOW, 3 * WINDOW), 0)
    col = lax.broadcasted_iota(jnp.int32, (WINDOW, 3 * WINDOW), 1)
    keep = (col >= row) & (col <= row + 2 * WINDOW)
    if edge:
        key_pos = col + first_key
        keep = keep & (key_pos >= 0) & (key_pos < seq_len)
    band = pl.ds(at, 3 * WINDOW)
    for pair in range(queries.shape[1] // PAIR):
        lanes = slice(pair * PAIR, (pair + 1) * PAIR)
        attended = jnp.zeros((WINDOW, PAIR), F32)
        for side in range(2):
            scores = lax.dot_general(
                queries[:, lanes], band_ref[side, band], nt, preferred_element_type=F32
            ) * HEAD_DIM ** (-0.5)
            scores = jnp.where(keep, scores, masked_score)
            sink = sink_ref[2 * pair + side]
            top = jnp.maximum(jnp.max(scores, axis=1, keepdims=True), sink)
            raised = jnp.exp(scores - top)
            total = jnp.sum(raised, axis=1, keepdims=True) + jnp.exp(sink - top)
            probs = (raised * (1.0 / total)).astype(BF16)
            attended += jnp.dot(probs, band_ref[2 + side, band], preferred_element_type=F32)
        attended_ref[to : to + WINDOW, lanes] = attended.astype(BF16)


def inner_kernel(
    seq_len,
    tokens_ref,
    own_ref,
    other_ref,
    kv_ref,
    sink_ref,
    query_ref,
    attended_ref,
    w_ref,
    band_ref,
):
    rows, query_cols = query_ref.shape
    whole_weights(own_ref, other_ref, w_ref, own_ref.shape[3] - query_cols)
    query_ref[...] = projected(tokens_ref, w_ref, 0, query_cols)
    split_band(kv_ref[...], band_ref)
    for b in range(1, rows // WINDOW - 1):
        attend_block(
            query_ref[b * WINDOW : (b + 1) * WINDOW],
            0,
            False,
            seq_len,
            band_ref,
            (b - 1) * WINDOW,
            sink_ref,
            attended_ref,
            (b - 1) * WINDOW,
        )


def outer_kernel(
    seq_len,
    query_ref,
    kv_ref,
    chan_ref,
    before_ref,
    after_ref,
    sink_ref,
    w_pool_ref,
    scale_ref,
    attended_ref,
    pooled_ref,
    band_ref,
):
    rows = chan_ref.shape[0]
    y = lax.axis_index(TP)
    offset = lax.axis_index(SP) * rows

    split_band(
        jnp.concatenate(
            [
                before_ref[:WINDOW],
                kv_ref[: 2 * WINDOW],
                kv_ref[rows - 2 * WINDOW :],
                after_ref[:WINDOW],
            ]
        ),
        band_ref,
    )
    for edge, start in enumerate((0, rows - WINDOW)):
        attend_block(
            query_ref[start : start + WINDOW],
            offset + start - WINDOW,
            True,
            seq_len,
            band_ref,
            edge * 3 * WINDOW,
            sink_ref,
            attended_ref,
            edge * WINDOW,
        )

    def rim(ref):
        packed = ref[WINDOW:].astype(F32)
        return jnp.concatenate([packed[:RIM], packed[RIM:]], axis=1)

    own = chan_ref[...].astype(F32)
    chan = jnp.concatenate([rim(before_ref), own, rim(after_ref)])
    length = chan.shape[0]
    sums = chan + pltpu.roll(chan, 1, 0)
    window_sum = sums
    for level in range(1, POOL_GROUPS):
        step = 2 ** (level - 1)
        sums = pltpu.roll(sums, step, 0) + pltpu.roll(sums, length - step, 0)
        window_sum = jnp.where(y >= level, sums, window_sum)
    half_width = jnp.left_shift(jnp.int32(1), y)
    pos = offset + lax.broadcasted_iota(jnp.int32, (rows, 1), 0)
    count = jnp.minimum(pos + half_width, seq_len) - jnp.maximum(pos - half_width, 0)
    spread = window_sum[RIM : RIM + rows] / count.astype(F32) - own
    pooled = jnp.dot(spread.astype(BF16), w_pool_ref[0], preferred_element_type=F32)
    pooled_ref[...] = (pooled * scale_ref[...]).astype(BF16)


def out_kernel(blocks, attended_refs, pooled_ref, own_ref, other_ref, out_refs, hidden_ref, w_ref):
    y = lax.axis_index(TP)
    whole_weights(own_ref, other_ref, w_ref, 0)
    _, query_cols = attended_refs[0].shape
    share = out_refs[0].shape[2]
    for half, attended_ref in zip(sorted({half for half, _ in sum(blocks, ())}), attended_refs):
        hidden_ref[:, :query_cols] = attended_ref[...]
        if half == 0:
            hidden_ref[:, query_cols:] = pooled_ref[WINDOW:-WINDOW]
        else:
            hidden_ref[:WINDOW, query_cols:] = pooled_ref[:WINDOW]
            hidden_ref[WINDOW:, query_cols:] = pooled_ref[pooled_ref.shape[0] - WINDOW :]
        for ref, slots in zip(out_refs, blocks):
            for slot, (of_half, mask) in enumerate(slots):
                if of_half == half:
                    columns = w_ref[pl.ds(pl.multiple_of((y ^ mask) * share, share), share)]
                    ref[slot] = lax.dot_general(
                        hidden_ref[...], columns, nt, preferred_element_type=F32
                    ).astype(BF16)


VMEM = pl.BlockSpec(memory_space=pltpu.VMEM)
SMEM = pl.BlockSpec(memory_space=pltpu.SMEM)
LIMIT = pltpu.CompilerParams(vmem_limit_bytes=20 * 1024 * 1024)


def layer(
    tokens,
    w_query,
    w_key,
    w_value,
    w_pool_in,
    sink,
    w_pool,
    pool_scale,
    w_out_attn,
    w_out_pool,
    out_gain,
):
    rows = tokens.shape[0]
    seq_len = rows * lax.axis_size(SP)
    query_cols, key_cols, chan_cols = w_query.shape[1], w_key.shape[1], w_pool_in.shape[1]
    in_cols = 2 * key_cols + chan_cols + query_cols
    hidden_cols = query_cols + chan_cols
    share = out_gain.shape[0]
    model_width = share * lax.axis_size(TP)

    gathered = from_everyone(tokens, TP)
    packed = jnp.concatenate(
        (w_key, w_value, w_pool_in, w_query, w_out_attn.T, w_out_pool.T), axis=1
    )
    over_z = lax.all_gather(packed, Z, axis=0)
    for_x = [
        jnp.broadcast_to(part[None], (lax.axis_size(X), *part.shape))
        for part in (over_z[:, :, :in_cols], over_z[:, :, in_cols:])
    ]
    for_x = lax.optimization_barrier(for_x)
    own1 = lax.all_to_all(for_x[0], X, 0, 0, tiled=True)
    own2 = lax.all_to_all(for_x[1], X, 0, 0, tiled=True)
    other1 = swapped(own1, CORE, 1)
    other2 = swapped(own2, CORE, 1)

    def rows_of(width, count=rows):
        return jax.ShapeDtypeStruct((count, width), BF16)

    def cost(flops, size):
        return pl.CostEstimate(flops=flops, bytes_accessed=size, transcendentals=0)

    rim_shape = rows_of(PAIR, WINDOW + 2 * RIM)
    kv, chan, head, tail = pl.pallas_call(
        project_kernel,
        out_shape=[rows_of(2 * key_cols), rows_of(chan_cols), rim_shape, rim_shape],
        in_specs=[VMEM] * 3,
        out_specs=[VMEM] * 4,
        scratch_shapes=[pltpu.VMEM((model_width, 2 * key_cols + chan_cols), BF16)],
        compiler_params=LIMIT,
        cost_estimate=cost(2 * rows * model_width * (in_cols - query_cols), 4 << 20),
        name="project",
    )(gathered, own1, other1)
    before, after = neighbours(head, tail, SP)
    band = pltpu.VMEM((4, rows, PAIR), BF16)
    query, attended0 = pl.pallas_call(
        functools.partial(inner_kernel, seq_len),
        out_shape=[rows_of(query_cols), rows_of(query_cols, rows - 2 * WINDOW)],
        in_specs=[VMEM] * 4 + [SMEM],
        out_specs=[VMEM] * 2,
        scratch_shapes=[pltpu.VMEM((model_width, query_cols), BF16), band],
        compiler_params=LIMIT,
        cost_estimate=cost(2 * rows * model_width * query_cols, 4 << 20),
        name="inner",
    )(gathered, own1, other1, kv, sink)
    attended1, pooled = pl.pallas_call(
        functools.partial(outer_kernel, seq_len),
        out_shape=[rows_of(query_cols, 2 * WINDOW), rows_of(chan_cols)],
        in_specs=[VMEM] * 5 + [SMEM] + [VMEM] * 2,
        out_specs=[VMEM] * 2,
        scratch_shapes=[pltpu.VMEM((4, 6 * WINDOW, PAIR), BF16)],
        compiler_params=LIMIT,
        cost_estimate=cost(2 * rows * model_width * query_cols, 2 << 20),
        name="outer",
    )(query, kv, chan, before, after, sink, w_pool, pool_scale.reshape(1, -1))

    def multiplied(blocks, *attended):
        count = len(attended)
        outs = len(blocks)

        def kernel(*refs):
            out_kernel(
                blocks,
                refs[:count],
                *refs[count : count + 3],
                refs[count + 3 : count + 3 + outs],
                *refs[count + 3 + outs :],
            )

        return pl.pallas_call(
            kernel,
            out_shape=[jax.ShapeDtypeStruct((2, rows // 2, share), BF16)] * outs,
            in_specs=[VMEM] * (count + 3),
            out_specs=[VMEM] * outs,
            scratch_shapes=[
                pltpu.VMEM((rows // 2, hidden_cols), BF16),
                pltpu.VMEM((model_width, hidden_cols), BF16),
            ],
            compiler_params=LIMIT,
            cost_estimate=cost(outs * rows // 2 * model_width * hidden_cols, 4 << 20),
        )(*attended, pooled, own2, other2)

    (sent0,) = multiplied((((0, 1), (0, 2)),), attended0)
    sent1, kept0, kept1 = multiplied(
        (((1, 3), (1, 2)), ((0, 0), (0, 3)), ((1, 0), (1, 1))), attended0, attended1
    )

    def exchanged(sent, kept, near_mask, far_mask):
        came = swapped(sent, TP, near_mask)
        both = kept.astype(F32) + came.astype(F32)
        passed = both[1].astype(BF16)
        rest = swapped(passed, TP, far_mask)
        return both[0] + rest.astype(F32)

    middle = exchanged(sent0, kept0, 1, 3)
    edges = exchanged(sent1, kept1, 3, 1)
    mix = jnp.concatenate([edges[:WINDOW], middle, edges[WINDOW:]])
    stats = jnp.stack([jnp.sum(mix, axis=1), jnp.sum(mix * mix, axis=1)])
    stats = of_everyone(stats, TP)
    row_mean = stats[0] / model_width
    variance = stats[1] / model_width - row_mean * row_mean
    normed = (mix - row_mean[:, None]) * lax.rsqrt(variance + epsilon)[:, None] * out_gain
    return normed.astype(BF16)


def solution(mesh):
    finer = Mesh(mesh.devices.reshape(16, 4, 2, mesh.shape["tp"]), ("sp_0", "sp_1", "sp_2", "tp"))
    return jax.shard_map(
        layer,
        mesh=finer,
        in_specs=(
            P(SP, "tp"),
            P(SP, "tp"),
            P(SP, "tp"),
            P(SP, "tp"),
            P(SP, "tp"),
            P("tp"),
            P("tp", None, None),
            P("tp"),
            P("tp", SP),
            P("tp", SP),
            P("tp"),
        ),
        out_specs=P(SP, "tp"),
        check_vma=False,
    )
```

```python
import functools

import jax
import jax.numpy as jnp
from jax import lax
from jax.experimental import pallas as pl
from jax.experimental.pallas import tpu as pltpu
from jax.sharding import Mesh
from jax.sharding import PartitionSpec as P


HEAD_DIM = 64
PAIR = 2 * HEAD_DIM
POOL_GROUPS = 4
RIM = 2 ** (POOL_GROUPS - 1)
WINDOW = 128
SP = ("sp_0", "sp_1", "sp_2")
Z, X, CORE = SP
TP = "tp"
BF16, F32 = jnp.bfloat16, jnp.float32

epsilon = 1e-05
masked_score = -1e30
nt = (((1,), (1,)), ((), ()))


def from_everyone(shard, axis):
    count = lax.axis_size(axis)
    return lax.all_to_all(
        jnp.broadcast_to(shard[None], (count, *shard.shape)), axis, 0, 0, tiled=True
    )


def of_everyone(shard, axis):
    return jnp.sum(from_everyone(shard, axis), axis=0)


def swapped(shard):
    return lax.ppermute(shard, CORE, [(0, 1), (1, 0)])


def neighbours(head, tail, axis):
    count = lax.axis_size(axis)
    before = lax.ppermute(tail, axis, [(i, i + 1) for i in range(count - 1)])
    after = lax.ppermute(head, axis, [(i + 1, i) for i in range(count - 1)])
    return before, after


def whole_weights(own_ref, other_ref, w_ref, at):
    core = lax.axis_index(CORE)
    xs, zs, rows = own_ref.shape[:3]
    lanes = slice(at, at + w_ref.shape[1])
    for z in range(zs):
        for x in range(xs):
            base = (z * xs + x) * 2 * rows
            w_ref[pl.ds(pl.multiple_of(base + core * rows, rows), rows), :] = own_ref[
                x, z, :, lanes
            ]
            w_ref[pl.ds(pl.multiple_of(base + (1 - core) * rows, rows), rows), :] = other_ref[
                x, z, :, lanes
            ]


def projected(tokens_ref, w_ref, at, width):
    depth = tokens_ref.shape[2]
    total = None
    for p in range(tokens_ref.shape[0]):
        part = jnp.dot(
            tokens_ref[p],
            w_ref[p * depth : (p + 1) * depth, at : at + width],
            preferred_element_type=F32,
        )
        total = part if total is None else total + part
    return total.astype(BF16)


def project_kernel(tokens_ref, own_ref, other_ref, kv_ref, chan_ref, head_ref, tail_ref, w_ref):
    rows = tokens_ref.shape[1]
    whole_weights(own_ref, other_ref, w_ref, 0)
    kv_cols = kv_ref.shape[1]
    kv_ref[...] = projected(tokens_ref, w_ref, 0, kv_cols)
    chan_ref[...] = projected(tokens_ref, w_ref, kv_cols, chan_ref.shape[1])
    for ref, kv_at, chan_at in ((head_ref, 0, 0), (tail_ref, rows - WINDOW, rows - RIM)):
        ref[:WINDOW] = kv_ref[kv_at : kv_at + WINDOW]
        edge = chan_ref[chan_at : chan_at + RIM].astype(F32)
        ref[WINDOW:] = jnp.concatenate([edge[:, :PAIR], edge[:, PAIR:]]).astype(BF16)


def split_band(kv, band_ref):
    kv = kv.astype(F32)
    turned = pltpu.roll(kv, HEAD_DIM, 1)
    low = lax.broadcasted_iota(jnp.int32, kv.shape, 1) < HEAD_DIM
    band_ref[0] = jnp.where(low, kv, 0.0).astype(BF16)
    band_ref[1] = jnp.where(low, 0.0, turned).astype(BF16)
    band_ref[2] = jnp.where(low, turned, 0.0).astype(BF16)
    band_ref[3] = jnp.where(low, 0.0, kv).astype(BF16)


def attend_block(queries, first_key, edge, seq_len, band_ref, at, sink_ref, attended_ref, to):
    row = lax.broadcasted_iota(jnp.int32, (WINDOW, 3 * WINDOW), 0)
    col = lax.broadcasted_iota(jnp.int32, (WINDOW, 3 * WINDOW), 1)
    keep = (col >= row) & (col <= row + 2 * WINDOW)
    if edge:
        key_pos = col + first_key
        keep = keep & (key_pos >= 0) & (key_pos < seq_len)
    band = pl.ds(at, 3 * WINDOW)
    for pair in range(queries.shape[1] // PAIR):
        lanes = slice(pair * PAIR, (pair + 1) * PAIR)
        attended = jnp.zeros((WINDOW, PAIR), F32)
        for side in range(2):
            scores = lax.dot_general(
                queries[:, lanes], band_ref[side, band], nt, preferred_element_type=F32
            ) * HEAD_DIM ** (-0.5)
            scores = jnp.where(keep, scores, masked_score)
            sink = sink_ref[2 * pair + side]
            top = jnp.maximum(jnp.max(scores, axis=1, keepdims=True), sink)
            raised = jnp.exp(scores - top)
            total = jnp.sum(raised, axis=1, keepdims=True) + jnp.exp(sink - top)
            probs = (raised * (1.0 / total)).astype(BF16)
            attended += jnp.dot(probs, band_ref[2 + side, band], preferred_element_type=F32)
        attended_ref[to : to + WINDOW, lanes] = attended.astype(BF16)


def inner_kernel(
    seq_len,
    tokens_ref,
    own_ref,
    other_ref,
    kv_ref,
    sink_ref,
    query_ref,
    attended_ref,
    w_ref,
    band_ref,
):
    rows, query_cols = query_ref.shape
    whole_weights(own_ref, other_ref, w_ref, own_ref.shape[3] - query_cols)
    query_ref[...] = projected(tokens_ref, w_ref, 0, query_cols)
    split_band(kv_ref[...], band_ref)
    for b in range(1, rows // WINDOW - 1):
        attend_block(
            query_ref[b * WINDOW : (b + 1) * WINDOW],
            0,
            False,
            seq_len,
            band_ref,
            (b - 1) * WINDOW,
            sink_ref,
            attended_ref,
            (b - 1) * WINDOW,
        )


def outer_kernel(
    seq_len,
    query_ref,
    kv_ref,
    chan_ref,
    before_ref,
    after_ref,
    sink_ref,
    w_pool_ref,
    scale_ref,
    attended_ref,
    pooled_ref,
    band_ref,
):
    rows = chan_ref.shape[0]
    y = lax.axis_index(TP)
    offset = lax.axis_index(SP) * rows

    split_band(
        jnp.concatenate(
            [
                before_ref[:WINDOW],
                kv_ref[: 2 * WINDOW],
                kv_ref[rows - 2 * WINDOW :],
                after_ref[:WINDOW],
            ]
        ),
        band_ref,
    )
    for edge, start in enumerate((0, rows - WINDOW)):
        attend_block(
            query_ref[start : start + WINDOW],
            offset + start - WINDOW,
            True,
            seq_len,
            band_ref,
            edge * 3 * WINDOW,
            sink_ref,
            attended_ref,
            edge * WINDOW,
        )

    def rim(ref):
        packed = ref[WINDOW:].astype(F32)
        return jnp.concatenate([packed[:RIM], packed[RIM:]], axis=1)

    own = chan_ref[...].astype(F32)
    chan = jnp.concatenate([rim(before_ref), own, rim(after_ref)])
    length = chan.shape[0]
    sums = chan + pltpu.roll(chan, 1, 0)
    window_sum = sums
    for level in range(1, POOL_GROUPS):
        step = 2 ** (level - 1)
        sums = pltpu.roll(sums, step, 0) + pltpu.roll(sums, length - step, 0)
        window_sum = jnp.where(y >= level, sums, window_sum)
    half_width = jnp.left_shift(jnp.int32(1), y)
    pos = offset + lax.broadcasted_iota(jnp.int32, (rows, 1), 0)
    count = jnp.minimum(pos + half_width, seq_len) - jnp.maximum(pos - half_width, 0)
    spread = window_sum[RIM : RIM + rows] / count.astype(F32) - own
    pooled = jnp.dot(spread.astype(BF16), w_pool_ref[0], preferred_element_type=F32)
    pooled_ref[...] = (pooled * scale_ref[...]).astype(BF16)


def out_kernel(
    ahead, first_ref, middle_ref, pooled_ref, own_ref, other_ref, out_ref, hidden_ref, w_ref
):
    edge = WINDOW
    rows, query_cols = pooled_ref.shape[0], first_ref.shape[1]
    to = lax.rem(lax.axis_index(TP) + ahead, lax.axis_size(TP))
    zs = own_ref.shape[1] // lax.axis_size(TP)
    at = own_ref.shape[3] - hidden_ref.shape[1]
    mine = pl.ds(to * zs, zs)
    whole_weights(own_ref.at[:, mine], other_ref.at[:, mine], w_ref, at)
    hidden_ref[:edge, :query_cols] = first_ref[:edge]
    hidden_ref[edge : rows - edge, :query_cols] = middle_ref[...]
    hidden_ref[rows - edge :, :query_cols] = first_ref[edge:]
    hidden_ref[:, query_cols:] = pooled_ref[...]
    out_ref[...] = lax.dot_general(
        hidden_ref[...], w_ref[...], nt, preferred_element_type=F32
    ).astype(BF16)


VMEM = pl.BlockSpec(memory_space=pltpu.VMEM)
SMEM = pl.BlockSpec(memory_space=pltpu.SMEM)
LIMIT = pltpu.CompilerParams(vmem_limit_bytes=20 * 1024 * 1024)


def layer(
    tokens,
    w_query,
    w_key,
    w_value,
    w_pool_in,
    sink,
    w_pool,
    pool_scale,
    w_out_attn,
    w_out_pool,
    out_gain,
):
    rows = tokens.shape[0]
    seq_len = rows * lax.axis_size(SP)
    query_cols, key_cols, chan_cols = w_query.shape[1], w_key.shape[1], w_pool_in.shape[1]
    in_cols = 2 * key_cols + chan_cols + query_cols
    hidden_cols = query_cols + chan_cols
    share = out_gain.shape[0]
    model_width = share * lax.axis_size(TP)

    gathered = from_everyone(tokens, TP)
    packed = jnp.concatenate(
        (w_key, w_value, w_pool_in, w_query, w_out_attn.T, w_out_pool.T), axis=1
    )
    over_z = lax.all_gather(packed, Z, axis=0)
    over_x = from_everyone(over_z, X)
    own1, own2 = over_x[..., :in_cols], over_x[..., in_cols:]
    other1 = swapped(own1)
    other2 = swapped(own2)

    def rows_of(width, count=rows):
        return jax.ShapeDtypeStruct((count, width), BF16)

    def cost(flops, size):
        return pl.CostEstimate(flops=flops, bytes_accessed=size, transcendentals=0)

    rim_shape = rows_of(PAIR, WINDOW + 2 * RIM)
    kv, chan, head, tail = pl.pallas_call(
        project_kernel,
        out_shape=[rows_of(2 * key_cols), rows_of(chan_cols), rim_shape, rim_shape],
        in_specs=[VMEM] * 3,
        out_specs=[VMEM] * 4,
        scratch_shapes=[pltpu.VMEM((model_width, 2 * key_cols + chan_cols), BF16)],
        compiler_params=LIMIT,
        cost_estimate=cost(2 * rows * model_width * (in_cols - query_cols), 4 << 20),
        name="project",
    )(gathered, own1, other1)
    before, after = neighbours(head, tail, SP)
    band = pltpu.VMEM((4, rows, PAIR), BF16)
    query, attended0 = pl.pallas_call(
        functools.partial(inner_kernel, seq_len),
        out_shape=[rows_of(query_cols), rows_of(query_cols, rows - 2 * WINDOW)],
        in_specs=[VMEM] * 4 + [SMEM],
        out_specs=[VMEM] * 2,
        scratch_shapes=[pltpu.VMEM((model_width, query_cols), BF16), band],
        compiler_params=LIMIT,
        cost_estimate=cost(2 * rows * model_width * query_cols, 4 << 20),
        name="inner",
    )(gathered, own1, other1, kv, sink)
    attended1, pooled = pl.pallas_call(
        functools.partial(outer_kernel, seq_len),
        out_shape=[rows_of(query_cols, 2 * WINDOW), rows_of(chan_cols)],
        in_specs=[VMEM] * 5 + [SMEM] + [VMEM] * 2,
        out_specs=[VMEM] * 2,
        scratch_shapes=[pltpu.VMEM((4, 6 * WINDOW, PAIR), BF16)],
        compiler_params=LIMIT,
        cost_estimate=cost(2 * rows * model_width * query_cols, 2 << 20),
        name="outer",
    )(query, kv, chan, before, after, sink, w_pool, pool_scale.reshape(1, -1))

    def multiplied(ahead):
        return pl.pallas_call(
            functools.partial(out_kernel, ahead),
            out_shape=rows_of(share),
            in_specs=[VMEM] * 5,
            out_specs=VMEM,
            scratch_shapes=[
                pltpu.VMEM((rows, hidden_cols), BF16),
                pltpu.VMEM((share, hidden_cols), BF16),
            ],
            compiler_params=LIMIT,
            cost_estimate=cost(2 * rows * share * hidden_cols, 1 << 20),
        )(attended1, attended0, pooled, own2, other2)

    count = lax.axis_size(TP)
    partials = []
    for ahead in (2, 1, 3):
        block = multiplied(ahead)
        perm = [(i, (i + ahead) % count) for i in range(count)]
        partials.append(lax.ppermute(block, TP, perm))
    mix = multiplied(0).astype(F32)
    for partial in partials[1:] + partials[:1]:
        mix = mix + partial.astype(F32)
    stats = jnp.stack([jnp.sum(mix, axis=1), jnp.sum(mix * mix, axis=1)])
    stats = of_everyone(stats, TP)
    row_mean = stats[0] / model_width
    variance = stats[1] / model_width - row_mean * row_mean
    normed = (mix - row_mean[:, None]) * lax.rsqrt(variance + epsilon)[:, None] * out_gain
    return normed.astype(BF16)


def solution(mesh):
    finer = Mesh(mesh.devices.reshape(16, 4, 2, mesh.shape["tp"]), ("sp_0", "sp_1", "sp_2", "tp"))
    return jax.shard_map(
        layer,
        mesh=finer,
        in_specs=(
            P(SP, "tp"),
            P(SP, "tp"),
            P(SP, "tp"),
            P(SP, "tp"),
            P(SP, "tp"),
            P("tp"),
            P("tp", None, None),
            P("tp"),
            P("tp", SP),
            P("tp", SP),
            P("tp"),
        ),
        out_specs=P(SP, "tp"),
        check_vma=False,
    )
```

```python
import functools

import jax
import jax.numpy as jnp
from jax import lax
from jax.experimental import pallas as pl
from jax.experimental.pallas import tpu as pltpu
from jax.sharding import Mesh
from jax.sharding import PartitionSpec as P


HEAD_DIM = 64
PAIR = 2 * HEAD_DIM
POOL_GROUPS = 4
RIM = 2 ** (POOL_GROUPS - 1)
WINDOW = 128
SP = ("sp_0", "sp_1", "sp_2")
Z, X, CORE = SP
TP = "tp"
BF16, F32 = jnp.bfloat16, jnp.float32

epsilon = 1e-05
masked_score = -1e30
BACK = (0, 2, 1, 3)
nt = (((1,), (1,)), ((), ()))


def from_everyone(shard, axis):
    count = lax.axis_size(axis)
    return lax.all_to_all(
        jnp.broadcast_to(shard[None], (count, *shard.shape)), axis, 0, 0, tiled=True
    )


def of_everyone(shard, axis):
    return jnp.sum(from_everyone(shard, axis), axis=0)


def ahead_by(shard, axis, places):
    count = lax.axis_size(axis)
    return lax.ppermute(shard, axis, [(i, (i + places) % count) for i in range(count)])


def swapped(shard):
    return lax.ppermute(shard, CORE, [(0, 1), (1, 0)])


def neighbours(head, tail, axis):
    count = lax.axis_size(axis)
    before = lax.ppermute(tail, axis, [(i, i + 1) for i in range(count - 1)])
    after = lax.ppermute(head, axis, [(i + 1, i) for i in range(count - 1)])
    return before, after


def whole_weights(own_ref, other_ref, w_ref, at):
    core, x = lax.axis_index(CORE), lax.axis_index(X)
    xs, zs, rows = own_ref.shape[:3]
    lanes = slice(at, at + w_ref.shape[1])
    for slot, back in enumerate(BACK):
        source = lax.rem(x + xs - back, xs)
        for z in range(zs):
            base = (z * xs + source) * 2 * rows
            w_ref[pl.ds(pl.multiple_of(base + core * rows, rows), rows), :] = own_ref[
                slot, z, :, lanes
            ]
            w_ref[pl.ds(pl.multiple_of(base + (1 - core) * rows, rows), rows), :] = other_ref[
                slot, z, :, lanes
            ]


def projected(tokens_ref, w_ref, at, width):
    depth = tokens_ref.shape[2]
    total = None
    for p in range(tokens_ref.shape[0]):
        part = jnp.dot(
            tokens_ref[p],
            w_ref[p * depth : (p + 1) * depth, at : at + width],
            preferred_element_type=F32,
        )
        total = part if total is None else total + part
    return total.astype(BF16)


def project_kernel(tokens_ref, own_ref, other_ref, kv_ref, chan_ref, head_ref, tail_ref, w_ref):
    rows = tokens_ref.shape[1]
    whole_weights(own_ref, other_ref, w_ref, 0)
    kv_cols = kv_ref.shape[1]
    kv_ref[...] = projected(tokens_ref, w_ref, 0, kv_cols)
    chan_ref[...] = projected(tokens_ref, w_ref, kv_cols, chan_ref.shape[1])
    for ref, kv_at, chan_at in ((head_ref, 0, 0), (tail_ref, rows - WINDOW, rows - RIM)):
        ref[:WINDOW] = kv_ref[kv_at : kv_at + WINDOW]
        edge = chan_ref[chan_at : chan_at + RIM].astype(F32)
        ref[WINDOW:] = jnp.concatenate([edge[:, :PAIR], edge[:, PAIR:]]).astype(BF16)


def split_band(kv, band_ref):
    kv = kv.astype(F32)
    turned = pltpu.roll(kv, HEAD_DIM, 1)
    low = lax.broadcasted_iota(jnp.int32, kv.shape, 1) < HEAD_DIM
    band_ref[0] = jnp.where(low, kv, 0.0).astype(BF16)
    band_ref[1] = jnp.where(low, 0.0, turned).astype(BF16)
    band_ref[2] = jnp.where(low, turned, 0.0).astype(BF16)
    band_ref[3] = jnp.where(low, 0.0, kv).astype(BF16)


def attend_block(queries, first_key, edge, seq_len, band_ref, at, sink_ref, attended_ref, to):
    row = lax.broadcasted_iota(jnp.int32, (WINDOW, 3 * WINDOW), 0)
    col = lax.broadcasted_iota(jnp.int32, (WINDOW, 3 * WINDOW), 1)
    keep = (col >= row) & (col <= row + 2 * WINDOW)
    if edge:
        key_pos = col + first_key
        keep = keep & (key_pos >= 0) & (key_pos < seq_len)
    band = pl.ds(at, 3 * WINDOW)
    for pair in range(queries.shape[1] // PAIR):
        lanes = slice(pair * PAIR, (pair + 1) * PAIR)
        attended = jnp.zeros((WINDOW, PAIR), F32)
        for side in range(2):
            scores = lax.dot_general(
                queries[:, lanes], band_ref[side, band], nt, preferred_element_type=F32
            ) * HEAD_DIM ** (-0.5)
            scores = jnp.where(keep, scores, masked_score)
            sink = sink_ref[2 * pair + side]
            top = jnp.maximum(jnp.max(scores, axis=1, keepdims=True), sink)
            raised = jnp.exp(scores - top)
            total = jnp.sum(raised, axis=1, keepdims=True) + jnp.exp(sink - top)
            probs = (raised * (1.0 / total)).astype(BF16)
            attended += jnp.dot(probs, band_ref[2 + side, band], preferred_element_type=F32)
        attended_ref[to : to + WINDOW, lanes] = attended.astype(BF16)


def inner_kernel(
    seq_len,
    tokens_ref,
    own_ref,
    other_ref,
    kv_ref,
    sink_ref,
    query_ref,
    attended_ref,
    w_ref,
    band_ref,
):
    rows, query_cols = query_ref.shape
    whole_weights(own_ref, other_ref, w_ref, own_ref.shape[3] - query_cols)
    query_ref[...] = projected(tokens_ref, w_ref, 0, query_cols)
    split_band(kv_ref[...], band_ref)
    for b in range(1, rows // WINDOW - 1):
        attend_block(
            query_ref[b * WINDOW : (b + 1) * WINDOW],
            0,
            False,
            seq_len,
            band_ref,
            (b - 1) * WINDOW,
            sink_ref,
            attended_ref,
            (b - 1) * WINDOW,
        )


def outer_kernel(
    seq_len,
    query_ref,
    kv_ref,
    chan_ref,
    before_ref,
    after_ref,
    sink_ref,
    w_pool_ref,
    scale_ref,
    attended_ref,
    pooled_ref,
    band_ref,
):
    rows = chan_ref.shape[0]
    y = lax.axis_index(TP)
    offset = lax.axis_index(SP) * rows

    split_band(
        jnp.concatenate(
            [
                before_ref[:WINDOW],
                kv_ref[: 2 * WINDOW],
                kv_ref[rows - 2 * WINDOW :],
                after_ref[:WINDOW],
            ]
        ),
        band_ref,
    )
    for edge, start in enumerate((0, rows - WINDOW)):
        attend_block(
            query_ref[start : start + WINDOW],
            offset + start - WINDOW,
            True,
            seq_len,
            band_ref,
            edge * 3 * WINDOW,
            sink_ref,
            attended_ref,
            edge * WINDOW,
        )

    def rim(ref):
        packed = ref[WINDOW:].astype(F32)
        return jnp.concatenate([packed[:RIM], packed[RIM:]], axis=1)

    own = chan_ref[...].astype(F32)
    chan = jnp.concatenate([rim(before_ref), own, rim(after_ref)])
    length = chan.shape[0]
    sums = chan + pltpu.roll(chan, 1, 0)
    window_sum = sums
    for level in range(1, POOL_GROUPS):
        step = 2 ** (level - 1)
        sums = pltpu.roll(sums, step, 0) + pltpu.roll(sums, length - step, 0)
        window_sum = jnp.where(y >= level, sums, window_sum)
    half_width = jnp.left_shift(jnp.int32(1), y)
    pos = offset + lax.broadcasted_iota(jnp.int32, (rows, 1), 0)
    count = jnp.minimum(pos + half_width, seq_len) - jnp.maximum(pos - half_width, 0)
    spread = window_sum[RIM : RIM + rows] / count.astype(F32) - own
    pooled = jnp.dot(spread.astype(BF16), w_pool_ref[0], preferred_element_type=F32)
    pooled_ref[...] = (pooled * scale_ref[...]).astype(BF16)


def out_kernel(
    ahead, first_ref, middle_ref, pooled_ref, own_ref, other_ref, out_ref, hidden_ref, w_ref
):
    edge = WINDOW
    rows, query_cols = pooled_ref.shape[0], first_ref.shape[1]
    to = lax.rem(lax.axis_index(TP) + ahead, lax.axis_size(TP))
    zs = own_ref.shape[1] // lax.axis_size(TP)
    at = own_ref.shape[3] - hidden_ref.shape[1]
    mine = pl.ds(to * zs, zs)
    whole_weights(own_ref.at[:, mine], other_ref.at[:, mine], w_ref, at)
    hidden_ref[:edge, :query_cols] = first_ref[:edge]
    hidden_ref[edge : rows - edge, :query_cols] = middle_ref[...]
    hidden_ref[rows - edge :, :query_cols] = first_ref[edge:]
    hidden_ref[:, query_cols:] = pooled_ref[...]
    out_ref[...] = lax.dot_general(
        hidden_ref[...], w_ref[...], nt, preferred_element_type=F32
    ).astype(BF16)


VMEM = pl.BlockSpec(memory_space=pltpu.VMEM)
SMEM = pl.BlockSpec(memory_space=pltpu.SMEM)
LIMIT = pltpu.CompilerParams(vmem_limit_bytes=20 * 1024 * 1024)


def layer(
    tokens,
    w_query,
    w_key,
    w_value,
    w_pool_in,
    sink,
    w_pool,
    pool_scale,
    w_out_attn,
    w_out_pool,
    out_gain,
):
    rows = tokens.shape[0]
    seq_len = rows * lax.axis_size(SP)
    query_cols, key_cols, chan_cols = w_query.shape[1], w_key.shape[1], w_pool_in.shape[1]
    in_cols = 2 * key_cols + chan_cols + query_cols
    hidden_cols = query_cols + chan_cols
    share = out_gain.shape[0]
    model_width = share * lax.axis_size(TP)

    gathered = from_everyone(tokens, TP)
    packed = jnp.concatenate(
        (w_key, w_value, w_pool_in, w_query, w_out_attn.T, w_out_pool.T), axis=1
    )
    over_z = lax.all_gather(packed, Z, axis=0)

    def gathered_over_x(part):
        pieces = [part]
        for back in BACK[1:]:
            pieces.append(ahead_by(part, X, back))
        return jnp.stack(pieces)

    own1 = gathered_over_x(over_z[..., :in_cols])
    own2 = gathered_over_x(over_z[..., in_cols:])
    other1 = swapped(own1)
    other2 = swapped(own2)

    def rows_of(width, count=rows):
        return jax.ShapeDtypeStruct((count, width), BF16)

    def cost(flops, size):
        return pl.CostEstimate(flops=flops, bytes_accessed=size, transcendentals=0)

    rim_shape = rows_of(PAIR, WINDOW + 2 * RIM)
    kv, chan, head, tail = pl.pallas_call(
        project_kernel,
        out_shape=[rows_of(2 * key_cols), rows_of(chan_cols), rim_shape, rim_shape],
        in_specs=[VMEM] * 3,
        out_specs=[VMEM] * 4,
        scratch_shapes=[pltpu.VMEM((model_width, 2 * key_cols + chan_cols), BF16)],
        compiler_params=LIMIT,
        cost_estimate=cost(2 * rows * model_width * (in_cols - query_cols), 4 << 20),
        name="project",
    )(gathered, own1, other1)
    before, after = neighbours(head, tail, SP)
    band = pltpu.VMEM((4, rows, PAIR), BF16)
    query, attended0 = pl.pallas_call(
        functools.partial(inner_kernel, seq_len),
        out_shape=[rows_of(query_cols), rows_of(query_cols, rows - 2 * WINDOW)],
        in_specs=[VMEM] * 4 + [SMEM],
        out_specs=[VMEM] * 2,
        scratch_shapes=[pltpu.VMEM((model_width, query_cols), BF16), band],
        compiler_params=LIMIT,
        cost_estimate=cost(2 * rows * model_width * query_cols, 4 << 20),
        name="inner",
    )(gathered, own1, other1, kv, sink)
    attended1, pooled = pl.pallas_call(
        functools.partial(outer_kernel, seq_len),
        out_shape=[rows_of(query_cols, 2 * WINDOW), rows_of(chan_cols)],
        in_specs=[VMEM] * 5 + [SMEM] + [VMEM] * 2,
        out_specs=[VMEM] * 2,
        scratch_shapes=[pltpu.VMEM((4, 6 * WINDOW, PAIR), BF16)],
        compiler_params=LIMIT,
        cost_estimate=cost(2 * rows * model_width * query_cols, 2 << 20),
        name="outer",
    )(query, kv, chan, before, after, sink, w_pool, pool_scale.reshape(1, -1))

    def multiplied(ahead):
        return pl.pallas_call(
            functools.partial(out_kernel, ahead),
            out_shape=rows_of(share),
            in_specs=[VMEM] * 5,
            out_specs=VMEM,
            scratch_shapes=[
                pltpu.VMEM((rows, hidden_cols), BF16),
                pltpu.VMEM((share, hidden_cols), BF16),
            ],
            compiler_params=LIMIT,
            cost_estimate=cost(2 * rows * share * hidden_cols, 1 << 20),
        )(attended1, attended0, pooled, own2, other2)

    partials = []
    for ahead in BACK[1:]:
        block = multiplied(ahead)
        partials.append(ahead_by(block, TP, ahead))
    mix = multiplied(0).astype(F32)
    for partial in partials[1:] + partials[:1]:
        mix = mix + partial.astype(F32)
    stats = jnp.stack([jnp.sum(mix, axis=1), jnp.sum(mix * mix, axis=1)])
    stats = of_everyone(stats, TP)
    row_mean = stats[0] / model_width
    variance = stats[1] / model_width - row_mean * row_mean
    normed = (mix - row_mean[:, None]) * lax.rsqrt(variance + epsilon)[:, None] * out_gain
    return normed.astype(BF16)


def solution(mesh):
    finer = Mesh(mesh.devices.reshape(16, 4, 2, mesh.shape["tp"]), ("sp_0", "sp_1", "sp_2", "tp"))
    return jax.shard_map(
        layer,
        mesh=finer,
        in_specs=(
            P(SP, "tp"),
            P(SP, "tp"),
            P(SP, "tp"),
            P(SP, "tp"),
            P(SP, "tp"),
            P("tp"),
            P("tp", None, None),
            P("tp"),
            P("tp", SP),
            P("tp", SP),
            P("tp"),
        ),
        out_specs=P(SP, "tp"),
        check_vma=False,
    )
```

```python
import functools

import jax
import jax.numpy as jnp
from jax import lax
from jax.experimental import pallas as pl
from jax.experimental.pallas import tpu as pltpu
from jax.sharding import Mesh
from jax.sharding import PartitionSpec as P


HEAD_DIM = 64
PAIR = 2 * HEAD_DIM
POOL_GROUPS = 4
RIM = 2 ** (POOL_GROUPS - 1)
WINDOW = 128
SP = ("sp_0", "sp_1", "sp_2")
Z, X, CORE = SP
TP = "tp"
BF16, F32 = jnp.bfloat16, jnp.float32

epsilon = 1e-05
masked_score = -1e30
nt = (((1,), (1,)), ((), ()))


def from_everyone(shard, axis):
    count = lax.axis_size(axis)
    return lax.all_to_all(
        jnp.broadcast_to(shard[None], (count, *shard.shape)), axis, 0, 0, tiled=True
    )


def of_everyone(shard, axis):
    return jnp.sum(from_everyone(shard, axis), axis=0)


def swapped(shard):
    return lax.ppermute(shard, CORE, [(0, 1), (1, 0)])


def neighbours(head, tail, axis):
    count = lax.axis_size(axis)
    before = lax.ppermute(tail, axis, [(i, i + 1) for i in range(count - 1)])
    after = lax.ppermute(head, axis, [(i + 1, i) for i in range(count - 1)])
    return before, after


def whole_weights(own_ref, other_ref, w_ref, at):
    core = lax.axis_index(CORE)
    xs, zs, rows = own_ref.shape[:3]
    lanes = slice(at, at + w_ref.shape[1])
    for z in range(zs):
        for x in range(xs):
            base = (z * xs + x) * 2 * rows
            w_ref[pl.ds(pl.multiple_of(base + core * rows, rows), rows), :] = own_ref[
                x, z, :, lanes
            ]
            w_ref[pl.ds(pl.multiple_of(base + (1 - core) * rows, rows), rows), :] = other_ref[
                x, z, :, lanes
            ]


def projected(tokens_ref, w_ref, at, width):
    depth = tokens_ref.shape[2]
    total = None
    for p in range(tokens_ref.shape[0]):
        part = jnp.dot(
            tokens_ref[p],
            w_ref[p * depth : (p + 1) * depth, at : at + width],
            preferred_element_type=F32,
        )
        total = part if total is None else total + part
    return total.astype(BF16)


def project_kernel(tokens_ref, own_ref, other_ref, kv_ref, chan_ref, head_ref, tail_ref, w_ref):
    rows = tokens_ref.shape[1]
    whole_weights(own_ref, other_ref, w_ref, 0)
    kv_cols = kv_ref.shape[1]
    kv_ref[...] = projected(tokens_ref, w_ref, 0, kv_cols)
    chan_ref[...] = projected(tokens_ref, w_ref, kv_cols, chan_ref.shape[1])
    for ref, kv_at, chan_at in ((head_ref, 0, 0), (tail_ref, rows - WINDOW, rows - RIM)):
        ref[:WINDOW] = kv_ref[kv_at : kv_at + WINDOW]
        edge = chan_ref[chan_at : chan_at + RIM].astype(F32)
        ref[WINDOW:] = jnp.concatenate([edge[:, :PAIR], edge[:, PAIR:]]).astype(BF16)


def split_band(kv, band_ref):
    kv = kv.astype(F32)
    turned = pltpu.roll(kv, HEAD_DIM, 1)
    low = lax.broadcasted_iota(jnp.int32, kv.shape, 1) < HEAD_DIM
    band_ref[0] = jnp.where(low, kv, 0.0).astype(BF16)
    band_ref[1] = jnp.where(low, 0.0, turned).astype(BF16)
    band_ref[2] = jnp.where(low, turned, 0.0).astype(BF16)
    band_ref[3] = jnp.where(low, 0.0, kv).astype(BF16)


def attend_block(queries, first_key, edge, seq_len, band_ref, at, sink_ref, attended_ref, to):
    row = lax.broadcasted_iota(jnp.int32, (WINDOW, 3 * WINDOW), 0)
    col = lax.broadcasted_iota(jnp.int32, (WINDOW, 3 * WINDOW), 1)
    keep = (col >= row) & (col <= row + 2 * WINDOW)
    if edge:
        key_pos = col + first_key
        keep = keep & (key_pos >= 0) & (key_pos < seq_len)
    band = pl.ds(at, 3 * WINDOW)
    for pair in range(queries.shape[1] // PAIR):
        lanes = slice(pair * PAIR, (pair + 1) * PAIR)
        attended = jnp.zeros((WINDOW, PAIR), F32)
        for side in range(2):
            scores = lax.dot_general(
                queries[:, lanes], band_ref[side, band], nt, preferred_element_type=F32
            ) * HEAD_DIM ** (-0.5)
            scores = jnp.where(keep, scores, masked_score)
            sink = sink_ref[2 * pair + side]
            top = jnp.maximum(jnp.max(scores, axis=1, keepdims=True), sink)
            raised = jnp.exp(scores - top)
            total = jnp.sum(raised, axis=1, keepdims=True) + jnp.exp(sink - top)
            probs = (raised * (1.0 / total)).astype(BF16)
            attended += jnp.dot(probs, band_ref[2 + side, band], preferred_element_type=F32)
        attended_ref[to : to + WINDOW, lanes] = attended.astype(BF16)


def pooled_rows(chan, centre, first_pos, seq_len, w_pool_ref, scale_ref):
    y = lax.axis_index(TP)
    length = chan.shape[0]
    sums = chan + pltpu.roll(chan, 1, 0)
    window_sum = sums
    for level in range(1, POOL_GROUPS):
        step = 2 ** (level - 1)
        sums = pltpu.roll(sums, step, 0) + pltpu.roll(sums, length - step, 0)
        window_sum = jnp.where(y >= level, sums, window_sum)
    half_width = jnp.left_shift(jnp.int32(1), y)
    rows = 2 * WINDOW
    row = lax.broadcasted_iota(jnp.int32, (rows, 1), 0)
    pos = row + jnp.where(row < WINDOW, first_pos[0], first_pos[1])
    count = jnp.minimum(pos + half_width, seq_len) - jnp.maximum(pos - half_width, 0)
    spread = centre(window_sum) / count.astype(F32) - centre(chan)
    pooled = jnp.dot(spread.astype(BF16), w_pool_ref[0], preferred_element_type=F32)
    return (pooled * scale_ref[...]).astype(BF16)


def inner_kernel(
    seq_len,
    tokens_ref,
    own_ref,
    other_ref,
    kv_ref,
    chan_ref,
    sink_ref,
    w_pool_ref,
    scale_ref,
    query_ref,
    attended_ref,
    pooled_ref,
    w_ref,
    band_ref,
):
    rows, query_cols = query_ref.shape
    whole_weights(own_ref, other_ref, w_ref, own_ref.shape[3] - query_cols)
    query_ref[...] = projected(tokens_ref, w_ref, 0, query_cols)
    split_band(kv_ref[...], band_ref)
    for b in range(1, rows // WINDOW - 1):
        attend_block(
            query_ref[b * WINDOW : (b + 1) * WINDOW],
            0,
            False,
            seq_len,
            band_ref,
            (b - 1) * WINDOW,
            sink_ref,
            attended_ref,
            (b - 1) * WINDOW,
        )
    near = 2 * RIM
    chan = chan_ref[WINDOW - near : rows - WINDOW + near].astype(F32)
    offset = lax.axis_index(SP) * rows + WINDOW
    pooled_ref[...] = pooled_rows(
        chan, lambda a: a[near:-near], (offset, offset), seq_len, w_pool_ref, scale_ref
    )


def outer_kernel(
    seq_len,
    query_ref,
    kv_ref,
    chan_ref,
    before_ref,
    after_ref,
    sink_ref,
    w_pool_ref,
    scale_ref,
    attended_ref,
    pooled_ref,
    band_ref,
):
    rows = chan_ref.shape[0]
    offset = lax.axis_index(SP) * rows

    split_band(
        jnp.concatenate(
            [
                before_ref[:WINDOW],
                kv_ref[: 2 * WINDOW],
                kv_ref[rows - 2 * WINDOW :],
                after_ref[:WINDOW],
            ]
        ),
        band_ref,
    )
    for edge, start in enumerate((0, rows - WINDOW)):
        attend_block(
            query_ref[start : start + WINDOW],
            offset + start - WINDOW,
            True,
            seq_len,
            band_ref,
            edge * 3 * WINDOW,
            sink_ref,
            attended_ref,
            edge * WINDOW,
        )

    def rim(ref):
        packed = ref[WINDOW:].astype(F32)
        return jnp.concatenate([packed[:RIM], packed[RIM:]], axis=1)

    near = 2 * RIM
    first = chan_ref[: WINDOW + near].astype(F32)
    last = chan_ref[rows - WINDOW - near :].astype(F32)
    chan = jnp.concatenate([rim(before_ref), first, last, rim(after_ref)])

    def centre(a):
        return jnp.concatenate([a[RIM : RIM + WINDOW], a[-RIM - WINDOW : -RIM]])

    pooled_ref[...] = pooled_rows(
        chan, centre, (offset, offset + rows - 2 * WINDOW), seq_len, w_pool_ref, scale_ref
    )


def out_kernel(ahead, count, *refs):
    mixed_refs, (own_ref, other_ref, out_ref, hidden_ref, w_ref) = refs[: 2 * count], refs[2 * count :]
    to = lax.rem(lax.axis_index(TP) + ahead, lax.axis_size(TP))
    zs = own_ref.shape[1] // lax.axis_size(TP)
    at = own_ref.shape[3] - hidden_ref.shape[1]
    mine = pl.ds(to * zs, zs)
    whole_weights(own_ref.at[:, mine], other_ref.at[:, mine], w_ref, at)
    for part in range(count):
        attended_ref, pooled_ref = mixed_refs[2 * part : 2 * part + 2]
        rows, query_cols = attended_ref.shape
        here = slice(part * rows, (part + 1) * rows)
        hidden_ref[here, :query_cols] = attended_ref[...]
        hidden_ref[here, query_cols:] = pooled_ref[...]
    out_ref[...] = lax.dot_general(
        hidden_ref[...], w_ref[...], nt, preferred_element_type=F32
    ).astype(BF16)


VMEM = pl.BlockSpec(memory_space=pltpu.VMEM)
SMEM = pl.BlockSpec(memory_space=pltpu.SMEM)
LIMIT = pltpu.CompilerParams(vmem_limit_bytes=20 * 1024 * 1024)


def layer(
    tokens,
    w_query,
    w_key,
    w_value,
    w_pool_in,
    sink,
    w_pool,
    pool_scale,
    w_out_attn,
    w_out_pool,
    out_gain,
):
    rows = tokens.shape[0]
    seq_len = rows * lax.axis_size(SP)
    query_cols, key_cols, chan_cols = w_query.shape[1], w_key.shape[1], w_pool_in.shape[1]
    in_cols = 2 * key_cols + chan_cols + query_cols
    hidden_cols = query_cols + chan_cols
    share = out_gain.shape[0]
    model_width = share * lax.axis_size(TP)

    gathered = from_everyone(tokens, TP)
    packed = jnp.concatenate(
        (w_key, w_value, w_pool_in, w_query, w_out_attn.T, w_out_pool.T), axis=1
    )
    over_z = lax.all_gather(packed, Z, axis=0)
    over_x = from_everyone(over_z, X)
    own1, own2 = over_x[..., :in_cols], over_x[..., in_cols:]
    other1 = swapped(own1)
    other2 = swapped(own2)

    def rows_of(width, count=rows):
        return jax.ShapeDtypeStruct((count, width), BF16)

    def cost(flops, size):
        return pl.CostEstimate(flops=flops, bytes_accessed=size, transcendentals=0)

    rim_shape = rows_of(PAIR, WINDOW + 2 * RIM)
    kv, chan, head, tail = pl.pallas_call(
        project_kernel,
        out_shape=[rows_of(2 * key_cols), rows_of(chan_cols), rim_shape, rim_shape],
        in_specs=[VMEM] * 3,
        out_specs=[VMEM] * 4,
        scratch_shapes=[pltpu.VMEM((model_width, 2 * key_cols + chan_cols), BF16)],
        compiler_params=LIMIT,
        cost_estimate=cost(2 * rows * model_width * (in_cols - query_cols), 4 << 20),
        name="project",
    )(gathered, own1, other1)
    before, after = neighbours(head, tail, SP)
    half = rows // 2
    scale = pool_scale.reshape(1, -1)
    query, *inner = pl.pallas_call(
        functools.partial(inner_kernel, seq_len),
        out_shape=[rows_of(query_cols), rows_of(query_cols, half), rows_of(chan_cols, half)],
        in_specs=[VMEM] * 5 + [SMEM] + [VMEM] * 2,
        out_specs=[VMEM] * 3,
        scratch_shapes=[
            pltpu.VMEM((model_width, query_cols), BF16),
            pltpu.VMEM((4, rows, PAIR), BF16),
        ],
        compiler_params=LIMIT,
        cost_estimate=cost(2 * rows * model_width * query_cols, 4 << 20),
        name="inner",
    )(gathered, own1, other1, kv, chan, sink, w_pool, scale)
    outer = pl.pallas_call(
        functools.partial(outer_kernel, seq_len),
        out_shape=[rows_of(query_cols, half), rows_of(chan_cols, half)],
        in_specs=[VMEM] * 5 + [SMEM] + [VMEM] * 2,
        out_specs=[VMEM] * 2,
        scratch_shapes=[pltpu.VMEM((4, 6 * WINDOW, PAIR), BF16)],
        compiler_params=LIMIT,
        cost_estimate=cost(2 * rows * model_width * query_cols, 2 << 20),
        name="outer",
    )(query, kv, chan, before, after, sink, w_pool, scale)

    def multiplied(ahead, *mixed):
        count = len(mixed)
        return pl.pallas_call(
            functools.partial(out_kernel, ahead, count),
            out_shape=rows_of(share, count * half),
            in_specs=[VMEM] * (2 * count + 2),
            out_specs=VMEM,
            scratch_shapes=[
                pltpu.VMEM((count * half, hidden_cols), BF16),
                pltpu.VMEM((share, hidden_cols), BF16),
            ],
            compiler_params=LIMIT,
            cost_estimate=cost(2 * count * half * share * hidden_cols, 1 << 20),
        )(*(a for pair in mixed for a in pair), own2, other2)

    def sent(ahead, *mixed):
        block = multiplied(ahead, *mixed)
        count = lax.axis_size(TP)
        return lax.ppermute(block, TP, [(i, (i + ahead) % count) for i in range(count)])

    far = jnp.concatenate([sent(2, inner), sent(2, outer)])
    partials = [sent(1, inner, outer), sent(3, inner, outer), far]
    mix = multiplied(0, inner, outer).astype(F32)
    for partial in partials:
        mix = mix + partial.astype(F32)
    stats = jnp.stack([jnp.sum(mix, axis=1), jnp.sum(mix * mix, axis=1)])
    stats = of_everyone(stats, TP)
    row_mean = stats[0] / model_width
    variance = stats[1] / model_width - row_mean * row_mean
    normed = (mix - row_mean[:, None]) * lax.rsqrt(variance + epsilon)[:, None] * out_gain
    normed = normed.astype(BF16)
    return jnp.concatenate([normed[half : half + WINDOW], normed[:half], normed[half + WINDOW :]])


def solution(mesh):
    finer = Mesh(mesh.devices.reshape(16, 4, 2, mesh.shape["tp"]), ("sp_0", "sp_1", "sp_2", "tp"))
    return jax.shard_map(
        layer,
        mesh=finer,
        in_specs=(
            P(SP, "tp"),
            P(SP, "tp"),
            P(SP, "tp"),
            P(SP, "tp"),
            P(SP, "tp"),
            P("tp"),
            P("tp", None, None),
            P("tp"),
            P("tp", SP),
            P("tp", SP),
            P("tp"),
        ),
        out_specs=P(SP, "tp"),
        check_vma=False,
    )
```

```python
import functools

import jax
import jax.numpy as jnp
from jax import lax
from jax.experimental import pallas as pl
from jax.experimental.pallas import tpu as pltpu
from jax.sharding import Mesh
from jax.sharding import PartitionSpec as P


HEAD_DIM = 64
PAIR = 2 * HEAD_DIM
POOL_GROUPS = 4
RIM = 2 ** (POOL_GROUPS - 1)
WINDOW = 128
SP = ("sp_0", "sp_1", "sp_2")
Z, X, CORE = SP
TP = "tp"
BF16, F32 = jnp.bfloat16, jnp.float32

epsilon = 1e-05
masked_score = -1e30
nt = (((1,), (1,)), ((), ()))


def from_everyone(shard, axis):
    count = lax.axis_size(axis)
    return lax.all_to_all(
        jnp.broadcast_to(shard[None], (count, *shard.shape)), axis, 0, 0, tiled=True
    )


def of_everyone(shard, axis):
    return jnp.sum(from_everyone(shard, axis), axis=0)


def swapped(shard):
    return lax.ppermute(shard, CORE, [(0, 1), (1, 0)])


def neighbours(inside, outside):
    count = lax.axis_size(SP)
    pairs = [(i, i + 1) for i in range(1, count - 1, 2)]
    return swapped(inside), lax.ppermute(outside, SP, pairs + [(b, a) for a, b in pairs])


def whole_weights(own_ref, other_ref, w_ref, at):
    core = lax.axis_index(CORE)
    xs, zs, rows = own_ref.shape[:3]
    lanes = slice(at, at + w_ref.shape[1])
    for z in range(zs):
        for x in range(xs):
            base = (z * xs + x) * 2 * rows
            w_ref[pl.ds(pl.multiple_of(base + core * rows, rows), rows), :] = own_ref[
                x, z, :, lanes
            ]
            w_ref[pl.ds(pl.multiple_of(base + (1 - core) * rows, rows), rows), :] = other_ref[
                x, z, :, lanes
            ]


def projected(tokens_ref, w_ref, at, width):
    depth = tokens_ref.shape[2]
    total = None
    for p in range(tokens_ref.shape[0]):
        part = jnp.dot(
            tokens_ref[p],
            w_ref[p * depth : (p + 1) * depth, at : at + width],
            preferred_element_type=F32,
        )
        total = part if total is None else total + part
    return total.astype(BF16)


def project_kernel(
    tokens_ref, own_ref, other_ref, kv_ref, chan_ref, inside_ref, outside_ref, w_ref
):
    rows = tokens_ref.shape[1]
    whole_weights(own_ref, other_ref, w_ref, 0)
    kv_cols = kv_ref.shape[1]
    kv_ref[...] = projected(tokens_ref, w_ref, 0, kv_cols)
    chan_ref[...] = projected(tokens_ref, w_ref, kv_cols, chan_ref.shape[1])

    def rim(kv_at, chan_at):
        edge = chan_ref[chan_at : chan_at + RIM].astype(F32)
        kv = kv_ref[kv_at : kv_at + WINDOW].astype(F32)
        return jnp.concatenate([kv, edge[:, :PAIR], edge[:, PAIR:]])

    first, last = rim(0, 0), rim(rows - WINDOW, rows - RIM)
    ahead = lax.axis_index(CORE) == 0
    inside_ref[...] = jnp.where(ahead, last, first).astype(BF16)
    outside_ref[...] = jnp.where(ahead, first, last).astype(BF16)


def split_band(kv, band_ref):
    kv = kv.astype(F32)
    turned = pltpu.roll(kv, HEAD_DIM, 1)
    low = lax.broadcasted_iota(jnp.int32, kv.shape, 1) < HEAD_DIM
    band_ref[0] = jnp.where(low, kv, 0.0).astype(BF16)
    band_ref[1] = jnp.where(low, 0.0, turned).astype(BF16)
    band_ref[2] = jnp.where(low, turned, 0.0).astype(BF16)
    band_ref[3] = jnp.where(low, 0.0, kv).astype(BF16)


def attend_block(queries, first_key, edge, seq_len, band_ref, at, sink_ref, attended_ref, to):
    row = lax.broadcasted_iota(jnp.int32, (WINDOW, 3 * WINDOW), 0)
    col = lax.broadcasted_iota(jnp.int32, (WINDOW, 3 * WINDOW), 1)
    keep = (col >= row) & (col <= row + 2 * WINDOW)
    if edge:
        key_pos = col + first_key
        keep = keep & (key_pos >= 0) & (key_pos < seq_len)
    band = pl.ds(at, 3 * WINDOW)
    for pair in range(queries.shape[1] // PAIR):
        lanes = slice(pair * PAIR, (pair + 1) * PAIR)
        attended = jnp.zeros((WINDOW, PAIR), F32)
        for side in range(2):
            scores = lax.dot_general(
                queries[:, lanes], band_ref[side, band], nt, preferred_element_type=F32
            ) * HEAD_DIM ** (-0.5)
            scores = jnp.where(keep, scores, masked_score)
            sink = sink_ref[2 * pair + side]
            top = jnp.maximum(jnp.max(scores, axis=1, keepdims=True), sink)
            raised = jnp.exp(scores - top)
            total = jnp.sum(raised, axis=1, keepdims=True) + jnp.exp(sink - top)
            probs = (raised * (1.0 / total)).astype(BF16)
            attended += jnp.dot(probs, band_ref[2 + side, band], preferred_element_type=F32)
        attended_ref[to : to + WINDOW, lanes] = attended.astype(BF16)


def pooled_rows(chan, centre, first_pos, seq_len, w_pool_ref, scale_ref):
    y = lax.axis_index(TP)
    length = chan.shape[0]
    sums = chan + pltpu.roll(chan, 1, 0)
    window_sum = sums
    for level in range(1, POOL_GROUPS):
        step = 2 ** (level - 1)
        sums = pltpu.roll(sums, step, 0) + pltpu.roll(sums, length - step, 0)
        window_sum = jnp.where(y >= level, sums, window_sum)
    half_width = jnp.left_shift(jnp.int32(1), y)
    rows = 2 * WINDOW
    row = lax.broadcasted_iota(jnp.int32, (rows, 1), 0)
    pos = row + jnp.where(row < WINDOW, first_pos[0], first_pos[1])
    count = jnp.minimum(pos + half_width, seq_len) - jnp.maximum(pos - half_width, 0)
    spread = centre(window_sum) / count.astype(F32) - centre(chan)
    pooled = jnp.dot(spread.astype(BF16), w_pool_ref[0], preferred_element_type=F32)
    return (pooled * scale_ref[...]).astype(BF16)


def inner_kernel(
    seq_len,
    tokens_ref,
    own_ref,
    other_ref,
    kv_ref,
    chan_ref,
    sink_ref,
    w_pool_ref,
    scale_ref,
    query_ref,
    attended_ref,
    pooled_ref,
    w_ref,
    band_ref,
):
    rows, query_cols = query_ref.shape
    whole_weights(own_ref, other_ref, w_ref, own_ref.shape[3] - query_cols)
    query_ref[...] = projected(tokens_ref, w_ref, 0, query_cols)
    split_band(kv_ref[...], band_ref)
    for b in range(1, rows // WINDOW - 1):
        attend_block(
            query_ref[b * WINDOW : (b + 1) * WINDOW],
            0,
            False,
            seq_len,
            band_ref,
            (b - 1) * WINDOW,
            sink_ref,
            attended_ref,
            (b - 1) * WINDOW,
        )
    near = 2 * RIM
    chan = chan_ref[WINDOW - near : rows - WINDOW + near].astype(F32)
    offset = lax.axis_index(SP) * rows + WINDOW
    pooled_ref[...] = pooled_rows(
        chan, lambda a: a[near:-near], (offset, offset), seq_len, w_pool_ref, scale_ref
    )


def outer_kernel(
    seq_len,
    query_ref,
    kv_ref,
    chan_ref,
    inside_ref,
    outside_ref,
    sink_ref,
    w_pool_ref,
    scale_ref,
    attended_ref,
    pooled_ref,
    band_ref,
):
    rows = chan_ref.shape[0]
    offset = lax.axis_index(SP) * rows
    ahead = lax.axis_index(CORE) == 0
    inside, outside = inside_ref[...].astype(F32), outside_ref[...].astype(F32)
    before, after = jnp.where(ahead, outside, inside), jnp.where(ahead, inside, outside)

    split_band(
        jnp.concatenate(
            [
                before[:WINDOW],
                kv_ref[: 2 * WINDOW].astype(F32),
                kv_ref[rows - 2 * WINDOW :].astype(F32),
                after[:WINDOW],
            ]
        ),
        band_ref,
    )
    for edge, start in enumerate((0, rows - WINDOW)):
        attend_block(
            query_ref[start : start + WINDOW],
            offset + start - WINDOW,
            True,
            seq_len,
            band_ref,
            edge * 3 * WINDOW,
            sink_ref,
            attended_ref,
            edge * WINDOW,
        )

    def rim(packed):
        return jnp.concatenate([packed[WINDOW : WINDOW + RIM], packed[WINDOW + RIM :]], axis=1)

    near = 2 * RIM
    first = chan_ref[: WINDOW + near].astype(F32)
    last = chan_ref[rows - WINDOW - near :].astype(F32)
    chan = jnp.concatenate([rim(before), first, last, rim(after)])

    def centre(a):
        return jnp.concatenate([a[RIM : RIM + WINDOW], a[-RIM - WINDOW : -RIM]])

    pooled_ref[...] = pooled_rows(
        chan, centre, (offset, offset + rows - 2 * WINDOW), seq_len, w_pool_ref, scale_ref
    )


def out_kernel(mask, count, *refs):
    mixed_refs, (own_ref, other_ref, out_ref, hidden_ref, w_ref) = refs[: 2 * count], refs[2 * count :]
    to = lax.axis_index(TP) ^ mask
    zs = own_ref.shape[1] // lax.axis_size(TP)
    at = own_ref.shape[3] - hidden_ref.shape[1]
    mine = pl.ds(to * zs, zs)
    whole_weights(own_ref.at[:, mine], other_ref.at[:, mine], w_ref, at)
    for part in range(count):
        attended_ref, pooled_ref = mixed_refs[2 * part : 2 * part + 2]
        rows, query_cols = attended_ref.shape
        here = slice(part * rows, (part + 1) * rows)
        hidden_ref[here, :query_cols] = attended_ref[...]
        hidden_ref[here, query_cols:] = pooled_ref[...]
    out_ref[...] = lax.dot_general(
        hidden_ref[...], w_ref[...], nt, preferred_element_type=F32
    ).astype(BF16)


VMEM = pl.BlockSpec(memory_space=pltpu.VMEM)
SMEM = pl.BlockSpec(memory_space=pltpu.SMEM)
LIMIT = pltpu.CompilerParams(vmem_limit_bytes=20 * 1024 * 1024)


def layer(
    tokens,
    w_query,
    w_key,
    w_value,
    w_pool_in,
    sink,
    w_pool,
    pool_scale,
    w_out_attn,
    w_out_pool,
    out_gain,
):
    rows = tokens.shape[0]
    seq_len = rows * lax.axis_size(SP)
    query_cols, key_cols, chan_cols = w_query.shape[1], w_key.shape[1], w_pool_in.shape[1]
    in_cols = 2 * key_cols + chan_cols + query_cols
    hidden_cols = query_cols + chan_cols
    share = out_gain.shape[0]
    model_width = share * lax.axis_size(TP)

    gathered = from_everyone(tokens, TP)
    packed = jnp.concatenate(
        (w_key, w_value, w_pool_in, w_query, w_out_attn.T, w_out_pool.T), axis=1
    )
    over_z = lax.all_gather(packed, Z, axis=0)
    over_x = from_everyone(over_z, X)
    own1, own2 = over_x[..., :in_cols], over_x[..., in_cols:]
    other1 = swapped(own1)
    other2 = swapped(own2)

    def rows_of(width, count=rows):
        return jax.ShapeDtypeStruct((count, width), BF16)

    def cost(flops, size):
        return pl.CostEstimate(flops=flops, bytes_accessed=size, transcendentals=0)

    rim_shape = rows_of(PAIR, WINDOW + 2 * RIM)
    kv, chan, inside, outside = pl.pallas_call(
        project_kernel,
        out_shape=[rows_of(2 * key_cols), rows_of(chan_cols), rim_shape, rim_shape],
        in_specs=[VMEM] * 3,
        out_specs=[VMEM] * 4,
        scratch_shapes=[pltpu.VMEM((model_width, 2 * key_cols + chan_cols), BF16)],
        compiler_params=LIMIT,
        cost_estimate=cost(2 * rows * model_width * (in_cols - query_cols), 4 << 20),
        name="project",
    )(gathered, own1, other1)
    inside, outside = neighbours(inside, outside)
    half = rows // 2
    scale = pool_scale.reshape(1, -1)
    query, *inner = pl.pallas_call(
        functools.partial(inner_kernel, seq_len),
        out_shape=[rows_of(query_cols), rows_of(query_cols, half), rows_of(chan_cols, half)],
        in_specs=[VMEM] * 5 + [SMEM] + [VMEM] * 2,
        out_specs=[VMEM] * 3,
        scratch_shapes=[
            pltpu.VMEM((model_width, query_cols), BF16),
            pltpu.VMEM((4, rows, PAIR), BF16),
        ],
        compiler_params=LIMIT,
        cost_estimate=cost(2 * rows * model_width * query_cols, 4 << 20),
        name="inner",
    )(gathered, own1, other1, kv, chan, sink, w_pool, scale)
    outer = pl.pallas_call(
        functools.partial(outer_kernel, seq_len),
        out_shape=[rows_of(query_cols, half), rows_of(chan_cols, half)],
        in_specs=[VMEM] * 5 + [SMEM] + [VMEM] * 2,
        out_specs=[VMEM] * 2,
        scratch_shapes=[pltpu.VMEM((4, 6 * WINDOW, PAIR), BF16)],
        compiler_params=LIMIT,
        cost_estimate=cost(2 * rows * model_width * query_cols, 2 << 20),
        name="outer",
    )(query, kv, chan, inside, outside, sink, w_pool, scale)

    def multiplied(mask, *mixed):
        count = len(mixed)
        return pl.pallas_call(
            functools.partial(out_kernel, mask, count),
            out_shape=rows_of(share, count * half),
            in_specs=[VMEM] * (2 * count + 2),
            out_specs=VMEM,
            scratch_shapes=[
                pltpu.VMEM((count * half, hidden_cols), BF16),
                pltpu.VMEM((share, hidden_cols), BF16),
            ],
            compiler_params=LIMIT,
            cost_estimate=cost(2 * count * half * share * hidden_cols, 1 << 20),
        )(*(a for pair in mixed for a in pair), own2, other2)

    def sent(mask, *mixed):
        block = multiplied(mask, *mixed)
        count = lax.axis_size(TP)
        return lax.ppermute(block, TP, [(i, i ^ mask) for i in range(count)])

    far = jnp.concatenate([sent(2, inner), sent(2, outer)])
    partials = [sent(1, inner, outer), sent(3, inner, outer), far]
    mix = multiplied(0, inner, outer).astype(F32)
    for partial in partials:
        mix = mix + partial.astype(F32)
    stats = jnp.stack([jnp.sum(mix, axis=1), jnp.sum(mix * mix, axis=1)])
    stats = of_everyone(stats, TP)
    row_mean = stats[0] / model_width
    variance = stats[1] / model_width - row_mean * row_mean
    normed = (mix - row_mean[:, None]) * lax.rsqrt(variance + epsilon)[:, None] * out_gain
    normed = normed.astype(BF16)
    return jnp.concatenate([normed[half : half + WINDOW], normed[:half], normed[half + WINDOW :]])


def solution(mesh):
    finer = Mesh(mesh.devices.reshape(16, 4, 2, mesh.shape["tp"]), ("sp_0", "sp_1", "sp_2", "tp"))
    return jax.shard_map(
        layer,
        mesh=finer,
        in_specs=(
            P(SP, "tp"),
            P(SP, "tp"),
            P(SP, "tp"),
            P(SP, "tp"),
            P(SP, "tp"),
            P("tp"),
            P("tp", None, None),
            P("tp"),
            P("tp", SP),
            P("tp", SP),
            P("tp"),
        ),
        out_specs=P(SP, "tp"),
        check_vma=False,
    )
```

```python
import functools

import jax
import jax.numpy as jnp
from jax import lax
from jax.experimental import pallas as pl
from jax.experimental.pallas import tpu as pltpu
from jax.sharding import Mesh
from jax.sharding import PartitionSpec as P


HEAD_DIM = 64
PAIR = 2 * HEAD_DIM
POOL_GROUPS = 4
RIM = 2 ** (POOL_GROUPS - 1)
WINDOW = 128
SP = ("sp_0", "sp_1", "sp_2")
Z, X, CORE = SP
TP = "tp"
BF16, F32 = jnp.bfloat16, jnp.float32

epsilon = 1e-05
masked_score = -1e30
MASKS = (0, 2, 1, 3)
nt = (((1,), (1,)), ((), ()))


def from_everyone(shard, axis):
    count = lax.axis_size(axis)
    return lax.all_to_all(
        jnp.broadcast_to(shard[None], (count, *shard.shape)), axis, 0, 0, tiled=True
    )


def of_everyone(shard, axis):
    return jnp.sum(from_everyone(shard, axis), axis=0)


def exchanged(shard, axis, mask):
    return lax.ppermute(shard, axis, [(i, i ^ mask) for i in range(lax.axis_size(axis))])


def swapped(shard):
    return exchanged(shard, CORE, 1)


def neighbours(inside, outside):
    count = lax.axis_size(SP)
    pairs = [(i, i + 1) for i in range(1, count - 1, 2)]
    return swapped(inside), lax.ppermute(outside, SP, pairs + [(b, a) for a, b in pairs])


def whole_weights(own_ref, other_ref, w_ref, at, sources):
    core = lax.axis_index(CORE)
    xs, zs, rows = own_ref.shape[:3]
    lanes = slice(at, at + w_ref.shape[1])
    for slot, source in enumerate(sources):
        for z in range(zs):
            base = (z * xs + source) * 2 * rows
            w_ref[pl.ds(pl.multiple_of(base + core * rows, rows), rows), :] = own_ref[
                slot, z, :, lanes
            ]
            w_ref[pl.ds(pl.multiple_of(base + (1 - core) * rows, rows), rows), :] = other_ref[
                slot, z, :, lanes
            ]


def projected(tokens_ref, w_ref, at, width):
    depth = tokens_ref.shape[2]
    total = None
    for p in range(tokens_ref.shape[0]):
        part = jnp.dot(
            tokens_ref[p],
            w_ref[p * depth : (p + 1) * depth, at : at + width],
            preferred_element_type=F32,
        )
        total = part if total is None else total + part
    return total.astype(BF16)


def project_kernel(
    tokens_ref, own_ref, other_ref, kv_ref, chan_ref, inside_ref, outside_ref, w_ref
):
    rows = tokens_ref.shape[1]
    whole_weights(own_ref, other_ref, w_ref, 0, range(own_ref.shape[0]))
    kv_cols = kv_ref.shape[1]
    kv_ref[...] = projected(tokens_ref, w_ref, 0, kv_cols)
    chan_ref[...] = projected(tokens_ref, w_ref, kv_cols, chan_ref.shape[1])

    def rim(kv_at, chan_at):
        edge = chan_ref[chan_at : chan_at + RIM].astype(F32)
        kv = kv_ref[kv_at : kv_at + WINDOW].astype(F32)
        return jnp.concatenate([kv, edge[:, :PAIR], edge[:, PAIR:]])

    first, last = rim(0, 0), rim(rows - WINDOW, rows - RIM)
    ahead = lax.axis_index(CORE) == 0
    inside_ref[...] = jnp.where(ahead, last, first).astype(BF16)
    outside_ref[...] = jnp.where(ahead, first, last).astype(BF16)


def split_band(kv, band_ref):
    kv = kv.astype(F32)
    turned = pltpu.roll(kv, HEAD_DIM, 1)
    low = lax.broadcasted_iota(jnp.int32, kv.shape, 1) < HEAD_DIM
    band_ref[0] = jnp.where(low, kv, 0.0).astype(BF16)
    band_ref[1] = jnp.where(low, 0.0, turned).astype(BF16)
    band_ref[2] = jnp.where(low, turned, 0.0).astype(BF16)
    band_ref[3] = jnp.where(low, 0.0, kv).astype(BF16)


def attend_block(queries, first_key, edge, seq_len, band_ref, at, sink_ref, attended_ref, to):
    row = lax.broadcasted_iota(jnp.int32, (WINDOW, 3 * WINDOW), 0)
    col = lax.broadcasted_iota(jnp.int32, (WINDOW, 3 * WINDOW), 1)
    keep = (col >= row) & (col <= row + 2 * WINDOW)
    if edge:
        key_pos = col + first_key
        keep = keep & (key_pos >= 0) & (key_pos < seq_len)
    band = pl.ds(at, 3 * WINDOW)
    for pair in range(queries.shape[1] // PAIR):
        lanes = slice(pair * PAIR, (pair + 1) * PAIR)
        attended = jnp.zeros((WINDOW, PAIR), F32)
        for side in range(2):
            scores = lax.dot_general(
                queries[:, lanes], band_ref[side, band], nt, preferred_element_type=F32
            ) * HEAD_DIM ** (-0.5)
            scores = jnp.where(keep, scores, masked_score)
            sink = sink_ref[2 * pair + side]
            top = jnp.maximum(jnp.max(scores, axis=1, keepdims=True), sink)
            raised = jnp.exp(scores - top)
            total = jnp.sum(raised, axis=1, keepdims=True) + jnp.exp(sink - top)
            probs = (raised * (1.0 / total)).astype(BF16)
            attended += jnp.dot(probs, band_ref[2 + side, band], preferred_element_type=F32)
        attended_ref[to : to + WINDOW, lanes] = attended.astype(BF16)


def pooled_rows(chan, centre, first_pos, seq_len, w_pool_ref, scale_ref):
    y = lax.axis_index(TP)
    length = chan.shape[0]
    sums = chan + pltpu.roll(chan, 1, 0)
    window_sum = sums
    for level in range(1, POOL_GROUPS):
        step = 2 ** (level - 1)
        sums = pltpu.roll(sums, step, 0) + pltpu.roll(sums, length - step, 0)
        window_sum = jnp.where(y >= level, sums, window_sum)
    half_width = jnp.left_shift(jnp.int32(1), y)
    rows = 2 * WINDOW
    row = lax.broadcasted_iota(jnp.int32, (rows, 1), 0)
    pos = row + jnp.where(row < WINDOW, first_pos[0], first_pos[1])
    count = jnp.minimum(pos + half_width, seq_len) - jnp.maximum(pos - half_width, 0)
    spread = centre(window_sum) / count.astype(F32) - centre(chan)
    pooled = jnp.dot(spread.astype(BF16), w_pool_ref[0], preferred_element_type=F32)
    return (pooled * scale_ref[...]).astype(BF16)


def inner_kernel(
    seq_len,
    tokens_ref,
    own_ref,
    other_ref,
    kv_ref,
    chan_ref,
    sink_ref,
    w_pool_ref,
    scale_ref,
    query_ref,
    attended_ref,
    pooled_ref,
    w_ref,
    band_ref,
):
    rows, query_cols = query_ref.shape
    whole_weights(
        own_ref, other_ref, w_ref, own_ref.shape[3] - query_cols, range(own_ref.shape[0])
    )
    query_ref[...] = projected(tokens_ref, w_ref, 0, query_cols)
    split_band(kv_ref[...], band_ref)
    for b in range(1, rows // WINDOW - 1):
        attend_block(
            query_ref[b * WINDOW : (b + 1) * WINDOW],
            0,
            False,
            seq_len,
            band_ref,
            (b - 1) * WINDOW,
            sink_ref,
            attended_ref,
            (b - 1) * WINDOW,
        )
    near = 2 * RIM
    chan = chan_ref[WINDOW - near : rows - WINDOW + near].astype(F32)
    offset = lax.axis_index(SP) * rows + WINDOW
    pooled_ref[...] = pooled_rows(
        chan, lambda a: a[near:-near], (offset, offset), seq_len, w_pool_ref, scale_ref
    )


def outer_kernel(
    seq_len,
    query_ref,
    kv_ref,
    chan_ref,
    inside_ref,
    outside_ref,
    sink_ref,
    w_pool_ref,
    scale_ref,
    attended_ref,
    pooled_ref,
    band_ref,
):
    rows = chan_ref.shape[0]
    offset = lax.axis_index(SP) * rows
    ahead = lax.axis_index(CORE) == 0
    inside, outside = inside_ref[...].astype(F32), outside_ref[...].astype(F32)
    before, after = jnp.where(ahead, outside, inside), jnp.where(ahead, inside, outside)

    split_band(
        jnp.concatenate(
            [
                before[:WINDOW],
                kv_ref[: 2 * WINDOW].astype(F32),
                kv_ref[rows - 2 * WINDOW :].astype(F32),
                after[:WINDOW],
            ]
        ),
        band_ref,
    )
    for edge, start in enumerate((0, rows - WINDOW)):
        attend_block(
            query_ref[start : start + WINDOW],
            offset + start - WINDOW,
            True,
            seq_len,
            band_ref,
            edge * 3 * WINDOW,
            sink_ref,
            attended_ref,
            edge * WINDOW,
        )

    def rim(packed):
        return jnp.concatenate([packed[WINDOW : WINDOW + RIM], packed[WINDOW + RIM :]], axis=1)

    near = 2 * RIM
    first = chan_ref[: WINDOW + near].astype(F32)
    last = chan_ref[rows - WINDOW - near :].astype(F32)
    chan = jnp.concatenate([rim(before), first, last, rim(after)])

    def centre(a):
        return jnp.concatenate([a[RIM : RIM + WINDOW], a[-RIM - WINDOW : -RIM]])

    pooled_ref[...] = pooled_rows(
        chan, centre, (offset, offset + rows - 2 * WINDOW), seq_len, w_pool_ref, scale_ref
    )


def out_kernel(mask, count, *refs):
    mixed_refs, (own_ref, other_ref, out_ref, hidden_ref, w_ref) = refs[: 2 * count], refs[2 * count :]
    to = lax.axis_index(TP) ^ mask
    zs = own_ref.shape[1] // lax.axis_size(TP)
    at = own_ref.shape[3] - hidden_ref.shape[1]
    mine = pl.ds(to * zs, zs)
    sources = [lax.axis_index(X) ^ m for m in MASKS]
    whole_weights(own_ref.at[:, mine], other_ref.at[:, mine], w_ref, at, sources)
    for part in range(count):
        attended_ref, pooled_ref = mixed_refs[2 * part : 2 * part + 2]
        rows, query_cols = attended_ref.shape
        here = slice(part * rows, (part + 1) * rows)
        hidden_ref[here, :query_cols] = attended_ref[...]
        hidden_ref[here, query_cols:] = pooled_ref[...]
    out_ref[...] = lax.dot_general(
        hidden_ref[...], w_ref[...], nt, preferred_element_type=F32
    ).astype(BF16)


VMEM = pl.BlockSpec(memory_space=pltpu.VMEM)
SMEM = pl.BlockSpec(memory_space=pltpu.SMEM)
LIMIT = pltpu.CompilerParams(vmem_limit_bytes=20 * 1024 * 1024)


def layer(
    tokens,
    w_query,
    w_key,
    w_value,
    w_pool_in,
    sink,
    w_pool,
    pool_scale,
    w_out_attn,
    w_out_pool,
    out_gain,
):
    rows = tokens.shape[0]
    seq_len = rows * lax.axis_size(SP)
    query_cols, key_cols, chan_cols = w_query.shape[1], w_key.shape[1], w_pool_in.shape[1]
    in_cols = 2 * key_cols + chan_cols + query_cols
    hidden_cols = query_cols + chan_cols
    share = out_gain.shape[0]
    model_width = share * lax.axis_size(TP)

    gathered = from_everyone(tokens, TP)
    packed = jnp.concatenate(
        (w_key, w_value, w_pool_in, w_query, w_out_attn.T, w_out_pool.T), axis=1
    )
    over_z = lax.all_gather(packed, Z, axis=0)
    for_all = jnp.broadcast_to(over_z[..., :in_cols], (lax.axis_size(X), *over_z.shape[:2], in_cols))
    for_all, piece = lax.optimization_barrier((for_all, over_z[..., in_cols:]))
    own1 = lax.all_to_all(for_all, X, 0, 0, tiled=True)
    pieces = [piece]
    for mask in MASKS[1:]:
        pieces.append(exchanged(pieces[0], X, mask))
    own2 = jnp.stack(pieces)
    other1 = swapped(own1)
    other2 = swapped(own2)

    def rows_of(width, count=rows):
        return jax.ShapeDtypeStruct((count, width), BF16)

    def cost(flops, size):
        return pl.CostEstimate(flops=flops, bytes_accessed=size, transcendentals=0)

    rim_shape = rows_of(PAIR, WINDOW + 2 * RIM)
    kv, chan, inside, outside = pl.pallas_call(
        project_kernel,
        out_shape=[rows_of(2 * key_cols), rows_of(chan_cols), rim_shape, rim_shape],
        in_specs=[VMEM] * 3,
        out_specs=[VMEM] * 4,
        scratch_shapes=[pltpu.VMEM((model_width, 2 * key_cols + chan_cols), BF16)],
        compiler_params=LIMIT,
        cost_estimate=cost(2 * rows * model_width * (in_cols - query_cols), 4 << 20),
        name="project",
    )(gathered, own1, other1)
    inside, outside = neighbours(inside, outside)
    half = rows // 2
    scale = pool_scale.reshape(1, -1)
    query, *inner = pl.pallas_call(
        functools.partial(inner_kernel, seq_len),
        out_shape=[rows_of(query_cols), rows_of(query_cols, half), rows_of(chan_cols, half)],
        in_specs=[VMEM] * 5 + [SMEM] + [VMEM] * 2,
        out_specs=[VMEM] * 3,
        scratch_shapes=[
            pltpu.VMEM((model_width, query_cols), BF16),
            pltpu.VMEM((4, rows, PAIR), BF16),
        ],
        compiler_params=LIMIT,
        cost_estimate=cost(2 * rows * model_width * query_cols, 4 << 20),
        name="inner",
    )(gathered, own1, other1, kv, chan, sink, w_pool, scale)
    outer = pl.pallas_call(
        functools.partial(outer_kernel, seq_len),
        out_shape=[rows_of(query_cols, half), rows_of(chan_cols, half)],
        in_specs=[VMEM] * 5 + [SMEM] + [VMEM] * 2,
        out_specs=[VMEM] * 2,
        scratch_shapes=[pltpu.VMEM((4, 6 * WINDOW, PAIR), BF16)],
        compiler_params=LIMIT,
        cost_estimate=cost(2 * rows * model_width * query_cols, 2 << 20),
        name="outer",
    )(query, kv, chan, inside, outside, sink, w_pool, scale)

    def multiplied(mask, *mixed):
        count = len(mixed)
        return pl.pallas_call(
            functools.partial(out_kernel, mask, count),
            out_shape=rows_of(share, count * half),
            in_specs=[VMEM] * (2 * count + 2),
            out_specs=VMEM,
            scratch_shapes=[
                pltpu.VMEM((count * half, hidden_cols), BF16),
                pltpu.VMEM((share, hidden_cols), BF16),
            ],
            compiler_params=LIMIT,
            cost_estimate=cost(2 * count * half * share * hidden_cols, 1 << 20),
        )(*(a for pair in mixed for a in pair), own2, other2)

    def sent(mask, *mixed):
        block = multiplied(mask, *mixed)
        return exchanged(block, TP, mask)

    far = jnp.concatenate([sent(2, inner), sent(2, outer)])
    partials = [sent(1, inner, outer), sent(3, inner, outer), far]
    mix = multiplied(0, inner, outer).astype(F32)
    for partial in partials:
        mix = mix + partial.astype(F32)
    stats = jnp.stack([jnp.sum(mix, axis=1), jnp.sum(mix * mix, axis=1)])
    stats = of_everyone(stats, TP)
    row_mean = stats[0] / model_width
    variance = stats[1] / model_width - row_mean * row_mean
    normed = (mix - row_mean[:, None]) * lax.rsqrt(variance + epsilon)[:, None] * out_gain
    normed = normed.astype(BF16)
    return jnp.concatenate([normed[half : half + WINDOW], normed[:half], normed[half + WINDOW :]])


def solution(mesh):
    finer = Mesh(mesh.devices.reshape(16, 4, 2, mesh.shape["tp"]), ("sp_0", "sp_1", "sp_2", "tp"))
    return jax.shard_map(
        layer,
        mesh=finer,
        in_specs=(
            P(SP, "tp"),
            P(SP, "tp"),
            P(SP, "tp"),
            P(SP, "tp"),
            P(SP, "tp"),
            P("tp"),
            P("tp", None, None),
            P("tp"),
            P("tp", SP),
            P("tp", SP),
            P("tp"),
        ),
        out_specs=P(SP, "tp"),
        check_vma=False,
    )
```

```python
import functools

import jax
import jax.numpy as jnp
from jax import lax
from jax.experimental import pallas as pl
from jax.experimental.pallas import tpu as pltpu
from jax.sharding import Mesh
from jax.sharding import PartitionSpec as P


HEAD_DIM = 64
PAIR = 2 * HEAD_DIM
POOL_GROUPS = 4
RIM = 2 ** (POOL_GROUPS - 1)
WINDOW = 128
SP = ("sp_0", "sp_1", "sp_2")
Z, X, CORE = SP
TP = "tp"
BF16, F32 = jnp.bfloat16, jnp.float32

epsilon = 1e-05
masked_score = -1e30
MASKS = (0, 2, 1, 3)
nt = (((1,), (1,)), ((), ()))


def from_everyone(shard, axis):
    count = lax.axis_size(axis)
    return lax.all_to_all(
        jnp.broadcast_to(shard[None], (count, *shard.shape)), axis, 0, 0, tiled=True
    )


def of_everyone(shard, axis):
    return jnp.sum(from_everyone(shard, axis), axis=0)


def exchanged(shard, axis, mask):
    return lax.ppermute(shard, axis, [(i, i ^ mask) for i in range(lax.axis_size(axis))])


def swapped(shard):
    return exchanged(shard, CORE, 1)


def neighbours(inside, outside):
    count = lax.axis_size(SP)
    pairs = [(i, i + 1) for i in range(1, count - 1, 2)]
    return swapped(inside), lax.ppermute(outside, SP, pairs + [(b, a) for a, b in pairs])


def whole_weights(own_ref, other_ref, w_ref, at):
    core = lax.axis_index(CORE)
    xs, zs, rows = own_ref.shape[:3]
    lanes = slice(at, at + w_ref.shape[1])
    for z in range(zs):
        for x in range(xs):
            base = (z * xs + x) * 2 * rows
            w_ref[pl.ds(pl.multiple_of(base + core * rows, rows), rows), :] = own_ref[
                x, z, :, lanes
            ]
            w_ref[pl.ds(pl.multiple_of(base + (1 - core) * rows, rows), rows), :] = other_ref[
                x, z, :, lanes
            ]


def projected(tokens_refs, w_ref, at, width):
    depth = tokens_refs[0].shape[1]
    total = None
    for mask, tokens_ref in zip(MASKS, tokens_refs):
        features = pl.ds(pl.multiple_of((lax.axis_index(TP) ^ mask) * depth, depth), depth)
        part = jnp.dot(
            tokens_ref[...], w_ref[features, at : at + width], preferred_element_type=F32
        )
        total = part if total is None else total + part
    return total.astype(BF16)


def project_kernel(*refs):
    tokens_refs = refs[: len(MASKS)]
    own_ref, other_ref, kv_ref, chan_ref, inside_ref, outside_ref, w_ref = refs[len(MASKS) :]
    rows = kv_ref.shape[0]
    whole_weights(own_ref, other_ref, w_ref, 0)
    kv_cols = kv_ref.shape[1]
    kv_ref[...] = projected(tokens_refs, w_ref, 0, kv_cols)
    chan_ref[...] = projected(tokens_refs, w_ref, kv_cols, chan_ref.shape[1])

    def rim(kv_at, chan_at):
        edge = chan_ref[chan_at : chan_at + RIM].astype(F32)
        kv = kv_ref[kv_at : kv_at + WINDOW].astype(F32)
        return jnp.concatenate([kv, edge[:, :PAIR], edge[:, PAIR:]])

    first, last = rim(0, 0), rim(rows - WINDOW, rows - RIM)
    ahead = lax.axis_index(CORE) == 0
    inside_ref[...] = jnp.where(ahead, last, first).astype(BF16)
    outside_ref[...] = jnp.where(ahead, first, last).astype(BF16)


def split_band(kv, band_ref):
    kv = kv.astype(F32)
    turned = pltpu.roll(kv, HEAD_DIM, 1)
    low = lax.broadcasted_iota(jnp.int32, kv.shape, 1) < HEAD_DIM
    band_ref[0] = jnp.where(low, kv, 0.0).astype(BF16)
    band_ref[1] = jnp.where(low, 0.0, turned).astype(BF16)
    band_ref[2] = jnp.where(low, turned, 0.0).astype(BF16)
    band_ref[3] = jnp.where(low, 0.0, kv).astype(BF16)


def attend_block(queries, first_key, edge, seq_len, band_ref, at, sink_ref, attended_ref, to):
    row = lax.broadcasted_iota(jnp.int32, (WINDOW, 3 * WINDOW), 0)
    col = lax.broadcasted_iota(jnp.int32, (WINDOW, 3 * WINDOW), 1)
    keep = (col >= row) & (col <= row + 2 * WINDOW)
    if edge:
        key_pos = col + first_key
        keep = keep & (key_pos >= 0) & (key_pos < seq_len)
    band = pl.ds(at, 3 * WINDOW)
    for pair in range(queries.shape[1] // PAIR):
        lanes = slice(pair * PAIR, (pair + 1) * PAIR)
        attended = jnp.zeros((WINDOW, PAIR), F32)
        for side in range(2):
            scores = lax.dot_general(
                queries[:, lanes], band_ref[side, band], nt, preferred_element_type=F32
            ) * HEAD_DIM ** (-0.5)
            scores = jnp.where(keep, scores, masked_score)
            sink = sink_ref[2 * pair + side]
            top = jnp.maximum(jnp.max(scores, axis=1, keepdims=True), sink)
            raised = jnp.exp(scores - top)
            total = jnp.sum(raised, axis=1, keepdims=True) + jnp.exp(sink - top)
            probs = (raised * (1.0 / total)).astype(BF16)
            attended += jnp.dot(probs, band_ref[2 + side, band], preferred_element_type=F32)
        attended_ref[to : to + WINDOW, lanes] = attended.astype(BF16)


def pooled_rows(chan, centre, first_pos, seq_len, w_pool_ref, scale_ref):
    y = lax.axis_index(TP)
    length = chan.shape[0]
    sums = chan + pltpu.roll(chan, 1, 0)
    window_sum = sums
    for level in range(1, POOL_GROUPS):
        step = 2 ** (level - 1)
        sums = pltpu.roll(sums, step, 0) + pltpu.roll(sums, length - step, 0)
        window_sum = jnp.where(y >= level, sums, window_sum)
    half_width = jnp.left_shift(jnp.int32(1), y)
    rows = 2 * WINDOW
    row = lax.broadcasted_iota(jnp.int32, (rows, 1), 0)
    pos = row + jnp.where(row < WINDOW, first_pos[0], first_pos[1])
    count = jnp.minimum(pos + half_width, seq_len) - jnp.maximum(pos - half_width, 0)
    spread = centre(window_sum) / count.astype(F32) - centre(chan)
    pooled = jnp.dot(spread.astype(BF16), w_pool_ref[0], preferred_element_type=F32)
    return (pooled * scale_ref[...]).astype(BF16)


def inner_kernel(seq_len, *refs):
    tokens_refs = refs[: len(MASKS)]
    own_ref, other_ref, kv_ref, chan_ref, sink_ref, w_pool_ref, scale_ref = refs[len(MASKS) : -5]
    query_ref, attended_ref, pooled_ref, w_ref, band_ref = refs[-5:]
    rows, query_cols = query_ref.shape
    whole_weights(own_ref, other_ref, w_ref, own_ref.shape[3] - query_cols)
    query_ref[...] = projected(tokens_refs, w_ref, 0, query_cols)
    split_band(kv_ref[...], band_ref)
    for b in range(1, rows // WINDOW - 1):
        attend_block(
            query_ref[b * WINDOW : (b + 1) * WINDOW],
            0,
            False,
            seq_len,
            band_ref,
            (b - 1) * WINDOW,
            sink_ref,
            attended_ref,
            (b - 1) * WINDOW,
        )
    near = 2 * RIM
    chan = chan_ref[WINDOW - near : rows - WINDOW + near].astype(F32)
    offset = lax.axis_index(SP) * rows + WINDOW
    pooled_ref[...] = pooled_rows(
        chan, lambda a: a[near:-near], (offset, offset), seq_len, w_pool_ref, scale_ref
    )


def outer_kernel(
    seq_len,
    query_ref,
    kv_ref,
    chan_ref,
    inside_ref,
    outside_ref,
    sink_ref,
    w_pool_ref,
    scale_ref,
    attended_ref,
    pooled_ref,
    band_ref,
):
    rows = chan_ref.shape[0]
    offset = lax.axis_index(SP) * rows
    ahead = lax.axis_index(CORE) == 0
    inside, outside = inside_ref[...].astype(F32), outside_ref[...].astype(F32)
    before, after = jnp.where(ahead, outside, inside), jnp.where(ahead, inside, outside)

    split_band(
        jnp.concatenate(
            [
                before[:WINDOW],
                kv_ref[: 2 * WINDOW].astype(F32),
                kv_ref[rows - 2 * WINDOW :].astype(F32),
                after[:WINDOW],
            ]
        ),
        band_ref,
    )
    for edge, start in enumerate((0, rows - WINDOW)):
        attend_block(
            query_ref[start : start + WINDOW],
            offset + start - WINDOW,
            True,
            seq_len,
            band_ref,
            edge * 3 * WINDOW,
            sink_ref,
            attended_ref,
            edge * WINDOW,
        )

    def rim(packed):
        return jnp.concatenate([packed[WINDOW : WINDOW + RIM], packed[WINDOW + RIM :]], axis=1)

    near = 2 * RIM
    first = chan_ref[: WINDOW + near].astype(F32)
    last = chan_ref[rows - WINDOW - near :].astype(F32)
    chan = jnp.concatenate([rim(before), first, last, rim(after)])

    def centre(a):
        return jnp.concatenate([a[RIM : RIM + WINDOW], a[-RIM - WINDOW : -RIM]])

    pooled_ref[...] = pooled_rows(
        chan, centre, (offset, offset + rows - 2 * WINDOW), seq_len, w_pool_ref, scale_ref
    )


def out_kernel(mask, count, *refs):
    mixed_refs, (own_ref, other_ref, out_ref, hidden_ref, w_ref) = refs[: 2 * count], refs[2 * count :]
    to = lax.axis_index(TP) ^ mask
    zs = own_ref.shape[1] // lax.axis_size(TP)
    at = own_ref.shape[3] - hidden_ref.shape[1]
    mine = pl.ds(to * zs, zs)
    whole_weights(own_ref.at[:, mine], other_ref.at[:, mine], w_ref, at)
    for part in range(count):
        attended_ref, pooled_ref = mixed_refs[2 * part : 2 * part + 2]
        rows, query_cols = attended_ref.shape
        here = slice(part * rows, (part + 1) * rows)
        hidden_ref[here, :query_cols] = attended_ref[...]
        hidden_ref[here, query_cols:] = pooled_ref[...]
    out_ref[...] = lax.dot_general(
        hidden_ref[...], w_ref[...], nt, preferred_element_type=F32
    ).astype(BF16)


VMEM = pl.BlockSpec(memory_space=pltpu.VMEM)
SMEM = pl.BlockSpec(memory_space=pltpu.SMEM)
LIMIT = pltpu.CompilerParams(vmem_limit_bytes=20 * 1024 * 1024)


def layer(
    tokens,
    w_query,
    w_key,
    w_value,
    w_pool_in,
    sink,
    w_pool,
    pool_scale,
    w_out_attn,
    w_out_pool,
    out_gain,
):
    rows = tokens.shape[0]
    seq_len = rows * lax.axis_size(SP)
    query_cols, key_cols, chan_cols = w_query.shape[1], w_key.shape[1], w_pool_in.shape[1]
    in_cols = 2 * key_cols + chan_cols + query_cols
    hidden_cols = query_cols + chan_cols
    share = out_gain.shape[0]
    model_width = share * lax.axis_size(TP)

    gathered = [tokens]
    for mask in MASKS[1:]:
        gathered.append(exchanged(tokens, TP, mask))
    packed = jnp.concatenate(
        (w_key, w_value, w_pool_in, w_query, w_out_attn.T, w_out_pool.T), axis=1
    )
    over_z = lax.all_gather(packed, Z, axis=0)
    over_x = from_everyone(over_z, X)
    own1, own2 = over_x[..., :in_cols], over_x[..., in_cols:]
    other1 = swapped(own1)
    other2 = swapped(own2)

    def rows_of(width, count=rows):
        return jax.ShapeDtypeStruct((count, width), BF16)

    def cost(flops, size):
        return pl.CostEstimate(flops=flops, bytes_accessed=size, transcendentals=0)

    rim_shape = rows_of(PAIR, WINDOW + 2 * RIM)
    kv, chan, inside, outside = pl.pallas_call(
        project_kernel,
        out_shape=[rows_of(2 * key_cols), rows_of(chan_cols), rim_shape, rim_shape],
        in_specs=[VMEM] * 6,
        out_specs=[VMEM] * 4,
        scratch_shapes=[pltpu.VMEM((model_width, 2 * key_cols + chan_cols), BF16)],
        compiler_params=LIMIT,
        cost_estimate=cost(2 * rows * model_width * (in_cols - query_cols), 4 << 20),
        name="project",
    )(*gathered, own1, other1)
    inside, outside = neighbours(inside, outside)
    half = rows // 2
    scale = pool_scale.reshape(1, -1)
    query, *inner = pl.pallas_call(
        functools.partial(inner_kernel, seq_len),
        out_shape=[rows_of(query_cols), rows_of(query_cols, half), rows_of(chan_cols, half)],
        in_specs=[VMEM] * 8 + [SMEM] + [VMEM] * 2,
        out_specs=[VMEM] * 3,
        scratch_shapes=[
            pltpu.VMEM((model_width, query_cols), BF16),
            pltpu.VMEM((4, rows, PAIR), BF16),
        ],
        compiler_params=LIMIT,
        cost_estimate=cost(2 * rows * model_width * query_cols, 4 << 20),
        name="inner",
    )(*gathered, own1, other1, kv, chan, sink, w_pool, scale)
    outer = pl.pallas_call(
        functools.partial(outer_kernel, seq_len),
        out_shape=[rows_of(query_cols, half), rows_of(chan_cols, half)],
        in_specs=[VMEM] * 5 + [SMEM] + [VMEM] * 2,
        out_specs=[VMEM] * 2,
        scratch_shapes=[pltpu.VMEM((4, 6 * WINDOW, PAIR), BF16)],
        compiler_params=LIMIT,
        cost_estimate=cost(2 * rows * model_width * query_cols, 2 << 20),
        name="outer",
    )(query, kv, chan, inside, outside, sink, w_pool, scale)

    def multiplied(mask, *mixed):
        count = len(mixed)
        return pl.pallas_call(
            functools.partial(out_kernel, mask, count),
            out_shape=rows_of(share, count * half),
            in_specs=[VMEM] * (2 * count + 2),
            out_specs=VMEM,
            scratch_shapes=[
                pltpu.VMEM((count * half, hidden_cols), BF16),
                pltpu.VMEM((share, hidden_cols), BF16),
            ],
            compiler_params=LIMIT,
            cost_estimate=cost(2 * count * half * share * hidden_cols, 1 << 20),
        )(*(a for pair in mixed for a in pair), own2, other2)

    def sent(mask, *mixed):
        block = multiplied(mask, *mixed)
        return exchanged(block, TP, mask)

    far = jnp.concatenate([sent(2, inner), sent(2, outer)])
    partials = [sent(1, inner, outer), sent(3, inner, outer), far]
    mix = multiplied(0, inner, outer).astype(F32)
    for partial in partials:
        mix = mix + partial.astype(F32)
    stats = jnp.stack([jnp.sum(mix, axis=1), jnp.sum(mix * mix, axis=1)])
    stats = of_everyone(stats, TP)
    row_mean = stats[0] / model_width
    variance = stats[1] / model_width - row_mean * row_mean
    normed = (mix - row_mean[:, None]) * lax.rsqrt(variance + epsilon)[:, None] * out_gain
    normed = normed.astype(BF16)
    return jnp.concatenate([normed[half : half + WINDOW], normed[:half], normed[half + WINDOW :]])


def solution(mesh):
    finer = Mesh(mesh.devices.reshape(16, 4, 2, mesh.shape["tp"]), ("sp_0", "sp_1", "sp_2", "tp"))
    return jax.shard_map(
        layer,
        mesh=finer,
        in_specs=(
            P(SP, "tp"),
            P(SP, "tp"),
            P(SP, "tp"),
            P(SP, "tp"),
            P(SP, "tp"),
            P("tp"),
            P("tp", None, None),
            P("tp"),
            P("tp", SP),
            P("tp", SP),
            P("tp"),
        ),
        out_specs=P(SP, "tp"),
        check_vma=False,
    )
```

```python
import functools

import jax
import jax.numpy as jnp
from jax import lax
from jax.experimental import pallas as pl
from jax.experimental.pallas import tpu as pltpu
from jax.sharding import Mesh
from jax.sharding import PartitionSpec as P


HEAD_DIM = 64
PAIR = 2 * HEAD_DIM
POOL_GROUPS = 4
RIM = 2 ** (POOL_GROUPS - 1)
WINDOW = 128
SP = ("sp_0", "sp_1", "sp_2")
Z, X, CORE = SP
TP = "tp"
BF16, F32 = jnp.bfloat16, jnp.float32

epsilon = 1e-05
masked_score = -1e30
nt = (((1,), (1,)), ((), ()))


def from_everyone(shard, axis):
    count = lax.axis_size(axis)
    return lax.all_to_all(
        jnp.broadcast_to(shard[None], (count, *shard.shape)), axis, 0, 0, tiled=True
    )


def of_everyone(shard, axis):
    return jnp.sum(from_everyone(shard, axis), axis=0)


def swapped(shard):
    return lax.ppermute(shard, CORE, [(0, 1), (1, 0)])


def neighbours(inside, outside):
    count = lax.axis_size(SP)
    pairs = [(i, i + 1) for i in range(1, count - 1, 2)]
    return swapped(inside), lax.ppermute(outside, SP, pairs + [(b, a) for a, b in pairs])


def whole_weights(own_ref, other_ref, w_ref, at):
    core = lax.axis_index(CORE)
    xs, zs, rows = own_ref.shape[:3]
    lanes = slice(at, at + w_ref.shape[1])
    for z in range(zs):
        for x in range(xs):
            base = (z * xs + x) * 2 * rows
            w_ref[pl.ds(pl.multiple_of(base + core * rows, rows), rows), :] = own_ref[
                x, z, :, lanes
            ]
            w_ref[pl.ds(pl.multiple_of(base + (1 - core) * rows, rows), rows), :] = other_ref[
                x, z, :, lanes
            ]


def projected(tokens_ref, w_ref, at, width):
    depth = tokens_ref.shape[2]
    total = None
    for p in range(tokens_ref.shape[0]):
        part = jnp.dot(
            tokens_ref[p],
            w_ref[p * depth : (p + 1) * depth, at : at + width],
            preferred_element_type=F32,
        )
        total = part if total is None else total + part
    return total.astype(BF16)


def copies_kernel(shard_ref, copies_ref, held_ref, read_sems, write_sems):
    count, chunks = copies_ref.shape[0], read_sems.shape[0]
    rows = shard_ref.shape[0] // chunks
    reads = [
        pltpu.make_async_copy(
            shard_ref.at[pl.ds(i * rows, rows)], held_ref.at[pl.ds(i * rows, rows)], read_sems.at[i]
        )
        for i in range(chunks)
    ]
    for read in reads:
        read.start()
    writes = []
    for i in range(chunks):
        reads[i].wait()
        here = pl.ds(i * rows, rows)
        for to in range(count):
            write = pltpu.make_async_copy(
                held_ref.at[here], copies_ref.at[to, here], write_sems.at[i, to]
            )
            write.start()
            writes.append(write)
    for write in writes:
        write.wait()


def project_kernel(
    tokens_ref, own_ref, other_ref, kv_ref, chan_ref, inside_ref, outside_ref, w_ref
):
    rows = tokens_ref.shape[1]
    whole_weights(own_ref, other_ref, w_ref, 0)
    kv_cols = kv_ref.shape[1]
    kv_ref[...] = projected(tokens_ref, w_ref, 0, kv_cols)
    chan_ref[...] = projected(tokens_ref, w_ref, kv_cols, chan_ref.shape[1])

    def rim(kv_at, chan_at):
        edge = chan_ref[chan_at : chan_at + RIM].astype(F32)
        kv = kv_ref[kv_at : kv_at + WINDOW].astype(F32)
        return jnp.concatenate([kv, edge[:, :PAIR], edge[:, PAIR:]])

    first, last = rim(0, 0), rim(rows - WINDOW, rows - RIM)
    ahead = lax.axis_index(CORE) == 0
    inside_ref[...] = jnp.where(ahead, last, first).astype(BF16)
    outside_ref[...] = jnp.where(ahead, first, last).astype(BF16)


def split_band(kv, band_ref):
    kv = kv.astype(F32)
    turned = pltpu.roll(kv, HEAD_DIM, 1)
    low = lax.broadcasted_iota(jnp.int32, kv.shape, 1) < HEAD_DIM
    band_ref[0] = jnp.where(low, kv, 0.0).astype(BF16)
    band_ref[1] = jnp.where(low, 0.0, turned).astype(BF16)
    band_ref[2] = jnp.where(low, turned, 0.0).astype(BF16)
    band_ref[3] = jnp.where(low, 0.0, kv).astype(BF16)


def attend_block(queries, band_ref, at, sink_ref, attended_ref, to):
    row = lax.broadcasted_iota(jnp.int32, (WINDOW, 3 * WINDOW), 0)
    col = lax.broadcasted_iota(jnp.int32, (WINDOW, 3 * WINDOW), 1)
    keep = (col >= row) & (col <= row + 2 * WINDOW)
    band = pl.ds(at, 3 * WINDOW)
    for pair in range(queries.shape[1] // PAIR):
        lanes = slice(pair * PAIR, (pair + 1) * PAIR)
        attended = jnp.zeros((WINDOW, PAIR), F32)
        for side in range(2):
            scores = lax.dot_general(
                queries[:, lanes], band_ref[side, band], nt, preferred_element_type=F32
            ) * HEAD_DIM ** (-0.5)
            scores = jnp.where(keep, scores, masked_score)
            sink = sink_ref[2 * pair + side]
            top = jnp.maximum(jnp.max(scores, axis=1, keepdims=True), sink)
            raised = jnp.exp(scores - top)
            total = jnp.sum(raised, axis=1, keepdims=True) + jnp.exp(sink - top)
            probs = (raised * (1.0 / total)).astype(BF16)
            attended += jnp.dot(probs, band_ref[2 + side, band], preferred_element_type=F32)
        attended_ref[to : to + WINDOW, lanes] = attended.astype(BF16)


def split_band_across(kv, keys_ref, values_ref):
    kv = kv.astype(F32)
    low = lax.broadcasted_iota(jnp.int32, kv.shape, 1) < HEAD_DIM
    keys_ref[0] = jnp.where(low, kv, 0.0).astype(BF16)
    keys_ref[1] = jnp.where(low, 0.0, pltpu.roll(kv, HEAD_DIM, 1)).astype(BF16)
    values_ref[...] = kv.T[HEAD_DIM:].astype(BF16)


def attend_edge(queries, has_before, has_after, keys_ref, values_ref, at, sink_ref, out_ref, to):
    key = lax.broadcasted_iota(jnp.int32, (WINDOW, WINDOW), 0)
    query = lax.broadcasted_iota(jnp.int32, (WINDOW, WINDOW), 1)
    band = pl.ds(at, 3 * WINDOW)
    keep_before, keep_after = (key >= query) & has_before, (key <= query) & has_after
    for pair in range(queries.shape[1] // PAIR):
        lanes = slice(pair * PAIR, (pair + 1) * PAIR)
        attended = []
        for side in range(2):
            scores = lax.dot_general(
                keys_ref[side, band], queries[:, lanes], nt, preferred_element_type=F32
            ) * HEAD_DIM ** (-0.5)
            thirds = (
                jnp.where(keep_before, scores[:WINDOW], masked_score),
                scores[WINDOW : 2 * WINDOW],
                jnp.where(keep_after, scores[2 * WINDOW :], masked_score),
            )
            sink = sink_ref[2 * pair + side]
            most = jnp.maximum(jnp.maximum(thirds[0], thirds[2]), thirds[1])
            top = jnp.maximum(jnp.max(most, axis=0, keepdims=True), sink)
            raised = [jnp.exp(third - top) for third in thirds]
            total = jnp.sum(raised[0] + raised[1] + raised[2], axis=0, keepdims=True)
            scale = 1.0 / (total + jnp.exp(sink - top))
            probs = jnp.concatenate([(third * scale).astype(BF16) for third in raised])
            attended.append(jnp.dot(values_ref[:, band], probs, preferred_element_type=F32))
        out_ref[to : to + WINDOW, lanes] = jnp.concatenate(attended).T.astype(BF16)


def pooled_rows(chan, centre, first_pos, seq_len, w_pool_ref, scale_ref):
    y = lax.axis_index(TP)
    length = chan.shape[0]
    sums = chan + pltpu.roll(chan, 1, 0)
    window_sum = sums
    for level in range(1, POOL_GROUPS):
        step = 2 ** (level - 1)
        sums = pltpu.roll(sums, step, 0) + pltpu.roll(sums, length - step, 0)
        window_sum = jnp.where(y >= level, sums, window_sum)
    half_width = jnp.left_shift(jnp.int32(1), y)
    rows = 2 * WINDOW
    row = lax.broadcasted_iota(jnp.int32, (rows, 1), 0)
    pos = row + jnp.where(row < WINDOW, first_pos[0], first_pos[1])
    count = jnp.minimum(pos + half_width, seq_len) - jnp.maximum(pos - half_width, 0)
    spread = centre(window_sum) / count.astype(F32) - centre(chan)
    pooled = jnp.dot(spread.astype(BF16), w_pool_ref[0], preferred_element_type=F32)
    return (pooled * scale_ref[...]).astype(BF16)


def inner_kernel(
    seq_len,
    tokens_ref,
    own_ref,
    other_ref,
    kv_ref,
    chan_ref,
    sink_ref,
    w_pool_ref,
    scale_ref,
    query_ref,
    attended_ref,
    pooled_ref,
    w_ref,
    band_ref,
):
    rows, query_cols = query_ref.shape
    whole_weights(own_ref, other_ref, w_ref, own_ref.shape[3] - query_cols)
    query_ref[...] = projected(tokens_ref, w_ref, 0, query_cols)
    split_band(kv_ref[...], band_ref)
    for b in range(1, rows // WINDOW - 1):
        attend_block(
            query_ref[b * WINDOW : (b + 1) * WINDOW],
            band_ref,
            (b - 1) * WINDOW,
            sink_ref,
            attended_ref,
            (b - 1) * WINDOW,
        )
    near = 2 * RIM
    chan = chan_ref[WINDOW - near : rows - WINDOW + near].astype(F32)
    offset = lax.axis_index(SP) * rows + WINDOW
    pooled_ref[...] = pooled_rows(
        chan, lambda a: a[near:-near], (offset, offset), seq_len, w_pool_ref, scale_ref
    )


def outer_kernel(
    seq_len,
    query_ref,
    kv_ref,
    chan_ref,
    inside_ref,
    outside_ref,
    sink_ref,
    w_pool_ref,
    scale_ref,
    attended_ref,
    pooled_ref,
    keys_ref,
    values_ref,
):
    rows = chan_ref.shape[0]
    offset = lax.axis_index(SP) * rows
    ahead = lax.axis_index(CORE) == 0
    inside, outside = inside_ref[...].astype(F32), outside_ref[...].astype(F32)
    before, after = jnp.where(ahead, outside, inside), jnp.where(ahead, inside, outside)

    split_band_across(
        jnp.concatenate(
            [
                before[:WINDOW],
                kv_ref[: 2 * WINDOW].astype(F32),
                kv_ref[rows - 2 * WINDOW :].astype(F32),
                after[:WINDOW],
            ]
        ),
        keys_ref,
        values_ref,
    )
    for edge, start in enumerate((0, rows - WINDOW)):
        attend_edge(
            query_ref[start : start + WINDOW],
            offset + start > 0,
            offset + start + WINDOW < seq_len,
            keys_ref,
            values_ref,
            edge * 3 * WINDOW,
            sink_ref,
            attended_ref,
            edge * WINDOW,
        )

    def rim(packed):
        return jnp.concatenate([packed[WINDOW : WINDOW + RIM], packed[WINDOW + RIM :]], axis=1)

    near = 2 * RIM
    first = chan_ref[: WINDOW + near].astype(F32)
    last = chan_ref[rows - WINDOW - near :].astype(F32)
    chan = jnp.concatenate([rim(before), first, last, rim(after)])

    def centre(a):
        return jnp.concatenate([a[RIM : RIM + WINDOW], a[-RIM - WINDOW : -RIM]])

    pooled_ref[...] = pooled_rows(
        chan, centre, (offset, offset + rows - 2 * WINDOW), seq_len, w_pool_ref, scale_ref
    )


def out_kernel(mask, count, *refs):
    mixed_refs, (own_ref, other_ref, out_ref, hidden_ref, w_ref) = refs[: 2 * count], refs[2 * count :]
    to = lax.axis_index(TP) ^ mask
    zs = own_ref.shape[1] // lax.axis_size(TP)
    at = own_ref.shape[3] - hidden_ref.shape[1]
    mine = pl.ds(to * zs, zs)
    whole_weights(own_ref.at[:, mine], other_ref.at[:, mine], w_ref, at)
    for part in range(count):
        attended_ref, pooled_ref = mixed_refs[2 * part : 2 * part + 2]
        rows, query_cols = attended_ref.shape
        here = slice(part * rows, (part + 1) * rows)
        hidden_ref[here, :query_cols] = attended_ref[...]
        hidden_ref[here, query_cols:] = pooled_ref[...]
    out_ref[...] = lax.dot_general(
        hidden_ref[...], w_ref[...], nt, preferred_element_type=F32
    ).astype(BF16)


VMEM = pl.BlockSpec(memory_space=pltpu.VMEM)
SMEM = pl.BlockSpec(memory_space=pltpu.SMEM)
ANY = pl.BlockSpec(memory_space=pl.ANY)
LIMIT = pltpu.CompilerParams(vmem_limit_bytes=20 * 1024 * 1024)


def layer(
    tokens,
    w_query,
    w_key,
    w_value,
    w_pool_in,
    sink,
    w_pool,
    pool_scale,
    w_out_attn,
    w_out_pool,
    out_gain,
):
    rows = tokens.shape[0]
    seq_len = rows * lax.axis_size(SP)
    query_cols, key_cols, chan_cols = w_query.shape[1], w_key.shape[1], w_pool_in.shape[1]
    in_cols = 2 * key_cols + chan_cols + query_cols
    hidden_cols = query_cols + chan_cols
    share = out_gain.shape[0]
    model_width = share * lax.axis_size(TP)

    count, chunks = lax.axis_size(TP), 4
    copies = pl.pallas_call(
        copies_kernel,
        out_shape=jax.ShapeDtypeStruct((count, *tokens.shape), BF16),
        in_specs=[ANY],
        out_specs=ANY,
        scratch_shapes=[
            pltpu.VMEM(tokens.shape, BF16),
            pltpu.SemaphoreType.DMA((chunks,)),
            pltpu.SemaphoreType.DMA((chunks, count)),
        ],
        cost_estimate=pl.CostEstimate(
            flops=0, bytes_accessed=5 * tokens.size * 2, transcendentals=0
        ),
        name="copies",
    )(tokens)
    gathered = lax.all_to_all(copies, TP, 0, 0, tiled=True)
    packed = jnp.concatenate(
        (w_key, w_value, w_pool_in, w_query, w_out_attn.T, w_out_pool.T), axis=1
    )
    over_z = lax.all_gather(packed, Z, axis=0)
    over_x = from_everyone(over_z, X)
    own1, own2 = over_x[..., :in_cols], over_x[..., in_cols:]
    other1 = swapped(own1)
    other2 = swapped(own2)

    def rows_of(width, count=rows):
        return jax.ShapeDtypeStruct((count, width), BF16)

    def cost(flops, size):
        return pl.CostEstimate(flops=flops, bytes_accessed=size, transcendentals=0)

    rim_shape = rows_of(PAIR, WINDOW + 2 * RIM)
    kv, chan, inside, outside = pl.pallas_call(
        project_kernel,
        out_shape=[rows_of(2 * key_cols), rows_of(chan_cols), rim_shape, rim_shape],
        in_specs=[VMEM] * 3,
        out_specs=[VMEM] * 4,
        scratch_shapes=[pltpu.VMEM((model_width, 2 * key_cols + chan_cols), BF16)],
        compiler_params=LIMIT,
        cost_estimate=cost(2 * rows * model_width * (in_cols - query_cols), 4 << 20),
        name="project",
    )(gathered, own1, other1)
    inside, outside = neighbours(inside, outside)
    half = rows // 2
    scale = pool_scale.reshape(1, -1)
    query, *inner = pl.pallas_call(
        functools.partial(inner_kernel, seq_len),
        out_shape=[rows_of(query_cols), rows_of(query_cols, half), rows_of(chan_cols, half)],
        in_specs=[VMEM] * 5 + [SMEM] + [VMEM] * 2,
        out_specs=[VMEM] * 3,
        scratch_shapes=[
            pltpu.VMEM((model_width, query_cols), BF16),
            pltpu.VMEM((4, rows, PAIR), BF16),
        ],
        compiler_params=LIMIT,
        cost_estimate=cost(2 * rows * model_width * query_cols, 4 << 20),
        name="inner",
    )(gathered, own1, other1, kv, chan, sink, w_pool, scale)
    outer = pl.pallas_call(
        functools.partial(outer_kernel, seq_len),
        out_shape=[rows_of(query_cols, half), rows_of(chan_cols, half)],
        in_specs=[VMEM] * 5 + [SMEM] + [VMEM] * 2,
        out_specs=[VMEM] * 2,
        scratch_shapes=[
            pltpu.VMEM((2, 6 * WINDOW, PAIR), BF16),
            pltpu.VMEM((HEAD_DIM, 6 * WINDOW), BF16),
        ],
        compiler_params=LIMIT,
        cost_estimate=cost(2 * rows * model_width * query_cols, 2 << 20),
        name="outer",
    )(query, kv, chan, inside, outside, sink, w_pool, scale)

    def multiplied(mask, *mixed):
        count = len(mixed)
        return pl.pallas_call(
            functools.partial(out_kernel, mask, count),
            out_shape=rows_of(share, count * half),
            in_specs=[VMEM] * (2 * count + 2),
            out_specs=VMEM,
            scratch_shapes=[
                pltpu.VMEM((count * half, hidden_cols), BF16),
                pltpu.VMEM((share, hidden_cols), BF16),
            ],
            compiler_params=LIMIT,
            cost_estimate=cost(2 * count * half * share * hidden_cols, 1 << 20),
        )(*(a for pair in mixed for a in pair), own2, other2)

    def sent(mask, *mixed):
        block = multiplied(mask, *mixed)
        count = lax.axis_size(TP)
        return lax.ppermute(block, TP, [(i, i ^ mask) for i in range(count)])

    far = jnp.concatenate([sent(2, inner), sent(2, outer)])
    partials = [sent(1, inner, outer), sent(3, inner, outer), far]
    mix = multiplied(0, inner, outer).astype(F32)
    for partial in partials:
        mix = mix + partial.astype(F32)
    stats = jnp.stack([jnp.sum(mix, axis=1), jnp.sum(mix * mix, axis=1)])
    stats = of_everyone(stats, TP)
    row_mean = stats[0] / model_width
    variance = stats[1] / model_width - row_mean * row_mean
    normed = (mix - row_mean[:, None]) * lax.rsqrt(variance + epsilon)[:, None] * out_gain
    normed = normed.astype(BF16)
    return jnp.concatenate([normed[half : half + WINDOW], normed[:half], normed[half + WINDOW :]])


def solution(mesh):
    finer = Mesh(mesh.devices.reshape(16, 4, 2, mesh.shape["tp"]), ("sp_0", "sp_1", "sp_2", "tp"))
    return jax.shard_map(
        layer,
        mesh=finer,
        in_specs=(
            P(SP, "tp"),
            P(SP, "tp"),
            P(SP, "tp"),
            P(SP, "tp"),
            P(SP, "tp"),
            P("tp"),
            P("tp", None, None),
            P("tp"),
            P("tp", SP),
            P("tp", SP),
            P("tp"),
        ),
        out_specs=P(SP, "tp"),
        check_vma=False,
    )
```

```python
import functools

import jax
import jax.numpy as jnp
from jax import lax
from jax.experimental import pallas as pl
from jax.experimental.pallas import tpu as pltpu
from jax.sharding import Mesh
from jax.sharding import PartitionSpec as P


HEAD_DIM = 64
PAIR = 2 * HEAD_DIM
POOL_GROUPS = 4
RIM = 2 ** (POOL_GROUPS - 1)
WINDOW = 128
SP = ("sp_0", "sp_1", "sp_2")
Z, X, CORE = SP
TP = "tp"
BF16, F32 = jnp.bfloat16, jnp.float32

epsilon = 1e-05
masked_score = -1e30
nt = (((1,), (1,)), ((), ()))


def from_everyone(shard, axis):
    count = lax.axis_size(axis)
    return lax.all_to_all(
        jnp.broadcast_to(shard[None], (count, *shard.shape)), axis, 0, 0, tiled=True
    )


def of_everyone(shard, axis):
    return jnp.sum(from_everyone(shard, axis), axis=0)


def swapped(shard):
    return lax.ppermute(shard, CORE, [(0, 1), (1, 0)])


def neighbours(inside, outside):
    count = lax.axis_size(SP)
    pairs = [(i, i + 1) for i in range(1, count - 1, 2)]
    return swapped(inside), lax.ppermute(outside, SP, pairs + [(b, a) for a, b in pairs])


def whole_weights(own_ref, other_ref, w_ref, at):
    core = lax.axis_index(CORE)
    xs, zs, rows = own_ref.shape[:3]
    lanes = slice(at, at + w_ref.shape[1])
    for z in range(zs):
        for x in range(xs):
            base = (z * xs + x) * 2 * rows
            w_ref[pl.ds(pl.multiple_of(base + core * rows, rows), rows), :] = own_ref[
                x, z, :, lanes
            ]
            w_ref[pl.ds(pl.multiple_of(base + (1 - core) * rows, rows), rows), :] = other_ref[
                x, z, :, lanes
            ]


def projected(tokens_ref, w_ref, at, width):
    depth = tokens_ref.shape[2]
    total = None
    for p in range(tokens_ref.shape[0]):
        part = jnp.dot(
            tokens_ref[p],
            w_ref[p * depth : (p + 1) * depth, at : at + width],
            preferred_element_type=F32,
        )
        total = part if total is None else total + part
    return total.astype(BF16)


def copies_kernel(shard_ref, copies_ref, held_ref, read_sems, write_sems):
    count, chunks = copies_ref.shape[0], read_sems.shape[0]
    rows = shard_ref.shape[0] // chunks
    reads = [
        pltpu.make_async_copy(
            shard_ref.at[pl.ds(i * rows, rows)], held_ref.at[pl.ds(i * rows, rows)], read_sems.at[i]
        )
        for i in range(chunks)
    ]
    for read in reads:
        read.start()
    writes = []
    for i in range(chunks):
        reads[i].wait()
        here = pl.ds(i * rows, rows)
        for to in range(count):
            write = pltpu.make_async_copy(
                held_ref.at[here], copies_ref.at[to, here], write_sems.at[i, to]
            )
            write.start()
            writes.append(write)
    for write in writes:
        write.wait()


def project_kernel(
    tokens_ref, own_ref, other_ref, kv_ref, chan_ref, inside_ref, outside_ref, w_ref
):
    rows = tokens_ref.shape[1]
    whole_weights(own_ref, other_ref, w_ref, 0)
    kv_cols = kv_ref.shape[1]
    kv_ref[...] = projected(tokens_ref, w_ref, 0, kv_cols)
    chan_ref[...] = projected(tokens_ref, w_ref, kv_cols, chan_ref.shape[1])

    def rim(kv_at, chan_at):
        edge = chan_ref[chan_at : chan_at + RIM].astype(F32)
        kv = kv_ref[kv_at : kv_at + WINDOW].astype(F32)
        return jnp.concatenate([kv, edge[:, :PAIR], edge[:, PAIR:]])

    first, last = rim(0, 0), rim(rows - WINDOW, rows - RIM)
    ahead = lax.axis_index(CORE) == 0
    inside_ref[...] = jnp.where(ahead, last, first).astype(BF16)
    outside_ref[...] = jnp.where(ahead, first, last).astype(BF16)


def split_band(kv, band_ref):
    kv = kv.astype(F32)
    turned = pltpu.roll(kv, HEAD_DIM, 1)
    low = lax.broadcasted_iota(jnp.int32, kv.shape, 1) < HEAD_DIM
    band_ref[0] = jnp.where(low, kv, 0.0).astype(BF16)
    band_ref[1] = jnp.where(low, 0.0, turned).astype(BF16)
    band_ref[2] = jnp.where(low, turned, 0.0).astype(BF16)
    band_ref[3] = jnp.where(low, 0.0, kv).astype(BF16)


def attend_block(queries, band_ref, at, sink_ref, attended_ref, to):
    row = lax.broadcasted_iota(jnp.int32, (WINDOW, 3 * WINDOW), 0)
    col = lax.broadcasted_iota(jnp.int32, (WINDOW, 3 * WINDOW), 1)
    keep = (col >= row) & (col <= row + 2 * WINDOW)
    band = pl.ds(at, 3 * WINDOW)
    for pair in range(queries.shape[1] // PAIR):
        lanes = slice(pair * PAIR, (pair + 1) * PAIR)
        attended = jnp.zeros((WINDOW, PAIR), F32)
        for side in range(2):
            scores = lax.dot_general(
                queries[:, lanes], band_ref[side, band], nt, preferred_element_type=F32
            ) * HEAD_DIM ** (-0.5)
            scores = jnp.where(keep, scores, masked_score)
            sink = sink_ref[2 * pair + side]
            top = jnp.maximum(jnp.max(scores, axis=1, keepdims=True), sink)
            raised = jnp.exp(scores - top)
            total = jnp.sum(raised, axis=1, keepdims=True) + jnp.exp(sink - top)
            probs = (raised * (1.0 / total)).astype(BF16)
            attended += jnp.dot(probs, band_ref[2 + side, band], preferred_element_type=F32)
        attended_ref[to : to + WINDOW, lanes] = attended.astype(BF16)


def split_band_across(kv, keys_ref, values_ref):
    kv = kv.astype(F32)
    low = lax.broadcasted_iota(jnp.int32, kv.shape, 1) < HEAD_DIM
    keys_ref[0] = jnp.where(low, kv, 0.0).astype(BF16)
    keys_ref[1] = jnp.where(low, 0.0, pltpu.roll(kv, HEAD_DIM, 1)).astype(BF16)
    values_ref[...] = kv.T[HEAD_DIM:].astype(BF16)


def attend_edge(queries, has_before, has_after, keys_ref, values_ref, at, sink_ref, out_ref, to):
    key = lax.broadcasted_iota(jnp.int32, (WINDOW, WINDOW), 0)
    query = lax.broadcasted_iota(jnp.int32, (WINDOW, WINDOW), 1)
    band = pl.ds(at, 3 * WINDOW)
    keep_before, keep_after = (key >= query) & has_before, (key <= query) & has_after
    for pair in range(queries.shape[1] // PAIR):
        lanes = slice(pair * PAIR, (pair + 1) * PAIR)
        attended = []
        for side in range(2):
            scores = lax.dot_general(
                keys_ref[side, band], queries[:, lanes], nt, preferred_element_type=F32
            ) * HEAD_DIM ** (-0.5)
            thirds = (
                jnp.where(keep_before, scores[:WINDOW], masked_score),
                scores[WINDOW : 2 * WINDOW],
                jnp.where(keep_after, scores[2 * WINDOW :], masked_score),
            )
            sink = sink_ref[2 * pair + side]
            most = jnp.maximum(jnp.maximum(thirds[0], thirds[2]), thirds[1])
            top = jnp.maximum(jnp.max(most, axis=0, keepdims=True), sink)
            raised = [jnp.exp(third - top) for third in thirds]
            total = jnp.sum(raised[0] + raised[1] + raised[2], axis=0, keepdims=True)
            scale = 1.0 / (total + jnp.exp(sink - top))
            probs = jnp.concatenate([(third * scale).astype(BF16) for third in raised])
            attended.append(jnp.dot(values_ref[:, band], probs, preferred_element_type=F32))
        out_ref[to : to + WINDOW, lanes] = jnp.concatenate(attended).T.astype(BF16)


def pooled_rows(chan, centre, first_pos, seq_len, w_pool_ref, scale_ref):
    y = lax.axis_index(TP)
    length = chan.shape[0]
    sums = chan + pltpu.roll(chan, 1, 0)
    window_sum = sums
    for level in range(1, POOL_GROUPS):
        step = 2 ** (level - 1)
        sums = pltpu.roll(sums, step, 0) + pltpu.roll(sums, length - step, 0)
        window_sum = jnp.where(y >= level, sums, window_sum)
    half_width = jnp.left_shift(jnp.int32(1), y)
    rows = 2 * WINDOW
    row = lax.broadcasted_iota(jnp.int32, (rows, 1), 0)
    pos = row + jnp.where(row < WINDOW, first_pos[0], first_pos[1])
    count = jnp.minimum(pos + half_width, seq_len) - jnp.maximum(pos - half_width, 0)
    spread = centre(window_sum) / count.astype(F32) - centre(chan)
    pooled = jnp.dot(spread.astype(BF16), w_pool_ref[0], preferred_element_type=F32)
    return (pooled * scale_ref[...]).astype(BF16)


def inner_kernel(
    seq_len,
    tokens_ref,
    own_ref,
    other_ref,
    kv_ref,
    chan_ref,
    sink_ref,
    w_pool_ref,
    scale_ref,
    query_ref,
    attended_ref,
    pooled_ref,
    w_ref,
    band_ref,
):
    rows, query_cols = kv_ref.shape[0], query_ref.shape[1]
    whole_weights(own_ref, other_ref, w_ref, own_ref.shape[3] - query_cols)
    split_band(kv_ref[...], band_ref)
    for b in (1, rows // WINDOW - 2, 0, rows // WINDOW - 1):
        here = slice(b * WINDOW, (b + 1) * WINDOW)
        queries = projected(tokens_ref.at[:, here], w_ref, 0, query_cols)
        if 0 < b < rows // WINDOW - 1:
            attend_block(
                queries, band_ref, (b - 1) * WINDOW, sink_ref, attended_ref, (b - 1) * WINDOW
            )
        else:
            query_ref[min(b, 1) * WINDOW : (min(b, 1) + 1) * WINDOW] = queries
    near = 2 * RIM
    chan = chan_ref[WINDOW - near : rows - WINDOW + near].astype(F32)
    offset = lax.axis_index(SP) * rows + WINDOW
    pooled_ref[...] = pooled_rows(
        chan, lambda a: a[near:-near], (offset, offset), seq_len, w_pool_ref, scale_ref
    )


def outer_kernel(
    seq_len,
    query_ref,
    kv_ref,
    chan_ref,
    inside_ref,
    outside_ref,
    sink_ref,
    w_pool_ref,
    scale_ref,
    attended_ref,
    pooled_ref,
    keys_ref,
    values_ref,
):
    rows = chan_ref.shape[0]
    offset = lax.axis_index(SP) * rows
    ahead = lax.axis_index(CORE) == 0
    inside, outside = inside_ref[...].astype(F32), outside_ref[...].astype(F32)
    before, after = jnp.where(ahead, outside, inside), jnp.where(ahead, inside, outside)

    split_band_across(
        jnp.concatenate(
            [
                before[:WINDOW],
                kv_ref[: 2 * WINDOW].astype(F32),
                kv_ref[rows - 2 * WINDOW :].astype(F32),
                after[:WINDOW],
            ]
        ),
        keys_ref,
        values_ref,
    )
    for edge, start in enumerate((0, rows - WINDOW)):
        attend_edge(
            query_ref[edge * WINDOW : (edge + 1) * WINDOW],
            offset + start > 0,
            offset + start + WINDOW < seq_len,
            keys_ref,
            values_ref,
            edge * 3 * WINDOW,
            sink_ref,
            attended_ref,
            edge * WINDOW,
        )

    def rim(packed):
        return jnp.concatenate([packed[WINDOW : WINDOW + RIM], packed[WINDOW + RIM :]], axis=1)

    near = 2 * RIM
    first = chan_ref[: WINDOW + near].astype(F32)
    last = chan_ref[rows - WINDOW - near :].astype(F32)
    chan = jnp.concatenate([rim(before), first, last, rim(after)])

    def centre(a):
        return jnp.concatenate([a[RIM : RIM + WINDOW], a[-RIM - WINDOW : -RIM]])

    pooled_ref[...] = pooled_rows(
        chan, centre, (offset, offset + rows - 2 * WINDOW), seq_len, w_pool_ref, scale_ref
    )


def out_kernel(mask, count, *refs):
    mixed_refs, (own_ref, other_ref, out_ref, hidden_ref, w_ref) = refs[: 2 * count], refs[2 * count :]
    to = lax.axis_index(TP) ^ mask
    zs = own_ref.shape[1] // lax.axis_size(TP)
    at = own_ref.shape[3] - hidden_ref.shape[1]
    mine = pl.ds(to * zs, zs)
    whole_weights(own_ref.at[:, mine], other_ref.at[:, mine], w_ref, at)
    for part in range(count):
        attended_ref, pooled_ref = mixed_refs[2 * part : 2 * part + 2]
        rows, query_cols = attended_ref.shape
        here = slice(part * rows, (part + 1) * rows)
        hidden_ref[here, :query_cols] = attended_ref[...]
        hidden_ref[here, query_cols:] = pooled_ref[...]
    out_ref[...] = lax.dot_general(
        hidden_ref[...], w_ref[...], nt, preferred_element_type=F32
    ).astype(BF16)


VMEM = pl.BlockSpec(memory_space=pltpu.VMEM)
SMEM = pl.BlockSpec(memory_space=pltpu.SMEM)
ANY = pl.BlockSpec(memory_space=pl.ANY)
LIMIT = pltpu.CompilerParams(vmem_limit_bytes=20 * 1024 * 1024)


def layer(
    tokens,
    w_query,
    w_key,
    w_value,
    w_pool_in,
    sink,
    w_pool,
    pool_scale,
    w_out_attn,
    w_out_pool,
    out_gain,
):
    rows = tokens.shape[0]
    seq_len = rows * lax.axis_size(SP)
    query_cols, key_cols, chan_cols = w_query.shape[1], w_key.shape[1], w_pool_in.shape[1]
    in_cols = 2 * key_cols + chan_cols + query_cols
    hidden_cols = query_cols + chan_cols
    share = out_gain.shape[0]
    model_width = share * lax.axis_size(TP)

    count, chunks = lax.axis_size(TP), 4
    copies = pl.pallas_call(
        copies_kernel,
        out_shape=jax.ShapeDtypeStruct((count, *tokens.shape), BF16),
        in_specs=[ANY],
        out_specs=ANY,
        scratch_shapes=[
            pltpu.VMEM(tokens.shape, BF16),
            pltpu.SemaphoreType.DMA((chunks,)),
            pltpu.SemaphoreType.DMA((chunks, count)),
        ],
        cost_estimate=pl.CostEstimate(
            flops=0, bytes_accessed=5 * tokens.size * 2, transcendentals=0
        ),
        name="copies",
    )(tokens)
    gathered = lax.all_to_all(copies, TP, 0, 0, tiled=True)
    packed = jnp.concatenate(
        (w_key, w_value, w_pool_in, w_query, w_out_attn.T, w_out_pool.T), axis=1
    )
    over_z = lax.all_gather(packed, Z, axis=0)
    over_x = from_everyone(over_z, X)
    own1, own2 = over_x[..., :in_cols], over_x[..., in_cols:]
    other1 = swapped(own1)
    other2 = swapped(own2)

    def rows_of(width, count=rows):
        return jax.ShapeDtypeStruct((count, width), BF16)

    def cost(flops, size):
        return pl.CostEstimate(flops=flops, bytes_accessed=size, transcendentals=0)

    rim_shape = rows_of(PAIR, WINDOW + 2 * RIM)
    kv, chan, inside, outside = pl.pallas_call(
        project_kernel,
        out_shape=[rows_of(2 * key_cols), rows_of(chan_cols), rim_shape, rim_shape],
        in_specs=[VMEM] * 3,
        out_specs=[VMEM] * 4,
        scratch_shapes=[pltpu.VMEM((model_width, 2 * key_cols + chan_cols), BF16)],
        compiler_params=LIMIT,
        cost_estimate=cost(2 * rows * model_width * (in_cols - query_cols), 4 << 20),
        name="project",
    )(gathered, own1, other1)
    inside, outside = neighbours(inside, outside)
    half = rows // 2
    scale = pool_scale.reshape(1, -1)
    query, *inner = pl.pallas_call(
        functools.partial(inner_kernel, seq_len),
        out_shape=[rows_of(query_cols, half), rows_of(query_cols, half), rows_of(chan_cols, half)],
        in_specs=[VMEM] * 5 + [SMEM] + [VMEM] * 2,
        out_specs=[VMEM] * 3,
        scratch_shapes=[
            pltpu.VMEM((model_width, query_cols), BF16),
            pltpu.VMEM((4, rows, PAIR), BF16),
        ],
        compiler_params=LIMIT,
        cost_estimate=cost(2 * rows * model_width * query_cols, 4 << 20),
        name="inner",
    )(gathered, own1, other1, kv, chan, sink, w_pool, scale)
    outer = pl.pallas_call(
        functools.partial(outer_kernel, seq_len),
        out_shape=[rows_of(query_cols, half), rows_of(chan_cols, half)],
        in_specs=[VMEM] * 5 + [SMEM] + [VMEM] * 2,
        out_specs=[VMEM] * 2,
        scratch_shapes=[
            pltpu.VMEM((2, 6 * WINDOW, PAIR), BF16),
            pltpu.VMEM((HEAD_DIM, 6 * WINDOW), BF16),
        ],
        compiler_params=LIMIT,
        cost_estimate=cost(2 * rows * model_width * query_cols, 2 << 20),
        name="outer",
    )(query, kv, chan, inside, outside, sink, w_pool, scale)

    def multiplied(mask, *mixed):
        count = len(mixed)
        return pl.pallas_call(
            functools.partial(out_kernel, mask, count),
            out_shape=rows_of(share, count * half),
            in_specs=[VMEM] * (2 * count + 2),
            out_specs=VMEM,
            scratch_shapes=[
                pltpu.VMEM((count * half, hidden_cols), BF16),
                pltpu.VMEM((share, hidden_cols), BF16),
            ],
            compiler_params=LIMIT,
            cost_estimate=cost(2 * count * half * share * hidden_cols, 1 << 20),
        )(*(a for pair in mixed for a in pair), own2, other2)

    def sent(mask, *mixed):
        block = multiplied(mask, *mixed)
        count = lax.axis_size(TP)
        return lax.ppermute(block, TP, [(i, i ^ mask) for i in range(count)])

    far = jnp.concatenate([sent(2, inner), sent(2, outer)])
    partials = [sent(1, inner, outer), sent(3, inner, outer), far]
    mix = multiplied(0, inner, outer).astype(F32)
    for partial in partials:
        mix = mix + partial.astype(F32)
    stats = jnp.stack([jnp.sum(mix, axis=1), jnp.sum(mix * mix, axis=1)])
    stats = of_everyone(stats, TP)
    row_mean = stats[0] / model_width
    variance = stats[1] / model_width - row_mean * row_mean
    normed = (mix - row_mean[:, None]) * lax.rsqrt(variance + epsilon)[:, None] * out_gain
    normed = normed.astype(BF16)
    return jnp.concatenate([normed[half : half + WINDOW], normed[:half], normed[half + WINDOW :]])


def solution(mesh):
    finer = Mesh(mesh.devices.reshape(16, 4, 2, mesh.shape["tp"]), ("sp_0", "sp_1", "sp_2", "tp"))
    return jax.shard_map(
        layer,
        mesh=finer,
        in_specs=(
            P(SP, "tp"),
            P(SP, "tp"),
            P(SP, "tp"),
            P(SP, "tp"),
            P(SP, "tp"),
            P("tp"),
            P("tp", None, None),
            P("tp"),
            P("tp", SP),
            P("tp", SP),
            P("tp"),
        ),
        out_specs=P(SP, "tp"),
        check_vma=False,
    )
```

```python
import functools

import jax
import jax.numpy as jnp
from jax import lax
from jax.experimental import pallas as pl
from jax.experimental.pallas import tpu as pltpu
from jax.sharding import Mesh
from jax.sharding import PartitionSpec as P


HEAD_DIM = 64
PAIR = 2 * HEAD_DIM
POOL_GROUPS = 4
RIM = 2 ** (POOL_GROUPS - 1)
WINDOW = 128
SP = ("sp_0", "sp_1", "sp_2")
Z, X, CORE = SP
TP = "tp"
BF16, F32 = jnp.bfloat16, jnp.float32

epsilon = 1e-05
masked_score = -1e30
nt = (((1,), (1,)), ((), ()))


def from_everyone(shard, axis):
    count = lax.axis_size(axis)
    return lax.all_to_all(
        jnp.broadcast_to(shard[None], (count, *shard.shape)), axis, 0, 0, tiled=True
    )


def of_everyone(shard, axis):
    return jnp.sum(from_everyone(shard, axis), axis=0)


def swapped(shard):
    return lax.ppermute(shard, CORE, [(0, 1), (1, 0)])


def neighbours(inside, outside):
    count = lax.axis_size(SP)
    pairs = [(i, i + 1) for i in range(1, count - 1, 2)]
    from_outside = lax.ppermute(outside, SP, pairs + [(b, a) for a, b in pairs])
    return swapped(inside), from_outside


def whole_weights(own_ref, other_ref, w_ref, at):
    core = lax.axis_index(CORE)
    xs, zs, rows = own_ref.shape[:3]
    lanes = slice(at, at + w_ref.shape[1])
    for z in range(zs):
        for x in range(xs):
            base = (z * xs + x) * 2 * rows
            w_ref[pl.ds(pl.multiple_of(base + core * rows, rows), rows), :] = own_ref[
                x, z, :, lanes
            ]
            w_ref[pl.ds(pl.multiple_of(base + (1 - core) * rows, rows), rows), :] = other_ref[
                x, z, :, lanes
            ]


def projected(tokens_ref, w_ref, at, width):
    depth = tokens_ref.shape[2]
    total = None
    for p in range(tokens_ref.shape[0]):
        part = jnp.dot(
            tokens_ref[p],
            w_ref[p * depth : (p + 1) * depth, at : at + width],
            preferred_element_type=F32,
        )
        total = part if total is None else total + part
    return total.astype(BF16)


def copies_kernel(shard_ref, copies_ref, held_ref, read_sems, write_sems):
    count, chunks = copies_ref.shape[0], read_sems.shape[0]
    rows = shard_ref.shape[0] // chunks
    reads = [
        pltpu.make_async_copy(
            shard_ref.at[pl.ds(i * rows, rows)], held_ref.at[pl.ds(i * rows, rows)], read_sems.at[i]
        )
        for i in range(chunks)
    ]
    for read in reads:
        read.start()
    writes = []
    for i in range(chunks):
        reads[i].wait()
        here = pl.ds(i * rows, rows)
        for to in range(count):
            write = pltpu.make_async_copy(
                held_ref.at[here], copies_ref.at[to, here], write_sems.at[i, to]
            )
            write.start()
            writes.append(write)
    for write in writes:
        write.wait()


def project_kernel(
    tokens_ref, own_ref, other_ref, kv_ref, chan_ref, inside_ref, outside_ref, w_ref
):
    rows = tokens_ref.shape[1]
    whole_weights(own_ref, other_ref, w_ref, 0)
    kv_cols = kv_ref.shape[1]
    kv_ref[...] = projected(tokens_ref, w_ref, 0, kv_cols)
    chan_ref[...] = projected(tokens_ref, w_ref, kv_cols, chan_ref.shape[1])

    def rim(kv_at, chan_at):
        edge = chan_ref[chan_at : chan_at + RIM].astype(F32)
        kv = kv_ref[kv_at : kv_at + WINDOW].astype(F32)
        return jnp.concatenate([kv, edge[:, :PAIR], edge[:, PAIR:]])

    first, last = rim(0, 0), rim(rows - WINDOW, rows - RIM)
    ahead = lax.axis_index(CORE) == 0
    inside_ref[...] = jnp.where(ahead, last, first).astype(BF16)
    outside_ref[...] = jnp.where(ahead, first, last).astype(BF16)


def split_band(kv, band_ref):
    kv = kv.astype(F32)
    turned = pltpu.roll(kv, HEAD_DIM, 1)
    low = lax.broadcasted_iota(jnp.int32, kv.shape, 1) < HEAD_DIM
    band_ref[0] = jnp.where(low, kv, 0.0).astype(BF16)
    band_ref[1] = jnp.where(low, 0.0, turned).astype(BF16)
    band_ref[2] = jnp.where(low, turned, 0.0).astype(BF16)
    band_ref[3] = jnp.where(low, 0.0, kv).astype(BF16)


def attend_block(queries, band_ref, at, sink_ref, attended_ref, to):
    row = lax.broadcasted_iota(jnp.int32, (WINDOW, 3 * WINDOW), 0)
    col = lax.broadcasted_iota(jnp.int32, (WINDOW, 3 * WINDOW), 1)
    keep = (col >= row) & (col <= row + 2 * WINDOW)
    band = pl.ds(at, 3 * WINDOW)
    for pair in range(queries.shape[1] // PAIR):
        lanes = slice(pair * PAIR, (pair + 1) * PAIR)
        attended = jnp.zeros((WINDOW, PAIR), F32)
        for side in range(2):
            scores = lax.dot_general(
                queries[:, lanes], band_ref[side, band], nt, preferred_element_type=F32
            ) * HEAD_DIM ** (-0.5)
            scores = jnp.where(keep, scores, masked_score)
            sink = sink_ref[2 * pair + side]
            top = jnp.maximum(jnp.max(scores, axis=1, keepdims=True), sink)
            raised = jnp.exp(scores - top)
            total = jnp.sum(raised, axis=1, keepdims=True) + jnp.exp(sink - top)
            probs = (raised * (1.0 / total)).astype(BF16)
            attended += jnp.dot(probs, band_ref[2 + side, band], preferred_element_type=F32)
        attended_ref[to : to + WINDOW, lanes] = attended.astype(BF16)


def split_band_across(kv, keys_ref, values_ref):
    kv = kv.astype(F32)
    low = lax.broadcasted_iota(jnp.int32, kv.shape, 1) < HEAD_DIM
    keys_ref[0] = jnp.where(low, kv, 0.0).astype(BF16)
    keys_ref[1] = jnp.where(low, 0.0, pltpu.roll(kv, HEAD_DIM, 1)).astype(BF16)
    values_ref[...] = kv.T[HEAD_DIM:].astype(BF16)


def attend_edge(queries, has_before, has_after, keys_ref, values_ref, at, sink_ref, out_ref, to):
    key = lax.broadcasted_iota(jnp.int32, (WINDOW, WINDOW), 0)
    query = lax.broadcasted_iota(jnp.int32, (WINDOW, WINDOW), 1)
    band = pl.ds(at, 3 * WINDOW)
    keep_before, keep_after = (key >= query) & has_before, (key <= query) & has_after
    for pair in range(queries.shape[1] // PAIR):
        lanes = slice(pair * PAIR, (pair + 1) * PAIR)
        attended = []
        for side in range(2):
            scores = lax.dot_general(
                keys_ref[side, band], queries[:, lanes], nt, preferred_element_type=F32
            ) * HEAD_DIM ** (-0.5)
            thirds = (
                jnp.where(keep_before, scores[:WINDOW], masked_score),
                scores[WINDOW : 2 * WINDOW],
                jnp.where(keep_after, scores[2 * WINDOW :], masked_score),
            )
            sink = sink_ref[2 * pair + side]
            most = jnp.maximum(jnp.maximum(thirds[0], thirds[2]), thirds[1])
            top = jnp.maximum(jnp.max(most, axis=0, keepdims=True), sink)
            raised = [jnp.exp(third - top) for third in thirds]
            total = jnp.sum(raised[0] + raised[1] + raised[2], axis=0, keepdims=True)
            scale = 1.0 / (total + jnp.exp(sink - top))
            probs = jnp.concatenate([(third * scale).astype(BF16) for third in raised])
            attended.append(jnp.dot(values_ref[:, band], probs, preferred_element_type=F32))
        out_ref[to : to + WINDOW, lanes] = jnp.concatenate(attended).T.astype(BF16)


def pooled_rows(chan, centre, first_pos, seq_len, w_pool_ref, scale_ref):
    y = lax.axis_index(TP)
    length = chan.shape[0]
    sums = chan + pltpu.roll(chan, 1, 0)
    window_sum = sums
    for level in range(1, POOL_GROUPS):
        step = 2 ** (level - 1)
        sums = pltpu.roll(sums, step, 0) + pltpu.roll(sums, length - step, 0)
        window_sum = jnp.where(y >= level, sums, window_sum)
    half_width = jnp.left_shift(jnp.int32(1), y)
    rows = 2 * WINDOW
    row = lax.broadcasted_iota(jnp.int32, (rows, 1), 0)
    pos = row + jnp.where(row < WINDOW, first_pos[0], first_pos[1])
    count = jnp.minimum(pos + half_width, seq_len) - jnp.maximum(pos - half_width, 0)
    spread = centre(window_sum) / count.astype(F32) - centre(chan)
    pooled = jnp.dot(spread.astype(BF16), w_pool_ref[0], preferred_element_type=F32)
    return (pooled * scale_ref[...]).astype(BF16)


def inner_kernel(
    seq_len,
    tokens_ref,
    own_ref,
    other_ref,
    kv_ref,
    chan_ref,
    sink_ref,
    w_pool_ref,
    scale_ref,
    query_ref,
    attended_ref,
    pooled_ref,
    w_ref,
    band_ref,
):
    rows, query_cols = query_ref.shape
    whole_weights(own_ref, other_ref, w_ref, own_ref.shape[3] - query_cols)
    split_band(kv_ref[...], band_ref)
    for b in (1, rows // WINDOW - 2, 0, rows // WINDOW - 1):
        here = slice(b * WINDOW, (b + 1) * WINDOW)
        queries = projected(tokens_ref.at[:, here], w_ref, 0, query_cols)
        query_ref[here] = queries
        if 0 < b < rows // WINDOW - 1:
            attend_block(
                queries, band_ref, (b - 1) * WINDOW, sink_ref, attended_ref, (b - 1) * WINDOW
            )
    near = 2 * RIM
    chan = chan_ref[WINDOW - near : rows - WINDOW + near].astype(F32)
    offset = lax.axis_index(SP) * rows + WINDOW
    pooled_ref[...] = pooled_rows(
        chan, lambda a: a[near:-near], (offset, offset), seq_len, w_pool_ref, scale_ref
    )


def outer_kernel(
    seq_len,
    query_ref,
    kv_ref,
    chan_ref,
    inside_ref,
    outside_ref,
    sink_ref,
    w_pool_ref,
    scale_ref,
    attended_ref,
    pooled_ref,
    keys_ref,
    values_ref,
):
    rows = chan_ref.shape[0]
    offset = lax.axis_index(SP) * rows
    ahead = lax.axis_index(CORE) == 0
    inside, outside = inside_ref[...].astype(F32), outside_ref[...].astype(F32)
    before, after = jnp.where(ahead, outside, inside), jnp.where(ahead, inside, outside)

    split_band_across(
        jnp.concatenate(
            [
                before[:WINDOW],
                kv_ref[: 2 * WINDOW].astype(F32),
                kv_ref[rows - 2 * WINDOW :].astype(F32),
                after[:WINDOW],
            ]
        ),
        keys_ref,
        values_ref,
    )
    for edge, start in enumerate((0, rows - WINDOW)):
        attend_edge(
            query_ref[start : start + WINDOW],
            offset + start > 0,
            offset + start + WINDOW < seq_len,
            keys_ref,
            values_ref,
            edge * 3 * WINDOW,
            sink_ref,
            attended_ref,
            edge * WINDOW,
        )

    def rim(packed):
        return jnp.concatenate([packed[WINDOW : WINDOW + RIM], packed[WINDOW + RIM :]], axis=1)

    near = 2 * RIM
    first = chan_ref[: WINDOW + near].astype(F32)
    last = chan_ref[rows - WINDOW - near :].astype(F32)
    chan = jnp.concatenate([rim(before), first, last, rim(after)])

    def centre(a):
        return jnp.concatenate([a[RIM : RIM + WINDOW], a[-RIM - WINDOW : -RIM]])

    pooled_ref[...] = pooled_rows(
        chan, centre, (offset, offset + rows - 2 * WINDOW), seq_len, w_pool_ref, scale_ref
    )


def out_kernel(mask, count, *refs):
    mixed_refs, (own_ref, other_ref, out_ref, hidden_ref, w_ref) = refs[: 2 * count], refs[2 * count :]
    to = lax.axis_index(TP) ^ mask
    zs = own_ref.shape[1] // lax.axis_size(TP)
    at = own_ref.shape[3] - hidden_ref.shape[1]
    mine = pl.ds(to * zs, zs)
    whole_weights(own_ref.at[:, mine], other_ref.at[:, mine], w_ref, at)
    for part in range(count):
        attended_ref, pooled_ref = mixed_refs[2 * part : 2 * part + 2]
        rows, query_cols = attended_ref.shape
        here = slice(part * rows, (part + 1) * rows)
        hidden_ref[here, :query_cols] = attended_ref[...]
        hidden_ref[here, query_cols:] = pooled_ref[...]
    out_ref[...] = lax.dot_general(
        hidden_ref[...], w_ref[...], nt, preferred_element_type=F32
    ).astype(BF16)


VMEM = pl.BlockSpec(memory_space=pltpu.VMEM)
SMEM = pl.BlockSpec(memory_space=pltpu.SMEM)
ANY = pl.BlockSpec(memory_space=pl.ANY)
LIMIT = pltpu.CompilerParams(vmem_limit_bytes=20 * 1024 * 1024)


def layer(
    tokens,
    w_query,
    w_key,
    w_value,
    w_pool_in,
    sink,
    w_pool,
    pool_scale,
    w_out_attn,
    w_out_pool,
    out_gain,
):
    rows = tokens.shape[0]
    seq_len = rows * lax.axis_size(SP)
    query_cols, key_cols, chan_cols = w_query.shape[1], w_key.shape[1], w_pool_in.shape[1]
    in_cols = 2 * key_cols + chan_cols + query_cols
    hidden_cols = query_cols + chan_cols
    share = out_gain.shape[0]
    model_width = share * lax.axis_size(TP)

    count, chunks = lax.axis_size(TP), 4
    copies = pl.pallas_call(
        copies_kernel,
        out_shape=jax.ShapeDtypeStruct((count, *tokens.shape), BF16),
        in_specs=[ANY],
        out_specs=ANY,
        scratch_shapes=[
            pltpu.VMEM(tokens.shape, BF16),
            pltpu.SemaphoreType.DMA((chunks,)),
            pltpu.SemaphoreType.DMA((chunks, count)),
        ],
        cost_estimate=pl.CostEstimate(
            flops=0, bytes_accessed=5 * tokens.size * 2, transcendentals=0
        ),
        name="copies",
    )(tokens)
    gathered = lax.all_to_all(copies, TP, 0, 0, tiled=True)
    packed = jnp.concatenate(
        (w_key, w_value, w_pool_in, w_query, w_out_attn.T, w_out_pool.T), axis=1
    )
    over_z = lax.all_gather(packed, Z, axis=0)
    over_x = from_everyone(over_z, X)
    own1, own2 = over_x[..., :in_cols], over_x[..., in_cols:]
    other1 = swapped(own1)
    other2 = swapped(own2)

    def rows_of(width, count=rows):
        return jax.ShapeDtypeStruct((count, width), BF16)

    def cost(flops, size):
        return pl.CostEstimate(flops=flops, bytes_accessed=size, transcendentals=0)

    rim_shape = rows_of(PAIR, WINDOW + 2 * RIM)
    kv, chan, inside, outside = pl.pallas_call(
        project_kernel,
        out_shape=[rows_of(2 * key_cols), rows_of(chan_cols), rim_shape, rim_shape],
        in_specs=[VMEM] * 3,
        out_specs=[VMEM] * 4,
        scratch_shapes=[pltpu.VMEM((model_width, 2 * key_cols + chan_cols), BF16)],
        compiler_params=LIMIT,
        cost_estimate=cost(2 * rows * model_width * (in_cols - query_cols), 4 << 20),
        name="project",
    )(gathered, own1, other1)
    inside, outside = neighbours(inside, outside)
    half = rows // 2
    scale = pool_scale.reshape(1, -1)
    query, *inner = pl.pallas_call(
        functools.partial(inner_kernel, seq_len),
        out_shape=[rows_of(query_cols), rows_of(query_cols, half), rows_of(chan_cols, half)],
        in_specs=[VMEM] * 5 + [SMEM] + [VMEM] * 2,
        out_specs=[VMEM] * 3,
        scratch_shapes=[
            pltpu.VMEM((model_width, query_cols), BF16),
            pltpu.VMEM((4, rows, PAIR), BF16),
        ],
        compiler_params=LIMIT,
        cost_estimate=cost(2 * rows * model_width * query_cols, 4 << 20),
        name="inner",
    )(gathered, own1, other1, kv, chan, sink, w_pool, scale)
    outer = pl.pallas_call(
        functools.partial(outer_kernel, seq_len),
        out_shape=[rows_of(query_cols, half), rows_of(chan_cols, half)],
        in_specs=[VMEM] * 5 + [SMEM] + [VMEM] * 2,
        out_specs=[VMEM] * 2,
        scratch_shapes=[
            pltpu.VMEM((2, 6 * WINDOW, PAIR), BF16),
            pltpu.VMEM((HEAD_DIM, 6 * WINDOW), BF16),
        ],
        compiler_params=LIMIT,
        cost_estimate=cost(2 * rows * model_width * query_cols, 2 << 20),
        name="outer",
    )(query, kv, chan, inside, outside, sink, w_pool, scale)

    def multiplied(mask, *mixed):
        count = len(mixed)
        return pl.pallas_call(
            functools.partial(out_kernel, mask, count),
            out_shape=rows_of(share, count * half),
            in_specs=[VMEM] * (2 * count + 2),
            out_specs=VMEM,
            scratch_shapes=[
                pltpu.VMEM((count * half, hidden_cols), BF16),
                pltpu.VMEM((share, hidden_cols), BF16),
            ],
            compiler_params=LIMIT,
            cost_estimate=cost(2 * count * half * share * hidden_cols, 1 << 20),
        )(*(a for pair in mixed for a in pair), own2, other2)

    def sent(mask, *mixed):
        block = multiplied(mask, *mixed)
        count = lax.axis_size(TP)
        return lax.ppermute(block, TP, [(i, i ^ mask) for i in range(count)])

    far = jnp.concatenate([sent(2, inner), sent(2, outer)])
    partials = [sent(1, inner, outer), sent(3, inner, outer), far]
    mix = multiplied(0, inner, outer).astype(F32)
    for partial in partials:
        mix = mix + partial.astype(F32)
    stats = jnp.stack([jnp.sum(mix, axis=1), jnp.sum(mix * mix, axis=1)])
    stats = of_everyone(stats, TP)
    row_mean = stats[0] / model_width
    variance = stats[1] / model_width - row_mean * row_mean
    normed = (mix - row_mean[:, None]) * lax.rsqrt(variance + epsilon)[:, None] * out_gain
    normed = normed.astype(BF16)
    return jnp.concatenate([normed[half : half + WINDOW], normed[:half], normed[half + WINDOW :]])


def solution(mesh):
    finer = Mesh(mesh.devices.reshape(16, 4, 2, mesh.shape["tp"]), ("sp_0", "sp_1", "sp_2", "tp"))
    return jax.shard_map(
        layer,
        mesh=finer,
        in_specs=(
            P(SP, "tp"),
            P(SP, "tp"),
            P(SP, "tp"),
            P(SP, "tp"),
            P(SP, "tp"),
            P("tp"),
            P("tp", None, None),
            P("tp"),
            P("tp", SP),
            P("tp", SP),
            P("tp"),
        ),
        out_specs=P(SP, "tp"),
        check_vma=False,
    )
```

```python
import functools

import jax
import jax.numpy as jnp
from jax import lax
from jax.experimental import pallas as pl
from jax.experimental.pallas import tpu as pltpu
from jax.sharding import Mesh
from jax.sharding import PartitionSpec as P


HEAD_DIM = 64
PAIR = 2 * HEAD_DIM
POOL_GROUPS = 4
RIM = 2 ** (POOL_GROUPS - 1)
WINDOW = 128
SP = ("sp_0", "sp_1", "sp_2")
Z, X, CORE = SP
TP = "tp"
BF16, F32 = jnp.bfloat16, jnp.float32

epsilon = 1e-05
masked_score = -1e30
nt = (((1,), (1,)), ((), ()))


def from_everyone(shard, axis):
    count = lax.axis_size(axis)
    return lax.all_to_all(
        jnp.broadcast_to(shard[None], (count, *shard.shape)), axis, 0, 0, tiled=True
    )


def of_everyone(shard, axis):
    return jnp.sum(from_everyone(shard, axis), axis=0)


def swapped(shard):
    return lax.ppermute(shard, CORE, [(0, 1), (1, 0)])


def neighbours(inside, outside):
    count = lax.axis_size(SP)
    pairs = [(i, i + 1) for i in range(1, count - 1, 2)]
    return swapped(inside), lax.ppermute(outside, SP, pairs + [(b, a) for a, b in pairs])


def whole_weights(own_ref, other_ref, w_ref, at):
    core = lax.axis_index(CORE)
    xs, zs, rows = own_ref.shape[:3]
    lanes = slice(at, at + w_ref.shape[1])
    for z in range(zs):
        for x in range(xs):
            base = (z * xs + x) * 2 * rows
            w_ref[pl.ds(pl.multiple_of(base + core * rows, rows), rows), :] = own_ref[
                x, z, :, lanes
            ]
            w_ref[pl.ds(pl.multiple_of(base + (1 - core) * rows, rows), rows), :] = other_ref[
                x, z, :, lanes
            ]


def projected(tokens_ref, w_ref, at, width):
    depth = tokens_ref.shape[2]
    total = None
    for p in range(tokens_ref.shape[0]):
        part = jnp.dot(
            tokens_ref[p],
            w_ref[p * depth : (p + 1) * depth, at : at + width],
            preferred_element_type=F32,
        )
        total = part if total is None else total + part
    return total.astype(BF16)


def copies_kernel(shard_ref, copies_ref, held_ref, read_sems, write_sems):
    count, chunks = copies_ref.shape[0], read_sems.shape[0]
    rows = shard_ref.shape[0] // chunks
    reads = [
        pltpu.make_async_copy(
            shard_ref.at[pl.ds(i * rows, rows)], held_ref.at[pl.ds(i * rows, rows)], read_sems.at[i]
        )
        for i in range(chunks)
    ]
    for read in reads:
        read.start()
    writes = []
    for i in range(chunks):
        reads[i].wait()
        here = pl.ds(i * rows, rows)
        for to in range(count):
            write = pltpu.make_async_copy(
                held_ref.at[here], copies_ref.at[to, here], write_sems.at[i, to]
            )
            write.start()
            writes.append(write)
    for write in writes:
        write.wait()


def project_kernel(
    tokens_ref, own_ref, other_ref, kv_ref, chan_ref, inside_ref, outside_ref, w_ref
):
    rows = tokens_ref.shape[1]
    whole_weights(own_ref, other_ref, w_ref, 0)
    kv_cols = kv_ref.shape[1]
    kv_ref[...] = projected(tokens_ref, w_ref, 0, kv_cols)
    chan_ref[...] = projected(tokens_ref, w_ref, kv_cols, chan_ref.shape[1])

    def rim(kv_at, chan_at):
        edge = chan_ref[chan_at : chan_at + RIM].astype(F32)
        kv = kv_ref[kv_at : kv_at + WINDOW].astype(F32)
        return jnp.concatenate([kv, edge[:, :PAIR], edge[:, PAIR:]])

    first, last = rim(0, 0), rim(rows - WINDOW, rows - RIM)
    ahead = lax.axis_index(CORE) == 0
    inside_ref[...] = jnp.where(ahead, last, first).astype(BF16)
    outside_ref[...] = jnp.where(ahead, first, last).astype(BF16)


def split_band(kv, band_ref):
    kv = kv.astype(F32)
    turned = pltpu.roll(kv, HEAD_DIM, 1)
    low = lax.broadcasted_iota(jnp.int32, kv.shape, 1) < HEAD_DIM
    band_ref[0] = jnp.where(low, kv, 0.0).astype(BF16)
    band_ref[1] = jnp.where(low, 0.0, turned).astype(BF16)
    band_ref[2] = jnp.where(low, turned, 0.0).astype(BF16)
    band_ref[3] = jnp.where(low, 0.0, kv).astype(BF16)


def attend_block(queries, band_ref, at, sink_ref, attended_ref, to):
    row = lax.broadcasted_iota(jnp.int32, (WINDOW, 3 * WINDOW), 0)
    col = lax.broadcasted_iota(jnp.int32, (WINDOW, 3 * WINDOW), 1)
    keep = (col >= row) & (col <= row + 2 * WINDOW)
    band = pl.ds(at, 3 * WINDOW)
    for pair in range(queries.shape[1] // PAIR):
        lanes = slice(pair * PAIR, (pair + 1) * PAIR)
        attended = jnp.zeros((WINDOW, PAIR), F32)
        for side in range(2):
            scores = lax.dot_general(
                queries[:, lanes], band_ref[side, band], nt, preferred_element_type=F32
            ) * HEAD_DIM ** (-0.5)
            scores = jnp.where(keep, scores, masked_score)
            sink = sink_ref[2 * pair + side]
            top = jnp.maximum(jnp.max(scores, axis=1, keepdims=True), sink)
            raised = jnp.exp(scores - top)
            total = jnp.sum(raised, axis=1, keepdims=True) + jnp.exp(sink - top)
            probs = (raised * (1.0 / total)).astype(BF16)
            attended += jnp.dot(probs, band_ref[2 + side, band], preferred_element_type=F32)
        attended_ref[to : to + WINDOW, lanes] = attended.astype(BF16)


def split_band_across(kv, keys_ref, values_ref):
    kv = kv.astype(F32)
    low = lax.broadcasted_iota(jnp.int32, kv.shape, 1) < HEAD_DIM
    keys_ref[0] = jnp.where(low, kv, 0.0).astype(BF16)
    keys_ref[1] = jnp.where(low, 0.0, pltpu.roll(kv, HEAD_DIM, 1)).astype(BF16)
    values_ref[...] = kv.T[HEAD_DIM:].astype(BF16)


def attend_edge(queries, has_before, has_after, keys_ref, values_ref, at, sink_ref, out_ref, to):
    key = lax.broadcasted_iota(jnp.int32, (WINDOW, WINDOW), 0)
    query = lax.broadcasted_iota(jnp.int32, (WINDOW, WINDOW), 1)
    band = pl.ds(at, 3 * WINDOW)
    keep_before, keep_after = (key >= query) & has_before, (key <= query) & has_after
    for pair in range(queries.shape[1] // PAIR):
        lanes = slice(pair * PAIR, (pair + 1) * PAIR)
        attended = []
        for side in range(2):
            scores = lax.dot_general(
                keys_ref[side, band], queries[:, lanes], nt, preferred_element_type=F32
            ) * HEAD_DIM ** (-0.5)
            thirds = (
                jnp.where(keep_before, scores[:WINDOW], masked_score),
                scores[WINDOW : 2 * WINDOW],
                jnp.where(keep_after, scores[2 * WINDOW :], masked_score),
            )
            sink = sink_ref[2 * pair + side]
            most = jnp.maximum(jnp.maximum(thirds[0], thirds[2]), thirds[1])
            top = jnp.maximum(jnp.max(most, axis=0, keepdims=True), sink)
            raised = [jnp.exp(third - top) for third in thirds]
            total = jnp.sum(raised[0] + raised[1] + raised[2], axis=0, keepdims=True)
            scale = 1.0 / (total + jnp.exp(sink - top))
            probs = jnp.concatenate([(third * scale).astype(BF16) for third in raised])
            attended.append(jnp.dot(values_ref[:, band], probs, preferred_element_type=F32))
        out_ref[to : to + WINDOW, lanes] = jnp.concatenate(attended).T.astype(BF16)


def pooled_rows(chan, centre, first_pos, seq_len, w_pool_ref, scale_ref):
    y = lax.axis_index(TP)
    length = chan.shape[0]
    sums = chan + pltpu.roll(chan, 1, 0)
    window_sum = sums
    for level in range(1, POOL_GROUPS):
        step = 2 ** (level - 1)
        sums = pltpu.roll(sums, step, 0) + pltpu.roll(sums, length - step, 0)
        window_sum = jnp.where(y >= level, sums, window_sum)
    half_width = jnp.left_shift(jnp.int32(1), y)
    rows = 2 * WINDOW
    row = lax.broadcasted_iota(jnp.int32, (rows, 1), 0)
    pos = row + jnp.where(row < WINDOW, first_pos[0], first_pos[1])
    count = jnp.minimum(pos + half_width, seq_len) - jnp.maximum(pos - half_width, 0)
    spread = centre(window_sum) / count.astype(F32) - centre(chan)
    pooled = jnp.dot(spread.astype(BF16), w_pool_ref[0], preferred_element_type=F32)
    return (pooled * scale_ref[...]).astype(BF16)


def inner_kernel(
    seq_len,
    tokens_ref,
    own_ref,
    other_ref,
    kv_ref,
    chan_ref,
    sink_ref,
    w_pool_ref,
    scale_ref,
    query_ref,
    attended_ref,
    pooled_ref,
    w_ref,
    band_ref,
):
    rows, query_cols = query_ref.shape
    whole_weights(own_ref, other_ref, w_ref, own_ref.shape[3] - query_cols)
    split_band(kv_ref[...], band_ref)
    for b in (1, rows // WINDOW - 2, 0, rows // WINDOW - 1):
        here = slice(b * WINDOW, (b + 1) * WINDOW)
        queries = projected(tokens_ref.at[:, here], w_ref, 0, query_cols)
        query_ref[here] = queries
        if 0 < b < rows // WINDOW - 1:
            attend_block(
                queries, band_ref, (b - 1) * WINDOW, sink_ref, attended_ref, (b - 1) * WINDOW
            )
    near = 2 * RIM
    chan = chan_ref[WINDOW - near : rows - WINDOW + near].astype(F32)
    offset = lax.axis_index(SP) * rows + WINDOW
    pooled_ref[...] = pooled_rows(
        chan, lambda a: a[near:-near], (offset, offset), seq_len, w_pool_ref, scale_ref
    )


def outer_kernel(
    seq_len,
    query_ref,
    kv_ref,
    chan_ref,
    inside_ref,
    outside_ref,
    sink_ref,
    w_pool_ref,
    scale_ref,
    attended_ref,
    pooled_ref,
    keys_ref,
    values_ref,
):
    rows = chan_ref.shape[0]
    offset = lax.axis_index(SP) * rows
    ahead = lax.axis_index(CORE) == 0
    inside, outside = inside_ref[...].astype(F32), outside_ref[...].astype(F32)
    before, after = jnp.where(ahead, outside, inside), jnp.where(ahead, inside, outside)

    split_band_across(
        jnp.concatenate(
            [
                before[:WINDOW],
                kv_ref[: 2 * WINDOW].astype(F32),
                kv_ref[rows - 2 * WINDOW :].astype(F32),
                after[:WINDOW],
            ]
        ),
        keys_ref,
        values_ref,
    )
    for edge, start in enumerate((0, rows - WINDOW)):
        attend_edge(
            query_ref[start : start + WINDOW],
            offset + start > 0,
            offset + start + WINDOW < seq_len,
            keys_ref,
            values_ref,
            edge * 3 * WINDOW,
            sink_ref,
            attended_ref,
            edge * WINDOW,
        )

    def rim(packed):
        return jnp.concatenate([packed[WINDOW : WINDOW + RIM], packed[WINDOW + RIM :]], axis=1)

    near = 2 * RIM
    first = chan_ref[: WINDOW + near].astype(F32)
    last = chan_ref[rows - WINDOW - near :].astype(F32)
    chan = jnp.concatenate([rim(before), first, last, rim(after)])

    def centre(a):
        return jnp.concatenate([a[RIM : RIM + WINDOW], a[-RIM - WINDOW : -RIM]])

    pooled_ref[...] = pooled_rows(
        chan, centre, (offset, offset + rows - 2 * WINDOW), seq_len, w_pool_ref, scale_ref
    )


def out_kernel(mask, count, *refs):
    mixed_refs, (own_ref, other_ref, out_ref, hidden_ref, w_ref) = refs[: 2 * count], refs[2 * count :]
    to = lax.axis_index(TP) ^ mask
    zs = own_ref.shape[1] // lax.axis_size(TP)
    at = own_ref.shape[3] - hidden_ref.shape[1]
    mine = pl.ds(to * zs, zs)
    whole_weights(own_ref.at[:, mine], other_ref.at[:, mine], w_ref, at)
    for part in range(count):
        attended_ref, pooled_ref = mixed_refs[2 * part : 2 * part + 2]
        rows, query_cols = attended_ref.shape
        here = slice(part * rows, (part + 1) * rows)
        hidden_ref[here, :query_cols] = attended_ref[...]
        hidden_ref[here, query_cols:] = pooled_ref[...]
    out_ref[...] = lax.dot_general(
        hidden_ref[...], w_ref[...], nt, preferred_element_type=F32
    ).astype(BF16)


def with_far_block(kernel, ins, outs, *refs):
    own_ref, other_ref = refs[ins : ins + 2]
    made, sent_ref = refs[ins + 2 : ins + 2 + outs], refs[ins + 2 + outs]
    kernel(*refs[:ins], *made, *refs[ins + 3 + outs : -2])
    out_kernel(2, 1, *made[-2:], own_ref, other_ref, sent_ref, *refs[-2:])


VMEM = pl.BlockSpec(memory_space=pltpu.VMEM)
SMEM = pl.BlockSpec(memory_space=pltpu.SMEM)
ANY = pl.BlockSpec(memory_space=pl.ANY)
LIMIT = pltpu.CompilerParams(vmem_limit_bytes=20 * 1024 * 1024)


def layer(
    tokens,
    w_query,
    w_key,
    w_value,
    w_pool_in,
    sink,
    w_pool,
    pool_scale,
    w_out_attn,
    w_out_pool,
    out_gain,
):
    rows = tokens.shape[0]
    seq_len = rows * lax.axis_size(SP)
    query_cols, key_cols, chan_cols = w_query.shape[1], w_key.shape[1], w_pool_in.shape[1]
    in_cols = 2 * key_cols + chan_cols + query_cols
    hidden_cols = query_cols + chan_cols
    share = out_gain.shape[0]
    model_width = share * lax.axis_size(TP)

    count, chunks = lax.axis_size(TP), 4
    copies = pl.pallas_call(
        copies_kernel,
        out_shape=jax.ShapeDtypeStruct((count, *tokens.shape), BF16),
        in_specs=[ANY],
        out_specs=ANY,
        scratch_shapes=[
            pltpu.VMEM(tokens.shape, BF16),
            pltpu.SemaphoreType.DMA((chunks,)),
            pltpu.SemaphoreType.DMA((chunks, count)),
        ],
        cost_estimate=pl.CostEstimate(
            flops=0, bytes_accessed=5 * tokens.size * 2, transcendentals=0
        ),
        name="copies",
    )(tokens)
    gathered = lax.all_to_all(copies, TP, 0, 0, tiled=True)
    packed = jnp.concatenate(
        (w_key, w_value, w_pool_in, w_query, w_out_attn.T, w_out_pool.T), axis=1
    )
    over_z = lax.all_gather(packed, Z, axis=0)
    over_x = from_everyone(over_z, X)
    own1, own2 = over_x[..., :in_cols], over_x[..., in_cols:]
    other1 = swapped(own1)
    other2 = swapped(own2)

    def rows_of(width, count=rows):
        return jax.ShapeDtypeStruct((count, width), BF16)

    def cost(flops, size):
        return pl.CostEstimate(flops=flops, bytes_accessed=size, transcendentals=0)

    rim_shape = rows_of(PAIR, WINDOW + 2 * RIM)
    kv, chan, inside, outside = pl.pallas_call(
        project_kernel,
        out_shape=[rows_of(2 * key_cols), rows_of(chan_cols), rim_shape, rim_shape],
        in_specs=[VMEM] * 3,
        out_specs=[VMEM] * 4,
        scratch_shapes=[pltpu.VMEM((model_width, 2 * key_cols + chan_cols), BF16)],
        compiler_params=LIMIT,
        cost_estimate=cost(2 * rows * model_width * (in_cols - query_cols), 4 << 20),
        name="project",
    )(gathered, own1, other1)
    inside, outside = neighbours(inside, outside)
    half = rows // 2
    scale = pool_scale.reshape(1, -1)
    far_scratch = [
        pltpu.VMEM((half, hidden_cols), BF16),
        pltpu.VMEM((share, hidden_cols), BF16),
    ]
    query, *inner, far_inner = pl.pallas_call(
        functools.partial(with_far_block, functools.partial(inner_kernel, seq_len), 8, 3),
        out_shape=[
            rows_of(query_cols),
            rows_of(query_cols, half),
            rows_of(chan_cols, half),
            rows_of(share, half),
        ],
        in_specs=[VMEM] * 5 + [SMEM] + [VMEM] * 4,
        out_specs=[VMEM] * 4,
        scratch_shapes=[
            pltpu.VMEM((model_width, query_cols), BF16),
            pltpu.VMEM((4, rows, PAIR), BF16),
            *far_scratch,
        ],
        compiler_params=LIMIT,
        cost_estimate=cost(2 * rows * model_width * query_cols, 4 << 20),
        name="inner",
    )(gathered, own1, other1, kv, chan, sink, w_pool, scale, own2, other2)
    *outer, far_outer = pl.pallas_call(
        functools.partial(with_far_block, functools.partial(outer_kernel, seq_len), 8, 2),
        out_shape=[
            rows_of(query_cols, half),
            rows_of(chan_cols, half),
            rows_of(share, half),
        ],
        in_specs=[VMEM] * 5 + [SMEM] + [VMEM] * 4,
        out_specs=[VMEM] * 3,
        scratch_shapes=[
            pltpu.VMEM((2, 6 * WINDOW, PAIR), BF16),
            pltpu.VMEM((HEAD_DIM, 6 * WINDOW), BF16),
            *far_scratch,
        ],
        compiler_params=LIMIT,
        cost_estimate=cost(2 * rows * model_width * query_cols, 2 << 20),
        name="outer",
    )(query, kv, chan, inside, outside, sink, w_pool, scale, own2, other2)

    def multiplied(mask, *mixed):
        count = len(mixed)
        return pl.pallas_call(
            functools.partial(out_kernel, mask, count),
            out_shape=rows_of(share, count * half),
            in_specs=[VMEM] * (2 * count + 2),
            out_specs=VMEM,
            scratch_shapes=[
                pltpu.VMEM((count * half, hidden_cols), BF16),
                pltpu.VMEM((share, hidden_cols), BF16),
            ],
            compiler_params=LIMIT,
            cost_estimate=cost(2 * count * half * share * hidden_cols, 1 << 20),
        )(*(a for pair in mixed for a in pair), own2, other2)

    def sent(mask, block):
        return lax.ppermute(block, TP, [(i, i ^ mask) for i in range(lax.axis_size(TP))])

    far = jnp.concatenate([sent(2, far_inner), sent(2, far_outer)])
    partials = [sent(1, multiplied(1, inner, outer)), sent(3, multiplied(3, inner, outer)), far]
    mix = multiplied(0, inner, outer).astype(F32)
    for partial in partials:
        mix = mix + partial.astype(F32)
    stats = jnp.stack([jnp.sum(mix, axis=1), jnp.sum(mix * mix, axis=1)])
    stats = of_everyone(stats, TP)
    row_mean = stats[0] / model_width
    variance = stats[1] / model_width - row_mean * row_mean
    normed = (mix - row_mean[:, None]) * lax.rsqrt(variance + epsilon)[:, None] * out_gain
    normed = normed.astype(BF16)
    return jnp.concatenate([normed[half : half + WINDOW], normed[:half], normed[half + WINDOW :]])


def solution(mesh):
    finer = Mesh(mesh.devices.reshape(16, 4, 2, mesh.shape["tp"]), ("sp_0", "sp_1", "sp_2", "tp"))
    return jax.shard_map(
        layer,
        mesh=finer,
        in_specs=(
            P(SP, "tp"),
            P(SP, "tp"),
            P(SP, "tp"),
            P(SP, "tp"),
            P(SP, "tp"),
            P("tp"),
            P("tp", None, None),
            P("tp"),
            P("tp", SP),
            P("tp", SP),
            P("tp"),
        ),
        out_specs=P(SP, "tp"),
        check_vma=False,
    )
```
